128 devices in a mesh: sp: 64 (over z, y, x), tp: 2 (over core).
Axes of the slice: x: 4, y: 4, z: 4, core: 2. Of those that a mesh axis runs over, the one named last changes fastest.
Arguments:
- residual: bfloat16 [16384, 2048], P(('sp', 'tp')), may hold values from -6 to 6
- queries: bfloat16 [16384, 512], P('sp', 'tp'), may hold values from -6 to 6
- key_rows: bfloat16 [16384, 512], P('sp', 'tp'), may hold values from -6 to 6
- value_rows: bfloat16 [16384, 1024], P('sp', 'tp'), may hold values from -6 to 6
- out_gate: bfloat16 [16384, 1024], P('sp', 'tp'), may hold values from -6 to 6
- gate_logits: bfloat16 [16384, 512], P('sp', 'tp')
- head_gain: float32 [128], replicated, may hold values from 0.1 to 1.9
- out_weight: bfloat16 [1024, 2048], replicated, may hold values from -0.1875 to 0.1875
- norm_gain: float32 [2048], replicated, may hold values from 0.1 to 1.9
- routes: int32 [16384, 2], P(('sp', 'tp')), may hold values from 0 to 127, as said below
- group_score: float32 [16384], P(('sp', 'tp')), may hold values from 0.25 to 1
- expert_score: float32 [16384, 2], P(('sp', 'tp')), may hold values from 0.1 to 1
- gate_weight: bfloat16 [128, 2048, 512], P(('sp', 'tp')), may hold values from -0.125 to 0.125
- up_weight: bfloat16 [128, 2048, 512], P(('sp', 'tp')), may hold values from -0.125 to 0.125
- down_weight: bfloat16 [128, 512, 2048], P(('sp', 'tp')), may hold values from -0.25 to 0.25
Outputs:
- layer_out: bfloat16 [16384, 2048], P(('sp', 'tp'))
The draws below stay inside these ranges and needn't reach their ends.
Inputs may be any that keep to these rules, and one draw needn't show every extreme that they name: `routes`: the two experts of a token differ and lie in one group of 8 consecutive expert numbers. In each aligned block of 128 tokens (the tokens of one device) no expert is named more than 3 times, and one expert, the same for all blocks of a draw, is named exactly 3 times in every block.
All inputs are finite; a program needn't handle non-finite values.
Results may differ from the reference program's by a relative error of at most 0.0056.
Values may be sent and summed in bfloat16 or wider, within the bound.
No kernel may reach another device: no remote copies, remote signals or barrier semaphores. Data moves between devices by JAX's collectives and lax.ppermute only.
A program may use at most 64 MiB of HBM per device.

```python
import math
from functools import partial
import jax
import jax.numpy as jnp
from jax import lax

MODEL_WIDTH = 2048
HEADS = 8
KEY_DIM = 64
VALUE_DIM = 128
EXPERT_WIDTH = 512
GROUP_SIZE = 8
BLOCK = 64
SEGMENT = 256
KEYS = 512
VALUES = 1024
ROWS = 128
TOKENS = 16384
EXPERTS = 128
GROUPS = 16
CAPACITY = 3


def draw_gate_logits(key, part):
    subkeys = jax.random.split(key, 7)
    slow_share = 0.5
    slow_heads = jax.random.bernoulli(subkeys[0], slow_share, (HEADS,))
    chain_loss = jnp.exp(jax.random.uniform(subkeys[1], (HEADS, KEY_DIM), jnp.float32, jnp.log(0.2), jnp.log(0.8)))
    slow_logit = jnp.log(TOKENS / (16.0 * chain_loss))
    fast_rate = jnp.exp(jax.random.uniform(subkeys[2], (HEADS, KEY_DIM), jnp.float32, jnp.log(1.0 / 100.0), jnp.log(1.0 / 30.0)))
    fast_logit = -jnp.log(jnp.expm1(16.0 * fast_rate))
    base_logit = jnp.where(slow_heads[:, None], slow_logit, fast_logit)
    jitter = jax.random.uniform(subkeys[3], (TOKENS, HEADS, KEY_DIM), jnp.float32, -1.0, 1.0)
    offset = jax.random.uniform(subkeys[4], (TOKENS // SEGMENT, HEADS), jnp.float32, -0.7, 0.7)
    offset = jnp.repeat(offset, SEGMENT, axis=0)
    router_scores = base_logit[None] + jitter + offset[:, :, None]
    slot_places = jax.random.randint(subkeys[5], (2, HEADS), 0, TOKENS)
    spike_strength = jax.random.uniform(subkeys[6], (2, HEADS), jnp.float32, -11.0, -4.0)
    token_position = jnp.arange(TOKENS, dtype=jnp.int32)[:, None]
    spike_value = jnp.where(token_position == slot_places[0][None, :], spike_strength[0][None, :], spike_strength[1][None, :])
    spike_mask = (token_position == slot_places[0][None, :]) | (token_position == slot_places[1][None, :])
    router_scores = jnp.where(spike_mask[:, :, None], spike_value[:, :, None], router_scores)
    return router_scores.reshape(TOKENS, HEADS * KEY_DIM).astype(jnp.bfloat16)


def shuffle_group(group_key):
    return jax.random.permutation(group_key, GROUP_SIZE).astype(jnp.int32)


def route_block(block_key, hot_expert):
    subkeys = jax.random.split(block_key, 4)
    slot_total = GROUPS * 3 * CAPACITY
    labels = (jax.random.permutation(subkeys[0], slot_total) // (3 * CAPACITY)).astype(jnp.int32)
    chosen = labels[:5 * ROWS // 8]
    group_index = jnp.arange(GROUPS, dtype=jnp.int32)
    extra_count = jnp.sum((chosen[:, None] == group_index[None, :]).astype(jnp.int32), axis=0)
    tickets = 2 * CAPACITY + 2 * extra_count
    group_rows = tickets // 2
    hot_group = hot_expert // GROUP_SIZE
    hot_local = hot_expert % GROUP_SIZE
    orders = jax.vmap(shuffle_group)(jax.random.split(subkeys[1], GROUPS))
    rank_grid = jnp.arange(GROUP_SIZE, dtype=jnp.int32)[None, :]
    hot_row = (group_index == hot_group)[:, None]
    sort_key = jnp.where(hot_row & (orders == hot_local), -1, rank_grid)
    orders = jnp.take_along_axis(orders, jnp.argsort(sort_key, axis=1, stable=True), axis=1)
    remaining = tickets[:, None] - CAPACITY
    hot_counts = jnp.where(rank_grid == 0, CAPACITY, remaining // (GROUP_SIZE - 1) + (rank_grid - 1 < remaining % (GROUP_SIZE - 1)).astype(jnp.int32))
    drawn_counts = tickets[:, None] // GROUP_SIZE + (rank_grid < tickets[:, None] % GROUP_SIZE).astype(jnp.int32)
    counts = jnp.where(hot_row, hot_counts, drawn_counts)
    count_ends = jnp.cumsum(counts, axis=1)
    row_ends = jnp.cumsum(group_rows)
    row_ids = jnp.arange(ROWS, dtype=jnp.int32)
    group_of = jnp.sum((row_ids[:, None] >= row_ends[None, :]).astype(jnp.int32), axis=1)
    start_of = row_ends[group_of] - group_rows[group_of]
    first_pos = row_ids - start_of
    second_pos = first_pos + group_rows[group_of]
    ends_table = count_ends[group_of]
    first_rank = jnp.sum((first_pos[:, None] >= ends_table).astype(jnp.int32), axis=1)
    second_rank = jnp.sum((second_pos[:, None] >= ends_table).astype(jnp.int32), axis=1)
    order_rows = orders[group_of]
    first_expert = group_of * GROUP_SIZE + jnp.take_along_axis(order_rows, first_rank[:, None], axis=1)[:, 0]
    second_expert = group_of * GROUP_SIZE + jnp.take_along_axis(order_rows, second_rank[:, None], axis=1)[:, 0]
    expert_pairs = jnp.stack([first_expert, second_expert], axis=1)
    flip_order = jax.random.randint(subkeys[2], (ROWS,), 0, 2)
    expert_pairs = jnp.where(flip_order[:, None] == 1, expert_pairs[:, ::-1], expert_pairs)
    shuffled = expert_pairs[jax.random.permutation(subkeys[3], ROWS)]
    return shuffled.astype(jnp.int32)


def draw_routes(key, part):
    hot_expert = jax.random.randint(jax.random.fold_in(key, 11), (), 0, EXPERTS)
    block_keys = jax.random.split(jax.random.fold_in(key, 12), TOKENS // ROWS)
    blocks_out = jax.vmap(partial(route_block, hot_expert=hot_expert))(block_keys)
    return blocks_out.reshape(TOKENS, 2).astype(jnp.int32)


def block_scale(stream_key, dims, cuts, smallest, top_value):
    factor_of = 1.0
    for position, blocks in cuts:
        steps = jax.random.uniform(jax.random.fold_in(jax.random.fold_in(stream_key, 6), position), (blocks,), jnp.float32, smallest / len(cuts), top_value / len(cuts))
        factor_of = factor_of * jnp.repeat(jnp.exp(steps), dims[position] // blocks).reshape((-1,) + (1,) * (len(dims) - 1 - position))
    return factor_of


def gaussian(key, dims, spread, reach, cuts=(), held_as=jnp.bfloat16):
    drawn = jax.random.normal(key, dims, jnp.float32) * spread
    if len(cuts) > 0:
        drawn = block_scale(key, dims, cuts, -0.22, 0.18) * drawn
    return jnp.clip(drawn, min=-reach, max=reach).astype(held_as)


def setup_inputs(seed: int = 0) -> dict:
    arg_keys = jax.random.split(jax.random.key(seed), 16)
    residual = gaussian(arg_keys[0], (TOKENS, MODEL_WIDTH), 1.0, 6.0, ((0, 128),))
    queries = gaussian(arg_keys[1], (TOKENS, KEYS), 1.0, 6.0, ((0, 64), (1, 2)))
    key_rows = gaussian(arg_keys[2], (TOKENS, KEYS), 1.0, 6.0, ((0, 64), (1, 2)))
    value_rows = gaussian(arg_keys[3], (TOKENS, VALUES), 1.0, 6.0, ((0, 64), (1, 2)))
    out_gate = gaussian(arg_keys[4], (TOKENS, VALUES), 1.0, 6.0, ((0, 64), (1, 2)))
    gate_logits = draw_gate_logits(jax.random.fold_in(arg_keys[15], 71), 0)
    head_gain = jnp.clip(1.0 + 0.18 * jax.random.normal(arg_keys[6], (VALUE_DIM,), jnp.float32), 0.1, 1.9)
    out_weight = gaussian(arg_keys[7], (VALUES, MODEL_WIDTH), VALUES ** -0.5, 0.1875)
    norm_gain = jnp.clip(1.0 + 0.18 * jax.random.normal(arg_keys[8], (MODEL_WIDTH,), jnp.float32), 0.1, 1.9)
    routes = draw_routes(jax.random.fold_in(arg_keys[15], 71), 0)
    group_score = jnp.clip(0.25 + 0.75 * jax.random.uniform(arg_keys[10], (TOKENS,), jnp.float32) ** block_scale(arg_keys[10], (TOKENS,), ((0, 128),), -0.2, 0.2), 0.25, 1.0)
    expert_score = jnp.clip(jnp.exp(math.log(1.0) - 2.3025851 * jax.random.uniform(arg_keys[11], (TOKENS, 2), jnp.float32) ** block_scale(arg_keys[11], (TOKENS, 2), ((0, 128),), -0.2, 0.2)), 0.1, 1.0)
    gate_weight = gaussian(arg_keys[12], (EXPERTS, MODEL_WIDTH, EXPERT_WIDTH), MODEL_WIDTH ** -0.5, 0.125, ((0, 128),))
    up_weight = gaussian(arg_keys[13], (EXPERTS, MODEL_WIDTH, EXPERT_WIDTH), MODEL_WIDTH ** -0.5, 0.125, ((0, 128),))
    down_weight = gaussian(arg_keys[14], (EXPERTS, EXPERT_WIDTH, MODEL_WIDTH), EXPERT_WIDTH ** -0.5, 0.25, ((0, 128),))
    return dict(residual=residual, queries=queries, key_rows=key_rows, value_rows=value_rows, out_gate=out_gate, gate_logits=gate_logits, head_gain=head_gain, out_weight=out_weight, norm_gain=norm_gain, routes=routes, group_score=group_score, expert_score=expert_score, gate_weight=gate_weight, up_weight=up_weight, down_weight=down_weight)


def block_parts(queries, key_rows, value_rows, gate_logits):
    length = queries.shape[0]
    head_count = queries.shape[1] // KEY_DIM
    blocks = length // BLOCK

    def arrange(source, inner_size):
        return source.astype(jnp.float32).reshape(blocks, BLOCK, head_count, inner_size).transpose(0, 2, 1, 3)
    decay_log = jax.nn.log_sigmoid(gate_logits.astype(jnp.float32)) / 16.0
    running = jnp.cumsum(arrange(decay_log, KEY_DIM), axis=2)
    closing = running[:, :, -1:, :]
    query_scaled = arrange(queries, KEY_DIM) * KEY_DIM ** (-0.5) * jnp.exp(running)
    key_float = arrange(key_rows, KEY_DIM)
    key_inverse = key_float * jnp.exp(-running)
    key_closing = key_float * jnp.exp(closing - running)
    value_float = arrange(value_rows, VALUE_DIM)
    causal = jnp.tril(jnp.ones((BLOCK, BLOCK), dtype=bool))
    scores = jnp.where(causal, jnp.einsum('nhcd,nhsd->nhcs', query_scaled, key_inverse, precision=lax.Precision.HIGHEST), 0.0)
    within = jnp.einsum('nhcs,nhsv->nhcv', scores, value_float, precision=lax.Precision.HIGHEST)
    increments = jnp.einsum('nhcd,nhcv->nhdv', key_closing, value_float, precision=lax.Precision.HIGHEST)
    return (query_scaled, within, increments, closing[:, :, 0, :])

def advance(carried, inputs):
    increment, block_log = inputs
    return (jnp.exp(block_log)[..., None] * carried + increment, carried)

def finish(attended, head_gain, out_gate):
    blocks = attended.shape[0]
    head_count = attended.shape[1]
    length = blocks * BLOCK
    ordered = attended.transpose(0, 2, 1, 3).reshape(length, head_count, VALUE_DIM)
    normed = ordered * lax.rsqrt(lax.optimization_barrier(jnp.mean(ordered * ordered, axis=-1, keepdims=True)) + 1e-06) * head_gain
    gating = jax.nn.silu(out_gate.astype(jnp.float32)).reshape(length, head_count, VALUE_DIM)
    return (normed * gating).reshape(length, head_count * VALUE_DIM).astype(jnp.bfloat16)

def route_slots(block_routes, experts_total, capacity):
    row_count = block_routes.shape[0]
    flattened = block_routes.reshape(-1)
    onehot = (flattened[:, None] == jnp.arange(experts_total, dtype=jnp.int32)[None, :]).astype(jnp.int32)
    ranking = lax.optimization_barrier(jnp.sum((jnp.cumsum(onehot, axis=0) - onehot) * onehot, axis=1))
    slot_index = flattened * capacity + ranking
    route_ids = jnp.arange(2 * row_count, dtype=jnp.int32) // 2
    owners = jnp.full((experts_total * capacity,), row_count, jnp.int32).at[slot_index].set(route_ids)
    return (slot_index, owners)

def expert_apply(rows_in, gate_matrix, up_matrix, down_matrix):
    gated = jnp.dot(rows_in, gate_matrix, preferred_element_type=jnp.float32)
    lifted = jnp.dot(rows_in, up_matrix, preferred_element_type=jnp.float32)
    inner_rows = (jax.nn.silu(gated) * lifted).astype(jnp.bfloat16)
    return jnp.dot(inner_rows, down_matrix, preferred_element_type=jnp.float32).astype(jnp.bfloat16)

def reference(residual, queries, key_rows, value_rows, out_gate, gate_logits, head_gain, out_weight, norm_gain, routes, group_score, expert_score, gate_weight, up_weight, down_weight):
    query_scaled, within, increments, block_logs = block_parts(queries, key_rows, value_rows, gate_logits)
    zero_state = jnp.zeros(increments.shape[1:], jnp.float32)
    _, states = lax.scan(advance, zero_state, (increments, block_logs))
    attended = within + jnp.einsum('nhcd,nhdv->nhcv', query_scaled, states, precision=lax.Precision.HIGHEST)
    mixer_out = finish(attended, head_gain, out_gate)
    summed = residual.astype(jnp.float32) + jnp.dot(mixer_out, out_weight, preferred_element_type=jnp.float32)
    merged = summed.astype(jnp.bfloat16)
    widened = lax.optimization_barrier(merged).astype(jnp.float32)
    normed = (widened * lax.rsqrt(lax.optimization_barrier(jnp.mean(widened * widened, axis=-1, keepdims=True)) + 1e-06) * norm_gain).astype(jnp.bfloat16)
    tokens_total = residual.shape[0]
    model_width = residual.shape[1]
    blocks = tokens_total // ROWS
    experts_total = gate_weight.shape[0]
    slot_index, owners = jax.vmap(partial(route_slots, experts_total=experts_total, capacity=CAPACITY))(routes.reshape(blocks, ROWS, 2))
    offsets = (jnp.arange(blocks, dtype=jnp.int32) * ROWS)[:, None]
    sources = jnp.where(owners < ROWS, owners + offsets, tokens_total).astype(jnp.int32)
    padded = jnp.concatenate([normed, jnp.zeros((1, model_width), jnp.bfloat16)], axis=0)
    per_expert = sources.reshape(blocks, experts_total, CAPACITY).transpose(1, 0, 2).reshape(experts_total, blocks * CAPACITY)

    def serve(inputs):
        indices, gate_matrix, up_matrix, down_matrix = inputs
        return expert_apply(padded[indices], gate_matrix, up_matrix, down_matrix)
    results = lax.map(serve, (per_expert, gate_weight, up_weight, down_weight))
    expert_ids = routes.reshape(blocks, 2 * ROWS)
    ranking = slot_index - expert_ids * CAPACITY
    block_base = (jnp.arange(blocks, dtype=jnp.int32) * CAPACITY)[:, None]
    token_position = (expert_ids * (blocks * CAPACITY) + block_base + ranking).astype(jnp.int32)
    picked = results.reshape(-1, model_width)[token_position.reshape(-1)].reshape(tokens_total, 2, model_width)
    weights = group_score[:, None] * expert_score / lax.optimization_barrier(jnp.sum(expert_score, axis=1, keepdims=True))
    combined = weights[:, 0:1] * picked[:, 0].astype(jnp.float32) + weights[:, 1:2] * picked[:, 1].astype(jnp.float32)
    return (widened + combined).astype(jnp.bfloat16)
```

```python
import jax
import jax.numpy as jnp
from jax import lax
from jax.experimental import pallas as pl
from jax.experimental.pallas import tpu as pltpu
from jax.sharding import Mesh
from jax.sharding import PartitionSpec as P

KEY_DIM = 64
VALUE_DIM = 128
BLOCK = 64
SP = ("sp_0", "sp_1", "sp_2")
SP_TP = ("sp_0", "sp_1", "sp_2", "tp")


def neutral_like(value, identity):
    return jax.tree.map(
        lambda part, zero: jnp.zeros_like(part) + jnp.asarray(zero, part.dtype), value, identity
    )


def entering_2(value, axes, combine, identity):
    before = start = neutral_like(value, identity)
    so_far = value
    for axis in reversed(axes):
        peers, place = (lax.axis_size(axis), lax.axis_index(axis))
        pieces = jax.tree.map(lambda part: lax.all_gather(part, axis), so_far)
        inside, so_far = (start, start)
        for k in range(peers):
            passed = k < place
            so_far = combine(so_far, jax.tree.map(lambda part: part[k], pieces))
            inside = jax.tree.map(lambda new, old: jnp.where(passed, new, old), so_far, inside)
        before = combine(inside, before)
    return before


def block_parts(queries, key_rows, value_rows, gate_logits):
    length = queries.shape[0]
    head_count = queries.shape[1] // KEY_DIM
    blocks = length // BLOCK

    def arrange(source, inner_size):
        return (
            source.astype(jnp.float32)
            .reshape(blocks, BLOCK, head_count, inner_size)
            .transpose(0, 2, 1, 3)
        )

    decay_log = jax.nn.log_sigmoid(gate_logits.astype(jnp.float32)) / 16.0
    running = jnp.cumsum(arrange(decay_log, KEY_DIM), axis=2)
    closing = running[:, :, -1:, :]
    query_scaled = arrange(queries, KEY_DIM) * KEY_DIM ** (-0.5) * jnp.exp(running)
    key_float = arrange(key_rows, KEY_DIM)
    key_inverse = key_float * jnp.exp(-running)
    key_closing = key_float * jnp.exp(closing - running)
    value_float = arrange(value_rows, VALUE_DIM)
    causal = jnp.tril(jnp.ones((BLOCK, BLOCK), dtype=bool))
    scores = jnp.where(
        causal,
        jnp.einsum("nhcd,nhsd->nhcs", query_scaled, key_inverse, precision=lax.Precision.HIGHEST),
        0.0,
    )
    within = jnp.einsum("nhcs,nhsv->nhcv", scores, value_float, precision=lax.Precision.HIGHEST)
    increments = jnp.einsum(
        "nhcd,nhcv->nhdv", key_closing, value_float, precision=lax.Precision.HIGHEST
    )
    return (query_scaled, within, increments, closing[:, :, 0, :])


def advance(carried, inputs):
    increment, block_log = inputs
    return (jnp.exp(block_log)[..., None] * carried + increment, carried)


def finish(attended, head_gain, out_gate):
    blocks = attended.shape[0]
    head_count = attended.shape[1]
    length = blocks * BLOCK
    ordered = attended.transpose(0, 2, 1, 3).reshape(length, head_count, VALUE_DIM)
    normed = (
        ordered * lax.rsqrt(jnp.mean(ordered * ordered, axis=-1, keepdims=True) + 1e-06) * head_gain
    )
    gating = jax.nn.silu(out_gate.astype(jnp.float32)).reshape(length, head_count, VALUE_DIM)
    return (normed * gating).reshape(length, head_count * VALUE_DIM).astype(jnp.bfloat16)


VMEM_SPEC = pl.BlockSpec(memory_space=pltpu.VMEM)
SMEM_SPEC = pl.BlockSpec(memory_space=pltpu.SMEM)
ANY_SPEC = pl.BlockSpec(memory_space=pl.ANY)
SUB = 16
LANES = 128
SWAP = SUB * SUB


def swap_matrix():
    row = lax.broadcasted_iota(jnp.int32, (SWAP, SWAP), 0)
    column = lax.broadcasted_iota(jnp.int32, (SWAP, SWAP), 1)
    partner = (row & (SUB - 1)) * SUB + (row >> 4)
    return (partner == column).astype(jnp.float32).astype(jnp.bfloat16)


def exchange(swap, block):
    return jnp.dot(swap, block, preferred_element_type=jnp.float32)


def routing_kernel(routes_ref, slots_ref, owners_ref, counts):
    experts_total = counts.shape[0]
    slot_count = owners_ref.shape[0]
    route_count = routes_ref.shape[0]
    capacity = slot_count // experts_total

    def clear_counts(i, carry):
        counts[i] = 0
        return carry

    def clear_owners(i, carry):
        owners_ref[i] = 0
        return carry

    def place(i, carry):
        expert = routes_ref[i]
        used = counts[expert]
        counts[expert] = used + 1
        slot = expert * capacity + used
        slots_ref[i] = slot
        owners_ref[slot] = i // 2
        return carry

    lax.fori_loop(0, experts_total, clear_counts, 0, unroll=8)
    lax.fori_loop(0, slot_count, clear_owners, 0, unroll=8)
    lax.fori_loop(0, route_count, place, 0, unroll=4)


def routing(routes, experts_total, capacity):
    flattened = routes.reshape(-1)
    return pl.pallas_call(
        routing_kernel,
        out_shape=(
            jax.ShapeDtypeStruct(flattened.shape, jnp.int32),
            jax.ShapeDtypeStruct((experts_total * capacity,), jnp.int32),
        ),
        in_specs=[SMEM_SPEC],
        out_specs=(SMEM_SPEC, SMEM_SPEC),
        scratch_shapes=[pltpu.SMEM((experts_total,), jnp.int32)],
        name="routing",
    )(flattened)


def dispatch_kernel(owners_ref, normed_ref, outgoing_ref, chunked):
    swap = swap_matrix()
    rows, width = normed_ref.shape
    for g in range(rows // SUB):
        stacked = jnp.concatenate(
            [normed_ref[g * SUB : (g + 1) * SUB, j * LANES : (j + 1) * LANES] for j in range(width // LANES)],
            axis=0,
        )
        chunked[g * SUB : (g + 1) * SUB] = (
            exchange(swap, stacked).astype(jnp.bfloat16).reshape(SUB, SUB, LANES)
        )

    def copy_row(slot, carry):
        outgoing_ref[slot] = chunked[owners_ref[slot]]
        return carry

    lax.fori_loop(0, outgoing_ref.shape[0], copy_row, 0, unroll=16)


def dispatch(owners, normed):
    rows, width = normed.shape
    return pl.pallas_call(
        dispatch_kernel,
        out_shape=jax.ShapeDtypeStruct((owners.shape[0], SUB, LANES), jnp.bfloat16),
        in_specs=[SMEM_SPEC, VMEM_SPEC],
        out_specs=VMEM_SPEC,
        scratch_shapes=[pltpu.VMEM((rows, SUB, LANES), jnp.bfloat16)],
        name="dispatch",
    )(owners, normed)


def experts_kernel(rows_ref, gate_hbm, up_hbm, down_hbm, out_ref, gate, up, down, rows_in, inner, served, sems):
    copies = [
        pltpu.make_async_copy(source.at[0], target, sems.at[k])
        for k, (source, target) in enumerate(((gate_hbm, gate), (up_hbm, up), (down_hbm, down)))
    ]
    for copy in copies:
        copy.start()
    swap = swap_matrix()
    count, width = rows_in.shape
    hidden = inner.shape[1]
    for g in range(count // SUB):
        block = rows_ref[g * SUB : (g + 1) * SUB].reshape(SWAP, LANES)
        turned = exchange(swap, block).astype(jnp.bfloat16)
        for j in range(width // LANES):
            rows_in[g * SUB : (g + 1) * SUB, j * LANES : (j + 1) * LANES] = turned[j * SUB : (j + 1) * SUB]
    copies[0].wait()
    copies[1].wait()
    tile = 256
    for n in range(hidden // tile):
        part = slice(n * tile, (n + 1) * tile)
        gated = jnp.dot(rows_in[...], gate[:, part], preferred_element_type=jnp.float32)
        lifted = jnp.dot(rows_in[...], up[:, part], preferred_element_type=jnp.float32)
        inner[:, part] = (gated / (1.0 + jnp.exp(-gated)) * lifted).astype(jnp.bfloat16)
    copies[2].wait()
    for n in range(width // tile):
        part = slice(n * tile, (n + 1) * tile)
        served[:, part] = jnp.dot(inner[...], down[:, part], preferred_element_type=jnp.float32).astype(jnp.bfloat16)
    for g in range(count // SUB):
        stacked = jnp.concatenate(
            [served[g * SUB : (g + 1) * SUB, j * LANES : (j + 1) * LANES] for j in range(width // LANES)], axis=0
        )
        out_ref[g * SUB : (g + 1) * SUB] = (
            exchange(swap, stacked).astype(jnp.bfloat16).reshape(SUB, SUB, LANES)
        )


def experts(arrived, gate_weight, up_weight, down_weight):
    count = arrived.shape[0]
    width, hidden = gate_weight.shape[1:]
    return pl.pallas_call(
        experts_kernel,
        out_shape=jax.ShapeDtypeStruct(arrived.shape, jnp.bfloat16),
        in_specs=[VMEM_SPEC, ANY_SPEC, ANY_SPEC, ANY_SPEC],
        out_specs=VMEM_SPEC,
        scratch_shapes=[
            pltpu.VMEM((width, hidden), jnp.bfloat16),
            pltpu.VMEM((width, hidden), jnp.bfloat16),
            pltpu.VMEM((hidden, width), jnp.bfloat16),
            pltpu.VMEM((count, width), jnp.bfloat16),
            pltpu.VMEM((count, hidden), jnp.bfloat16),
            pltpu.VMEM((count, width), jnp.bfloat16),
            pltpu.SemaphoreType.DMA((3,)),
        ],
        name="experts",
    )(arrived, gate_weight, up_weight, down_weight)


def combine_kernel(slots_ref, returned_ref, merged_ref, weights_ref, out_ref, picked):
    swap = swap_matrix()
    rows, width = merged_ref.shape

    def copy_row(i, carry):
        picked[0, i] = returned_ref[slots_ref[2 * i]]
        picked[1, i] = returned_ref[slots_ref[2 * i + 1]]
        return carry

    lax.fori_loop(0, rows, copy_row, 0, unroll=8)
    for g in range(rows // SUB):
        group = slice(g * SUB, (g + 1) * SUB)
        first = exchange(swap, picked[0, group].reshape(SWAP, LANES))
        second = exchange(swap, picked[1, group].reshape(SWAP, LANES))
        weight_first = jnp.broadcast_to(weights_ref[group, 0:1], (SUB, LANES))
        weight_second = jnp.broadcast_to(weights_ref[group, 1:2], (SUB, LANES))
        for j in range(width // LANES):
            lanes = slice(j * LANES, (j + 1) * LANES)
            part = slice(j * SUB, (j + 1) * SUB)
            total = weight_first * first[part] + weight_second * second[part]
            out_ref[group, lanes] = (merged_ref[group, lanes].astype(jnp.float32) + total).astype(jnp.bfloat16)


def combine(slots, returned, merged, weights):
    rows = merged.shape[0]
    return pl.pallas_call(
        combine_kernel,
        out_shape=jax.ShapeDtypeStruct(merged.shape, jnp.bfloat16),
        in_specs=[SMEM_SPEC, VMEM_SPEC, VMEM_SPEC, VMEM_SPEC],
        out_specs=VMEM_SPEC,
        scratch_shapes=[pltpu.VMEM((2, rows, SUB, LANES), jnp.bfloat16)],
        name="combine",
    )(slots, returned, merged, weights)


def merge_states(earlier, later):
    return (earlier[0] * later[0], later[0][..., None] * earlier[1] + later[1])


def local(
    residual,
    queries,
    key_rows,
    value_rows,
    out_gate,
    gate_logits,
    head_gain,
    out_weight,
    norm_gain,
    routes,
    group_score,
    expert_score,
    gate_weight,
    up_weight,
    down_weight,
):
    query_scaled, within, increments, block_logs = block_parts(
        queries, key_rows, value_rows, gate_logits
    )
    zero_state = jnp.zeros(increments.shape[1:], jnp.float32)
    local_end, local_prefix = lax.scan(advance, zero_state, (increments, block_logs))
    device_decay = jnp.exp(jnp.sum(block_logs, axis=0))
    identity = (jnp.ones_like(device_decay), jnp.zeros_like(local_end))
    entering = entering_2((device_decay, local_end), SP, merge_states, identity)[1]
    leading = jnp.exp(jnp.cumsum(block_logs, axis=0) - block_logs)
    states = leading[..., None] * entering[None] + local_prefix
    attended = within + jnp.einsum(
        "nhcd,nhdv->nhcv", query_scaled, states, precision=lax.Precision.HIGHEST
    )
    mixer_out = finish(attended, head_gain, out_gate)
    row_count = residual.shape[0]
    model_width = residual.shape[1]
    pair_count = lax.axis_size("tp")
    chip_count = lax.axis_size(SP)
    regrouped = lax.all_to_all(mixer_out, "tp", split_axis=0, concat_axis=1, tiled=True)
    projected = jnp.dot(regrouped, out_weight, preferred_element_type=jnp.float32)
    merged = (residual.astype(jnp.float32) + projected).astype(jnp.bfloat16)
    widened = lax.optimization_barrier(merged).astype(jnp.float32)
    normed = (
        widened * lax.rsqrt(jnp.mean(widened * widened, axis=-1, keepdims=True) + 1e-06) * norm_gain
    ).astype(jnp.bfloat16)
    experts_total = chip_count * pair_count
    capacity = 3 * row_count // experts_total
    slots, owners = routing(routes, experts_total, capacity)
    outgoing = dispatch(owners, normed)
    block = (experts_total, capacity * SUB, LANES)
    arrived = lax.all_to_all(outgoing.reshape(block), SP_TP, split_axis=0, concat_axis=0, tiled=True)
    served = experts(arrived.reshape(outgoing.shape), gate_weight, up_weight, down_weight)
    returned = lax.all_to_all(served.reshape(block), SP_TP, split_axis=0, concat_axis=0, tiled=True)
    weights = group_score[:, None] * expert_score / jnp.sum(expert_score, axis=1, keepdims=True)
    return combine(slots, returned.reshape(outgoing.shape), merged, weights)


def solution(mesh):
    torus = Mesh(mesh.devices.reshape(4, 4, 4, mesh.shape["tp"]), ("sp_0", "sp_1", "sp_2", "tp"))
    in_specs = (
        P(SP_TP, None),
        P(SP, "tp"),
        P(SP, "tp"),
        P(SP, "tp"),
        P(SP, "tp"),
        P(SP, "tp"),
        P(),
        P(),
        P(),
        P(SP_TP, None),
        P(SP_TP),
        P(SP_TP, None),
        P(SP_TP, None, None),
        P(SP_TP, None, None),
        P(SP_TP, None, None),
    )
    out_specs = P(SP_TP, None)
    return jax.shard_map(local, mesh=torus, in_specs=in_specs, out_specs=out_specs, check_vma=False)
```

```python
import jax
import jax.numpy as jnp
from jax import lax
from jax.experimental import pallas as pl
from jax.experimental.pallas import tpu as pltpu
from jax.sharding import Mesh
from jax.sharding import PartitionSpec as P

KEY_DIM = 64
VALUE_DIM = 128
BLOCK = 64
RING = 4
SP = ("sp_0", "sp_1", "sp_2")
SP_TP = ("sp_0", "sp_1", "sp_2", "tp")


VMEM_SPEC = pl.BlockSpec(memory_space=pltpu.VMEM)
SMEM_SPEC = pl.BlockSpec(memory_space=pltpu.SMEM)
ANY_SPEC = pl.BlockSpec(memory_space=pl.ANY)
SUB = 16
LANES = 128
SWAP = SUB * SUB


def swap_matrix():
    row = lax.broadcasted_iota(jnp.int32, (SWAP, SWAP), 0)
    column = lax.broadcasted_iota(jnp.int32, (SWAP, SWAP), 1)
    partner = (row & (SUB - 1)) * SUB + (row >> 4)
    return (partner == column).astype(jnp.float32).astype(jnp.bfloat16)


def exchange(swap, block):
    return jnp.dot(swap, block, preferred_element_type=jnp.float32)


def routing_kernel(routes_ref, slots_ref, owners_ref, counts):
    experts_total = counts.shape[0]
    slot_count = owners_ref.shape[0]
    route_count = routes_ref.shape[0]
    capacity = slot_count // experts_total

    def clear_counts(i, carry):
        counts[i] = 0
        return carry

    def clear_owners(i, carry):
        owners_ref[i] = 0
        return carry

    def place(i, carry):
        expert = routes_ref[i]
        used = counts[expert]
        counts[expert] = used + 1
        slot = expert * capacity + used
        slots_ref[i] = slot
        owners_ref[slot] = i // 2
        return carry

    lax.fori_loop(0, experts_total, clear_counts, 0, unroll=8)
    lax.fori_loop(0, slot_count, clear_owners, 0, unroll=8)
    lax.fori_loop(0, route_count, place, 0, unroll=4)


def routing(routes, experts_total, capacity):
    flattened = routes.reshape(-1)
    return pl.pallas_call(
        routing_kernel,
        out_shape=(
            jax.ShapeDtypeStruct(flattened.shape, jnp.int32),
            jax.ShapeDtypeStruct((experts_total * capacity,), jnp.int32),
        ),
        in_specs=[SMEM_SPEC],
        out_specs=(SMEM_SPEC, SMEM_SPEC),
        scratch_shapes=[pltpu.SMEM((experts_total,), jnp.int32)],
        name="routing",
    )(flattened)


def experts_kernel(rows_ref, gate_hbm, up_hbm, down_hbm, out_ref, gate, up, down, rows_in, inner, served, sems):
    copies = [
        pltpu.make_async_copy(source.at[0], target, sems.at[k])
        for k, (source, target) in enumerate(((gate_hbm, gate), (up_hbm, up), (down_hbm, down)))
    ]
    for copy in copies:
        copy.start()
    swap = swap_matrix()
    count, width = rows_in.shape
    hidden = inner.shape[1]
    for g in range(count // SUB):
        block = rows_ref[g * SUB : (g + 1) * SUB].reshape(SWAP, LANES)
        turned = exchange(swap, block).astype(jnp.bfloat16)
        for j in range(width // LANES):
            rows_in[g * SUB : (g + 1) * SUB, j * LANES : (j + 1) * LANES] = turned[j * SUB : (j + 1) * SUB]
    copies[0].wait()
    copies[1].wait()
    tile = 256
    for n in range(hidden // tile):
        part = slice(n * tile, (n + 1) * tile)
        gated = jnp.dot(rows_in[...], gate[:, part], preferred_element_type=jnp.float32)
        lifted = jnp.dot(rows_in[...], up[:, part], preferred_element_type=jnp.float32)
        inner[:, part] = (gated / (1.0 + jnp.exp(-gated)) * lifted).astype(jnp.bfloat16)
    copies[2].wait()
    for n in range(width // tile):
        part = slice(n * tile, (n + 1) * tile)
        served[:, part] = jnp.dot(inner[...], down[:, part], preferred_element_type=jnp.float32).astype(jnp.bfloat16)
    for g in range(count // SUB):
        stacked = jnp.concatenate(
            [served[g * SUB : (g + 1) * SUB, j * LANES : (j + 1) * LANES] for j in range(width // LANES)], axis=0
        )
        out_ref[g * SUB : (g + 1) * SUB] = (
            exchange(swap, stacked).astype(jnp.bfloat16).reshape(SUB, SUB, LANES)
        )


def experts(arrived, gate_weight, up_weight, down_weight):
    count = arrived.shape[0]
    width, hidden = gate_weight.shape[1:]
    return pl.pallas_call(
        experts_kernel,
        out_shape=jax.ShapeDtypeStruct(arrived.shape, jnp.bfloat16),
        in_specs=[VMEM_SPEC, ANY_SPEC, ANY_SPEC, ANY_SPEC],
        out_specs=VMEM_SPEC,
        scratch_shapes=[
            pltpu.VMEM((width, hidden), jnp.bfloat16),
            pltpu.VMEM((width, hidden), jnp.bfloat16),
            pltpu.VMEM((hidden, width), jnp.bfloat16),
            pltpu.VMEM((count, width), jnp.bfloat16),
            pltpu.VMEM((count, hidden), jnp.bfloat16),
            pltpu.VMEM((count, width), jnp.bfloat16),
            pltpu.SemaphoreType.DMA((3,)),
        ],
        name="experts",
    )(arrived, gate_weight, up_weight, down_weight)


def combine_kernel(slots_ref, returned_ref, merged_ref, weights_ref, out_ref, picked):
    swap = swap_matrix()
    rows, width = merged_ref.shape

    def copy_row(i, carry):
        picked[0, i] = returned_ref[slots_ref[2 * i]]
        picked[1, i] = returned_ref[slots_ref[2 * i + 1]]
        return carry

    lax.fori_loop(0, rows, copy_row, 0, unroll=8)
    for g in range(rows // SUB):
        group = slice(g * SUB, (g + 1) * SUB)
        first = exchange(swap, picked[0, group].reshape(SWAP, LANES))
        second = exchange(swap, picked[1, group].reshape(SWAP, LANES))
        weight_first = jnp.broadcast_to(weights_ref[group, 0:1], (SUB, LANES))
        weight_second = jnp.broadcast_to(weights_ref[group, 1:2], (SUB, LANES))
        for j in range(width // LANES):
            lanes = slice(j * LANES, (j + 1) * LANES)
            part = slice(j * SUB, (j + 1) * SUB)
            total = weight_first * first[part] + weight_second * second[part]
            out_ref[group, lanes] = (merged_ref[group, lanes].astype(jnp.float32) + total).astype(jnp.bfloat16)


def combine(slots, returned, merged, weights):
    rows = merged.shape[0]
    return pl.pallas_call(
        combine_kernel,
        out_shape=jax.ShapeDtypeStruct(merged.shape, jnp.bfloat16),
        in_specs=[SMEM_SPEC, VMEM_SPEC, VMEM_SPEC, VMEM_SPEC],
        out_specs=VMEM_SPEC,
        scratch_shapes=[pltpu.VMEM((2, rows, SUB, LANES), jnp.bfloat16)],
        name="combine",
    )(slots, returned, merged, weights)


def pieces(value, count):
    parts = []
    for _ in range(count):
        part = value.astype(jnp.bfloat16)
        parts.append(part)
        value = value - part.astype(jnp.float32)
    return parts


def product(left, right, left_dim=1, right_dim=0):
    return lax.dot_general(
        left, right, (((left_dim,), (right_dim,)), ((), ())), preferred_element_type=jnp.float32
    )


def state_kernel(keys_ref, values_ref, logits_ref, running_ref, states_ref, message_ref):
    length, channels = keys_ref.shape
    blocks = length // BLOCK
    pairs = channels // LANES
    wide = 2 * VALUE_DIM
    logits = logits_ref[...].astype(jnp.float32)
    decay_log = (jnp.minimum(logits, 0.0) - jnp.log1p(jnp.exp(-jnp.abs(logits)))) / 16.0
    parts = pieces(decay_log, 3)
    row = lax.broadcasted_iota(jnp.int32, (length, length), 0)
    column = lax.broadcasted_iota(jnp.int32, (length, length), 1)
    earlier = (row >= column) & (row // BLOCK == column // BLOCK)
    earlier = earlier.astype(jnp.float32).astype(jnp.bfloat16)
    running = sum(product(earlier, part) for part in parts)
    running_ref[...] = running
    token = lax.broadcasted_iota(jnp.int32, (length, blocks * LANES), 0)
    lane = lax.broadcasted_iota(jnp.int32, (length, blocks * LANES), 1)
    member = (token // BLOCK == lane // LANES).astype(jnp.float32).astype(jnp.bfloat16)
    block_decay = jnp.exp(sum(product(part, member, 0, 0) for part in parts))
    states = [jnp.zeros((LANES, VALUE_DIM), jnp.float32)] * pairs
    total = jnp.zeros((1, channels), jnp.float32)
    for n in range(blocks):
        rows = slice(n * BLOCK, (n + 1) * BLOCK)
        closing = running[(n + 1) * BLOCK - 1 : (n + 1) * BLOCK]
        total = total + closing
        key_closing = keys_ref[rows].astype(jnp.float32) * jnp.exp(closing - running[rows])
        key_closing = key_closing.astype(jnp.bfloat16)
        for p in range(pairs):
            states_ref[p, n] = states[p].astype(jnp.bfloat16)
            grown = product(
                key_closing[:, p * LANES : (p + 1) * LANES], values_ref[rows, p * wide : (p + 1) * wide], 0, 0
            )
            grown = jnp.concatenate([grown[:KEY_DIM, :VALUE_DIM], grown[KEY_DIM:, VALUE_DIM:]], axis=0)
            decay = block_decay[p * LANES : (p + 1) * LANES, n * LANES : (n + 1) * LANES]
            states[p] = decay * states[p] + grown
    for p in range(pairs):
        message_ref[p * LANES : (p + 1) * LANES] = states[p].astype(jnp.bfloat16)
    message_ref[channels:] = pack_decay(jnp.exp(total))


def pack_decay(decay):
    pairs = decay.shape[1] // LANES
    place = lax.broadcasted_iota(jnp.int32, (SUB, LANES), 0)
    high, low = pieces(decay, 2)
    packed = jnp.zeros((SUB, LANES), jnp.float32)
    for p in range(pairs):
        lanes = slice(p * LANES, (p + 1) * LANES)
        packed = jnp.where(place == p, high[:, lanes].astype(jnp.float32), packed)
        packed = jnp.where(place == pairs + p, low[:, lanes].astype(jnp.float32), packed)
    return packed.astype(jnp.bfloat16)


def unpack_decay(message_ref):
    channels = message_ref.shape[0] - SUB
    pairs = channels // LANES
    packed = message_ref[channels:].astype(jnp.float32)
    diagonal = lax.broadcasted_iota(jnp.int32, (LANES, LANES), 0) == lax.broadcasted_iota(
        jnp.int32, (LANES, LANES), 1
    )
    ones = jnp.ones((LANES, VALUE_DIM), jnp.bfloat16)
    spread = []
    for p in range(pairs):
        both = [jnp.where(diagonal, packed[k : k + 1], 0.0).astype(jnp.bfloat16) for k in (p, pairs + p)]
        spread.append(product(both[0], ones) + product(both[1], ones))
    line = jnp.concatenate([packed[p : p + 1] + packed[pairs + p : pairs + p + 1] for p in range(pairs)], axis=1)
    return line, jnp.concatenate(spread, axis=0)


def stage_kernel(place_ref, own_ref, back1_ref, back2_ref, back3_ref, before_ref, decay_ref, message_ref):
    place = place_ref[0]
    channels = own_ref.shape[0] - SUB
    received = []
    for ref in (back1_ref, back2_ref, back3_ref):
        line, spread = unpack_decay(ref)
        received.append((line, spread, ref[:channels].astype(jnp.float32)))
    own_line, own_spread = unpack_decay(own_ref)
    before = jnp.zeros((channels, VALUE_DIM), jnp.float32)
    decay = jnp.ones((channels, VALUE_DIM), jnp.float32)
    for k in (3, 2, 1):
        valid = place >= k
        _, spread, state = received[k - 1]
        before = jnp.where(valid, spread * before + state, before)
        decay = jnp.where(valid, spread * decay, decay)
    before_ref[...] = before
    decay_ref[...] = decay
    total = own_spread * before + own_ref[:channels].astype(jnp.float32)
    for k in (3, 2, 1):
        later = place < k
        _, spread, state = received[k - 1]
        total = jnp.where(later, spread * total + state, total)
    message_ref[:channels] = total.astype(jnp.bfloat16)
    line = own_line * received[0][0] * received[1][0] * received[2][0]
    message_ref[channels:] = pack_decay(line)


def masked_heads(rows):
    lane = lax.broadcasted_iota(jnp.int32, rows.shape, 1)
    return jnp.concatenate(
        [jnp.where(lane < KEY_DIM, rows, 0.0), jnp.where(lane >= KEY_DIM, rows, 0.0)], axis=0
    ).astype(jnp.bfloat16)


def within_kernel(queries_ref, keys_ref, values_ref, running_ref, states_ref, partial_ref, reach_ref):
    length, channels = keys_ref.shape
    blocks = length // BLOCK
    pairs = channels // LANES
    lead = jnp.zeros((1, channels), jnp.float32)
    row = lax.broadcasted_iota(jnp.int32, (2 * BLOCK, BLOCK), 0)
    column = lax.broadcasted_iota(jnp.int32, (2 * BLOCK, BLOCK), 1)
    causal = (row & (BLOCK - 1)) >= column
    for n in range(blocks):
        rows = slice(n * BLOCK, (n + 1) * BLOCK)
        running = running_ref[rows]
        query_scaled = queries_ref[rows].astype(jnp.float32) * KEY_DIM ** (-0.5) * jnp.exp(running)
        key_inverse = (keys_ref[rows].astype(jnp.float32) * jnp.exp(-running)).astype(jnp.bfloat16)
        reach_ref[rows] = query_scaled * jnp.exp(lead)
        lead = lead + running[BLOCK - 1 : BLOCK]
        for p in range(pairs):
            lanes = slice(p * LANES, (p + 1) * LANES)
            masked = masked_heads(query_scaled[:, lanes])
            scores = jnp.where(causal, product(masked, key_inverse[:, lanes], 1, 1), 0.0).astype(jnp.bfloat16)
            carried = product(masked, states_ref[p, n])
            for h in range(2):
                place = slice((2 * p + h) * VALUE_DIM, (2 * p + h + 1) * VALUE_DIM)
                part = slice(h * BLOCK, (h + 1) * BLOCK)
                partial_ref[rows, place] = product(scores[part], values_ref[rows, place]) + carried[part]


def finish_kernel(
    place_ref, back1_ref, back2_ref, back3_ref, before_y_ref, decay_y_ref, before_x_ref, decay_x_ref,
    partial_ref, reach_ref, head_gain_ref, out_gate_ref, kept_ref, given_ref, whole,
):
    core = place_ref[0]
    length, channels = reach_ref.shape
    pairs = channels // LANES
    state = jnp.zeros((channels, VALUE_DIM), jnp.float32)
    for ref in (back3_ref, back2_ref, back1_ref):
        state = unpack_decay(ref)[1] * state + ref[:channels].astype(jnp.float32)
    state = before_y_ref[...] + decay_y_ref[...] * state
    state = (before_x_ref[...] + decay_x_ref[...] * state).astype(jnp.bfloat16)
    half = length // 2
    for p in range(pairs):
        lanes = slice(p * LANES, (p + 1) * LANES)
        carried = product(masked_heads(reach_ref[:, lanes]), state[lanes])
        for h in range(2):
            place = slice((2 * p + h) * VALUE_DIM, (2 * p + h + 1) * VALUE_DIM)
            attended = partial_ref[:, place] + carried[h * length : (h + 1) * length]
            scale = lax.rsqrt(jnp.mean(attended * attended, axis=1, keepdims=True) + 1e-06)
            gate = out_gate_ref[:, place].astype(jnp.float32)
            result = attended * scale * head_gain_ref[...] * (gate / (1.0 + jnp.exp(-gate)))
            result = result.astype(jnp.bfloat16)
            whole[0, :, place] = result[:half]
            whole[1, :, place] = result[half:]
    kept_ref[...] = whole[core]
    given_ref[...] = whole[1 - core]


def project_kernel(
    place_ref, owners_ref, kept_ref, taken_ref, weight_ref, residual_ref, norm_gain_ref, merged_ref, outgoing_ref,
    chunked,
):
    core = place_ref[0]
    rows, width = residual_ref.shape
    depth = kept_ref.shape[1]
    tile = 256
    own = pl.ds(pl.multiple_of(core * depth, depth), depth)
    other = pl.ds(pl.multiple_of((1 - core) * depth, depth), depth)
    square = jnp.zeros((rows, 1), jnp.float32)
    for n in range(width // tile):
        part = slice(n * tile, (n + 1) * tile)
        projected = product(kept_ref[...], weight_ref[own, part]) + product(taken_ref[...], weight_ref[other, part])
        merged = (residual_ref[:, part].astype(jnp.float32) + projected).astype(jnp.bfloat16)
        merged_ref[:, part] = merged
        widened = merged.astype(jnp.float32)
        square = square + jnp.sum(widened * widened, axis=1, keepdims=True)
    scale = lax.rsqrt(square / width + 1e-06)
    swap = swap_matrix()
    for g in range(rows // SUB):
        group = slice(g * SUB, (g + 1) * SUB)
        stacked = []
        for j in range(width // LANES):
            lanes = slice(j * LANES, (j + 1) * LANES)
            widened = merged_ref[group, lanes].astype(jnp.float32)
            stacked.append((widened * scale[group] * norm_gain_ref[:, lanes]).astype(jnp.bfloat16))
        turned = exchange(swap, jnp.concatenate(stacked, axis=0)).astype(jnp.bfloat16)
        chunked[group] = turned.reshape(SUB, SUB, LANES)

    def copy_row(slot, carry):
        outgoing_ref[slot] = chunked[owners_ref[slot]]
        return carry

    lax.fori_loop(0, outgoing_ref.shape[0], copy_row, 0, unroll=16)


def shape_of(shape, dtype):
    return jax.ShapeDtypeStruct(shape, dtype)


def call(kernel, name, outs, operands, scalars=0, scratch=(), cost=2000000):
    return pl.pallas_call(
        kernel,
        out_shape=outs,
        in_specs=[SMEM_SPEC] * scalars + [VMEM_SPEC] * (len(operands) - scalars),
        out_specs=jax.tree.map(lambda _: VMEM_SPEC, outs),
        scratch_shapes=list(scratch),
        cost_estimate=pl.CostEstimate(flops=cost * 400, bytes_accessed=cost, transcendentals=0),
        name=name,
    )(*operands)


def from_behind(message, axis, wrap):
    return [
        lax.ppermute(
            message, axis, [(i, (i + k) % RING) for i in range(RING) if wrap or i + k < RING]
        )
        for k in range(1, RING)
    ]


def local(
    residual,
    queries,
    key_rows,
    value_rows,
    out_gate,
    gate_logits,
    head_gain,
    out_weight,
    norm_gain,
    routes,
    group_score,
    expert_score,
    gate_weight,
    up_weight,
    down_weight,
):
    row_count, model_width = residual.shape
    length, channels = queries.shape
    values = value_rows.shape[1]
    blocks = length // BLOCK
    pairs = channels // LANES
    f32, bf16 = jnp.float32, jnp.bfloat16
    z, y, x, core = (lax.axis_index(axis).astype(jnp.int32).reshape(1) for axis in SP_TP)
    message_shape = shape_of((channels + SUB, VALUE_DIM), bf16)
    state_shape = shape_of((channels, VALUE_DIM), f32)
    running, states, message = call(
        state_kernel,
        "local_state",
        (
            shape_of((length, channels), f32),
            shape_of((pairs, blocks, LANES, VALUE_DIM), bf16),
            message_shape,
        ),
        (key_rows, value_rows, gate_logits),
    )
    behind = from_behind(message, "sp_2", True)
    before_x, decay_x, message_x = call(
        stage_kernel, "stage_x", (state_shape, state_shape, message_shape), (x, message, *behind), 1
    )
    partial, reach = call(
        within_kernel,
        "within",
        (shape_of((length, values), f32), shape_of((length, channels), f32)),
        (queries, key_rows, value_rows, running, states),
    )
    behind = from_behind(message_x, "sp_1", True)
    before_y, decay_y, message_y = call(
        stage_kernel, "stage_y", (state_shape, state_shape, message_shape), (y, message_x, *behind), 1
    )
    behind = from_behind(message_y, "sp_0", False)
    half = shape_of((length // 2, values), bf16)
    kept, given = call(
        finish_kernel,
        "finish",
        (half, half),
        (core, *behind, before_y, decay_y, before_x, decay_x, partial, reach, head_gain.reshape(1, -1), out_gate),
        1,
        [pltpu.VMEM((2, length // 2, values), bf16)],
    )
    taken = lax.ppermute(given, "tp", [(0, 1), (1, 0)])
    experts_total = lax.axis_size(SP_TP)
    capacity = 3 * row_count // experts_total
    slots, owners = routing(routes, experts_total, capacity)
    merged, outgoing = call(
        project_kernel,
        "project",
        (
            shape_of((row_count, model_width), bf16),
            shape_of((experts_total * capacity, SUB, LANES), bf16),
        ),
        (core, owners, kept, taken, out_weight, residual, norm_gain.reshape(1, -1)),
        2,
        [pltpu.VMEM((row_count, SUB, LANES), bf16)],
    )
    block = (experts_total, capacity * SUB, LANES)
    arrived = lax.all_to_all(outgoing.reshape(block), SP_TP, split_axis=0, concat_axis=0, tiled=True)
    served = experts(arrived.reshape(outgoing.shape), gate_weight, up_weight, down_weight)
    returned = lax.all_to_all(served.reshape(block), SP_TP, split_axis=0, concat_axis=0, tiled=True)
    weights = group_score[:, None] * expert_score / jnp.sum(expert_score, axis=1, keepdims=True)
    return combine(slots, returned.reshape(outgoing.shape), merged, weights)


def solution(mesh):
    torus = Mesh(mesh.devices.reshape(4, 4, 4, mesh.shape["tp"]), ("sp_0", "sp_1", "sp_2", "tp"))
    in_specs = (
        P(SP_TP, None),
        P(SP, "tp"),
        P(SP, "tp"),
        P(SP, "tp"),
        P(SP, "tp"),
        P(SP, "tp"),
        P(),
        P(),
        P(),
        P(SP_TP, None),
        P(SP_TP),
        P(SP_TP, None),
        P(SP_TP, None, None),
        P(SP_TP, None, None),
        P(SP_TP, None, None),
    )
    out_specs = P(SP_TP, None)
    return jax.shard_map(local, mesh=torus, in_specs=in_specs, out_specs=out_specs, check_vma=False)
```

```python
import jax
import jax.numpy as jnp
from jax import lax
from jax.experimental import pallas as pl
from jax.experimental.pallas import tpu as pltpu
from jax.sharding import Mesh
from jax.sharding import PartitionSpec as P

KEY_DIM = 64
VALUE_DIM = 128
BLOCK = 64
RING = 4
SP = ("sp_0", "sp_1", "sp_2")
SP_TP = ("sp_0", "sp_1", "sp_2", "tp")


VMEM_SPEC = pl.BlockSpec(memory_space=pltpu.VMEM)
SMEM_SPEC = pl.BlockSpec(memory_space=pltpu.SMEM)
ANY_SPEC = pl.BlockSpec(memory_space=pl.ANY)
SUB = 16
LANES = 128
SWAP = SUB * SUB


def swap_matrix():
    row = lax.broadcasted_iota(jnp.int32, (SWAP, SWAP), 0)
    column = lax.broadcasted_iota(jnp.int32, (SWAP, SWAP), 1)
    partner = (row & (SUB - 1)) * SUB + (row >> 4)
    return (partner == column).astype(jnp.float32).astype(jnp.bfloat16)


def exchange(swap, block):
    return jnp.dot(swap, block, preferred_element_type=jnp.float32)


def routing_kernel(routes_ref, slots_ref, owners_ref, counts):
    experts_total = counts.shape[0]
    slot_count = owners_ref.shape[0]
    route_count = routes_ref.shape[0]
    capacity = slot_count // experts_total

    def clear_counts(i, carry):
        counts[i] = 0
        return carry

    def clear_owners(i, carry):
        owners_ref[i] = 0
        return carry

    def place(i, carry):
        expert = routes_ref[i]
        used = counts[expert]
        counts[expert] = used + 1
        slot = expert * capacity + used
        slots_ref[i] = slot
        owners_ref[slot] = i // 2
        return carry

    lax.fori_loop(0, experts_total, clear_counts, 0, unroll=8)
    lax.fori_loop(0, slot_count, clear_owners, 0, unroll=8)
    lax.fori_loop(0, route_count, place, 0, unroll=4)


def routing(routes, experts_total, capacity):
    flattened = routes.reshape(-1)
    return pl.pallas_call(
        routing_kernel,
        out_shape=(
            jax.ShapeDtypeStruct(flattened.shape, jnp.int32),
            jax.ShapeDtypeStruct((experts_total * capacity,), jnp.int32),
        ),
        in_specs=[SMEM_SPEC],
        out_specs=(SMEM_SPEC, SMEM_SPEC),
        scratch_shapes=[pltpu.SMEM((experts_total,), jnp.int32)],
        compiler_params=limited(1),
        name="routing",
    )(flattened)


def experts_kernel(rows_ref, gate, up, down, out_ref, rows_in, inner, served):
    swap = swap_matrix()
    count, width = rows_in.shape
    hidden = inner.shape[1]
    for g in range(count // SUB):
        block = rows_ref[g * SUB : (g + 1) * SUB].reshape(SWAP, LANES)
        turned = exchange(swap, block).astype(jnp.bfloat16)
        for j in range(width // LANES):
            rows_in[g * SUB : (g + 1) * SUB, j * LANES : (j + 1) * LANES] = turned[j * SUB : (j + 1) * SUB]
    tile = 256
    for n in range(hidden // tile):
        part = slice(n * tile, (n + 1) * tile)
        gated = jnp.dot(rows_in[...], gate[0, :, part], preferred_element_type=jnp.float32)
        lifted = jnp.dot(rows_in[...], up[0, :, part], preferred_element_type=jnp.float32)
        inner[:, part] = (gated / (1.0 + jnp.exp(-gated)) * lifted).astype(jnp.bfloat16)
    for n in range(width // tile):
        part = slice(n * tile, (n + 1) * tile)
        served[:, part] = jnp.dot(inner[...], down[0, :, part], preferred_element_type=jnp.float32).astype(jnp.bfloat16)
    for g in range(count // SUB):
        stacked = jnp.concatenate(
            [served[g * SUB : (g + 1) * SUB, j * LANES : (j + 1) * LANES] for j in range(width // LANES)], axis=0
        )
        out_ref[g * SUB : (g + 1) * SUB] = (
            exchange(swap, stacked).astype(jnp.bfloat16).reshape(SUB, SUB, LANES)
        )


def experts(arrived, gate_weight, up_weight, down_weight):
    count = arrived.shape[0]
    width, hidden = gate_weight.shape[1:]
    return pl.pallas_call(
        experts_kernel,
        out_shape=jax.ShapeDtypeStruct(arrived.shape, jnp.bfloat16),
        in_specs=[VMEM_SPEC] * 4,
        out_specs=VMEM_SPEC,
        scratch_shapes=[
            pltpu.VMEM((count, width), jnp.bfloat16),
            pltpu.VMEM((count, hidden), jnp.bfloat16),
            pltpu.VMEM((count, width), jnp.bfloat16),
        ],
        compiler_params=limited(16),
        name="experts",
    )(arrived, gate_weight, up_weight, down_weight)


def combine_kernel(slots_ref, returned_ref, merged_ref, weights_ref, out_ref, picked):
    swap = swap_matrix()
    rows, width = merged_ref.shape

    def copy_row(i, carry):
        picked[0, i] = returned_ref[slots_ref[2 * i]]
        picked[1, i] = returned_ref[slots_ref[2 * i + 1]]
        return carry

    lax.fori_loop(0, rows, copy_row, 0, unroll=8)
    for g in range(rows // SUB):
        group = slice(g * SUB, (g + 1) * SUB)
        first = exchange(swap, picked[0, group].reshape(SWAP, LANES))
        second = exchange(swap, picked[1, group].reshape(SWAP, LANES))
        weight_first = jnp.broadcast_to(weights_ref[group, 0:1], (SUB, LANES))
        weight_second = jnp.broadcast_to(weights_ref[group, 1:2], (SUB, LANES))
        for j in range(width // LANES):
            lanes = slice(j * LANES, (j + 1) * LANES)
            part = slice(j * SUB, (j + 1) * SUB)
            total = weight_first * first[part] + weight_second * second[part]
            out_ref[group, lanes] = (merged_ref[group, lanes].astype(jnp.float32) + total).astype(jnp.bfloat16)


def combine(slots, returned, merged, weights):
    rows = merged.shape[0]
    return pl.pallas_call(
        combine_kernel,
        out_shape=jax.ShapeDtypeStruct(merged.shape, jnp.bfloat16),
        in_specs=[SMEM_SPEC, VMEM_SPEC, VMEM_SPEC, VMEM_SPEC],
        out_specs=VMEM_SPEC,
        scratch_shapes=[pltpu.VMEM((2, rows, SUB, LANES), jnp.bfloat16)],
        compiler_params=limited(8),
        name="combine",
    )(slots, returned, merged, weights)


def pieces(value, count):
    parts = []
    for _ in range(count):
        part = value.astype(jnp.bfloat16)
        parts.append(part)
        value = value - part.astype(jnp.float32)
    return parts


def product(left, right, left_dim=1, right_dim=0):
    return lax.dot_general(
        left, right, (((left_dim,), (right_dim,)), ((), ())), preferred_element_type=jnp.float32
    )


def state_kernel(keys_ref, values_ref, logits_ref, running_ref, states_ref, message_ref):
    length, channels = keys_ref.shape
    blocks = length // BLOCK
    pairs = channels // LANES
    wide = 2 * VALUE_DIM
    logits = logits_ref[...].astype(jnp.float32)
    decay_log = (jnp.minimum(logits, 0.0) - jnp.log1p(jnp.exp(-jnp.abs(logits)))) / 16.0
    parts = pieces(decay_log, 3)
    row = lax.broadcasted_iota(jnp.int32, (length, length), 0)
    column = lax.broadcasted_iota(jnp.int32, (length, length), 1)
    earlier = (row >= column) & (row // BLOCK == column // BLOCK)
    earlier = earlier.astype(jnp.float32).astype(jnp.bfloat16)
    running = sum(product(earlier, part) for part in parts)
    running_ref[...] = running
    token = lax.broadcasted_iota(jnp.int32, (length, blocks * LANES), 0)
    lane = lax.broadcasted_iota(jnp.int32, (length, blocks * LANES), 1)
    member = (token // BLOCK == lane // LANES).astype(jnp.float32).astype(jnp.bfloat16)
    block_decay = jnp.exp(sum(product(part, member, 0, 0) for part in parts))
    states = [jnp.zeros((LANES, VALUE_DIM), jnp.float32)] * pairs
    total = jnp.zeros((1, channels), jnp.float32)
    for n in range(blocks):
        rows = slice(n * BLOCK, (n + 1) * BLOCK)
        closing = running[(n + 1) * BLOCK - 1 : (n + 1) * BLOCK]
        total = total + closing
        key_closing = keys_ref[rows].astype(jnp.float32) * jnp.exp(closing - running[rows])
        key_closing = key_closing.astype(jnp.bfloat16)
        for p in range(pairs):
            states_ref[p, n] = states[p].astype(jnp.bfloat16)
            grown = product(
                key_closing[:, p * LANES : (p + 1) * LANES], values_ref[rows, p * wide : (p + 1) * wide], 0, 0
            )
            grown = jnp.concatenate([grown[:KEY_DIM, :VALUE_DIM], grown[KEY_DIM:, VALUE_DIM:]], axis=0)
            decay = block_decay[p * LANES : (p + 1) * LANES, n * LANES : (n + 1) * LANES]
            states[p] = decay * states[p] + grown
    for p in range(pairs):
        message_ref[p * LANES : (p + 1) * LANES] = states[p].astype(jnp.bfloat16)
    message_ref[channels:] = pack_decay(jnp.exp(total))


def pack_decay(decay):
    pairs = decay.shape[1] // LANES
    place = lax.broadcasted_iota(jnp.int32, (SUB, LANES), 0)
    high, low = pieces(decay, 2)
    packed = jnp.zeros((SUB, LANES), jnp.float32)
    for p in range(pairs):
        lanes = slice(p * LANES, (p + 1) * LANES)
        packed = jnp.where(place == p, high[:, lanes].astype(jnp.float32), packed)
        packed = jnp.where(place == pairs + p, low[:, lanes].astype(jnp.float32), packed)
    return packed.astype(jnp.bfloat16)


def unpack_decay(message_ref):
    channels = message_ref.shape[0] - SUB
    pairs = channels // LANES
    packed = message_ref[channels:].astype(jnp.float32)
    diagonal = lax.broadcasted_iota(jnp.int32, (LANES, LANES), 0) == lax.broadcasted_iota(
        jnp.int32, (LANES, LANES), 1
    )
    ones = jnp.ones((LANES, VALUE_DIM), jnp.bfloat16)
    spread = []
    for p in range(pairs):
        both = [jnp.where(diagonal, packed[k : k + 1], 0.0).astype(jnp.bfloat16) for k in (p, pairs + p)]
        spread.append(product(both[0], ones) + product(both[1], ones))
    line = jnp.concatenate([packed[p : p + 1] + packed[pairs + p : pairs + p + 1] for p in range(pairs)], axis=1)
    return line, jnp.concatenate(spread, axis=0)


def stage_kernel(place_ref, own_ref, back1_ref, back2_ref, back3_ref, before_ref, decay_ref, message_ref):
    place = place_ref[0]
    channels = own_ref.shape[0] - SUB
    received = []
    for ref in (back1_ref, back2_ref, back3_ref):
        line, spread = unpack_decay(ref)
        received.append((line, spread, ref[:channels].astype(jnp.float32)))
    own_line, own_spread = unpack_decay(own_ref)
    before = jnp.zeros((channels, VALUE_DIM), jnp.float32)
    decay = jnp.ones((channels, VALUE_DIM), jnp.float32)
    for k in (3, 2, 1):
        valid = place >= k
        _, spread, state = received[k - 1]
        before = jnp.where(valid, spread * before + state, before)
        decay = jnp.where(valid, spread * decay, decay)
    before_ref[...] = before
    decay_ref[...] = decay
    total = own_spread * before + own_ref[:channels].astype(jnp.float32)
    for k in (3, 2, 1):
        later = place < k
        _, spread, state = received[k - 1]
        total = jnp.where(later, spread * total + state, total)
    message_ref[:channels] = total.astype(jnp.bfloat16)
    line = own_line * received[0][0] * received[1][0] * received[2][0]
    message_ref[channels:] = pack_decay(line)


def masked_heads(rows):
    lane = lax.broadcasted_iota(jnp.int32, rows.shape, 1)
    return jnp.concatenate(
        [jnp.where(lane < KEY_DIM, rows, 0.0), jnp.where(lane >= KEY_DIM, rows, 0.0)], axis=0
    ).astype(jnp.bfloat16)


def within_kernel(queries_ref, keys_ref, values_ref, running_ref, states_ref, partial_ref, reach_ref):
    length, channels = keys_ref.shape
    blocks = length // BLOCK
    pairs = channels // LANES
    lead = jnp.zeros((1, channels), jnp.float32)
    row = lax.broadcasted_iota(jnp.int32, (2 * BLOCK, BLOCK), 0)
    column = lax.broadcasted_iota(jnp.int32, (2 * BLOCK, BLOCK), 1)
    causal = (row & (BLOCK - 1)) >= column
    for n in range(blocks):
        rows = slice(n * BLOCK, (n + 1) * BLOCK)
        running = running_ref[rows]
        query_scaled = queries_ref[rows].astype(jnp.float32) * KEY_DIM ** (-0.5) * jnp.exp(running)
        key_inverse = (keys_ref[rows].astype(jnp.float32) * jnp.exp(-running)).astype(jnp.bfloat16)
        reach_ref[rows] = query_scaled * jnp.exp(lead)
        lead = lead + running[BLOCK - 1 : BLOCK]
        for p in range(pairs):
            lanes = slice(p * LANES, (p + 1) * LANES)
            masked = masked_heads(query_scaled[:, lanes])
            scores = jnp.where(causal, product(masked, key_inverse[:, lanes], 1, 1), 0.0).astype(jnp.bfloat16)
            carried = product(masked, states_ref[p, n])
            for h in range(2):
                place = slice((2 * p + h) * VALUE_DIM, (2 * p + h + 1) * VALUE_DIM)
                part = slice(h * BLOCK, (h + 1) * BLOCK)
                partial_ref[rows, place] = product(scores[part], values_ref[rows, place]) + carried[part]


def finish_kernel(
    place_ref, back1_ref, back2_ref, back3_ref, before_y_ref, decay_y_ref, before_x_ref, decay_x_ref,
    partial_ref, reach_ref, head_gain_ref, out_gate_ref, kept_ref, given_ref, whole,
):
    core = place_ref[0]
    length, channels = reach_ref.shape
    pairs = channels // LANES
    state = jnp.zeros((channels, VALUE_DIM), jnp.float32)
    for ref in (back3_ref, back2_ref, back1_ref):
        state = unpack_decay(ref)[1] * state + ref[:channels].astype(jnp.float32)
    state = before_y_ref[...] + decay_y_ref[...] * state
    state = (before_x_ref[...] + decay_x_ref[...] * state).astype(jnp.bfloat16)
    half = length // 2
    for p in range(pairs):
        lanes = slice(p * LANES, (p + 1) * LANES)
        carried = product(masked_heads(reach_ref[:, lanes]), state[lanes])
        for h in range(2):
            place = slice((2 * p + h) * VALUE_DIM, (2 * p + h + 1) * VALUE_DIM)
            attended = partial_ref[:, place] + carried[h * length : (h + 1) * length]
            scale = lax.rsqrt(jnp.mean(attended * attended, axis=1, keepdims=True) + 1e-06)
            gate = out_gate_ref[:, place].astype(jnp.float32)
            result = attended * scale * head_gain_ref[...] * (gate / (1.0 + jnp.exp(-gate)))
            result = result.astype(jnp.bfloat16)
            whole[0, :, place] = result[:half]
            whole[1, :, place] = result[half:]
    kept_ref[...] = whole[core]
    given_ref[...] = whole[1 - core]


def project_kernel(
    place_ref, owners_ref, kept_ref, taken_ref, weight_ref, residual_ref, norm_gain_ref, merged_ref, outgoing_ref,
    chunked,
):
    core = place_ref[0]
    rows, width = residual_ref.shape
    depth = kept_ref.shape[1]
    tile = 256
    own = pl.ds(pl.multiple_of(core * depth, depth), depth)
    other = pl.ds(pl.multiple_of((1 - core) * depth, depth), depth)
    square = jnp.zeros((rows, 1), jnp.float32)
    for n in range(width // tile):
        part = slice(n * tile, (n + 1) * tile)
        projected = product(kept_ref[...], weight_ref[own, part]) + product(taken_ref[...], weight_ref[other, part])
        merged = (residual_ref[:, part].astype(jnp.float32) + projected).astype(jnp.bfloat16)
        merged_ref[:, part] = merged
        widened = merged.astype(jnp.float32)
        square = square + jnp.sum(widened * widened, axis=1, keepdims=True)
    scale = lax.rsqrt(square / width + 1e-06)
    swap = swap_matrix()
    for g in range(rows // SUB):
        group = slice(g * SUB, (g + 1) * SUB)
        stacked = []
        for j in range(width // LANES):
            lanes = slice(j * LANES, (j + 1) * LANES)
            widened = merged_ref[group, lanes].astype(jnp.float32)
            stacked.append((widened * scale[group] * norm_gain_ref[:, lanes]).astype(jnp.bfloat16))
        turned = exchange(swap, jnp.concatenate(stacked, axis=0)).astype(jnp.bfloat16)
        chunked[group] = turned.reshape(SUB, SUB, LANES)

    def copy_row(slot, carry):
        outgoing_ref[slot] = chunked[owners_ref[slot]]
        return carry

    lax.fori_loop(0, outgoing_ref.shape[0], copy_row, 0, unroll=16)


def shape_of(shape, dtype):
    return jax.ShapeDtypeStruct(shape, dtype)


def limited(mebibytes):
    return pltpu.CompilerParams(vmem_limit_bytes=mebibytes << 20)


def call(kernel, name, outs, operands, scalars=0, scratch=(), cost=2000000, room=6):
    return pl.pallas_call(
        kernel,
        out_shape=outs,
        in_specs=[SMEM_SPEC] * scalars + [VMEM_SPEC] * (len(operands) - scalars),
        out_specs=jax.tree.map(lambda _: VMEM_SPEC, outs),
        scratch_shapes=list(scratch),
        cost_estimate=pl.CostEstimate(flops=cost * 400, bytes_accessed=cost, transcendentals=0),
        compiler_params=limited(room),
        name=name,
    )(*operands)


def from_behind(message, axis, wrap):
    return [
        lax.ppermute(
            message, axis, [(i, (i + k) % RING) for i in range(RING) if wrap or i + k < RING]
        )
        for k in range(1, RING)
    ]


def local(
    residual,
    queries,
    key_rows,
    value_rows,
    out_gate,
    gate_logits,
    head_gain,
    out_weight,
    norm_gain,
    routes,
    group_score,
    expert_score,
    gate_weight,
    up_weight,
    down_weight,
):
    row_count, model_width = residual.shape
    length, channels = queries.shape
    values = value_rows.shape[1]
    blocks = length // BLOCK
    pairs = channels // LANES
    f32, bf16 = jnp.float32, jnp.bfloat16
    z, y, x, core = (lax.axis_index(axis).astype(jnp.int32).reshape(1) for axis in SP_TP)
    message_shape = shape_of((channels + SUB, VALUE_DIM), bf16)
    state_shape = shape_of((channels, VALUE_DIM), f32)
    running, states, message = call(
        state_kernel,
        "local_state",
        (
            shape_of((length, channels), f32),
            shape_of((pairs, blocks, LANES, VALUE_DIM), bf16),
            message_shape,
        ),
        (key_rows, value_rows, gate_logits),
    )
    experts_total = lax.axis_size(SP_TP)
    capacity = 3 * row_count // experts_total
    slots, owners = routing(routes, experts_total, capacity)
    behind = from_behind(message, "sp_2", True)
    slots, owners, *behind = lax.optimization_barrier((slots, owners, *behind))
    before_x, decay_x, message_x = call(
        stage_kernel, "stage_x", (state_shape, state_shape, message_shape), (x, message, *behind), 1
    )
    partial, reach = call(
        within_kernel,
        "within",
        (shape_of((length, values), f32), shape_of((length, channels), f32)),
        (queries, key_rows, value_rows, running, states),
    )
    behind = from_behind(message_x, "sp_1", True)
    partial, reach, *behind = lax.optimization_barrier((partial, reach, *behind))
    before_y, decay_y, message_y = call(
        stage_kernel, "stage_y", (state_shape, state_shape, message_shape), (y, message_x, *behind), 1
    )
    behind = from_behind(message_y, "sp_0", False)
    half = shape_of((length // 2, values), bf16)
    kept, given = call(
        finish_kernel,
        "finish",
        (half, half),
        (core, *behind, before_y, decay_y, before_x, decay_x, partial, reach, head_gain.reshape(1, -1), out_gate),
        1,
        [pltpu.VMEM((2, length // 2, values), bf16)],
    )
    taken = lax.ppermute(given, "tp", [(0, 1), (1, 0)])
    merged, outgoing = call(
        project_kernel,
        "project",
        (
            shape_of((row_count, model_width), bf16),
            shape_of((experts_total * capacity, SUB, LANES), bf16),
        ),
        (core, owners, kept, taken, out_weight, residual, norm_gain.reshape(1, -1)),
        2,
        [pltpu.VMEM((row_count, SUB, LANES), bf16)],
        room=14,
    )
    block = (experts_total, capacity * SUB, LANES)
    arrived = lax.all_to_all(outgoing.reshape(block), SP_TP, split_axis=0, concat_axis=0, tiled=True)
    served = experts(arrived.reshape(outgoing.shape), gate_weight, up_weight, down_weight)
    returned = lax.all_to_all(served.reshape(block), SP_TP, split_axis=0, concat_axis=0, tiled=True)
    weights = group_score[:, None] * expert_score / jnp.sum(expert_score, axis=1, keepdims=True)
    return combine(slots, returned.reshape(outgoing.shape), merged, weights)


def solution(mesh):
    torus = Mesh(mesh.devices.reshape(4, 4, 4, mesh.shape["tp"]), ("sp_0", "sp_1", "sp_2", "tp"))
    in_specs = (
        P(SP_TP, None),
        P(SP, "tp"),
        P(SP, "tp"),
        P(SP, "tp"),
        P(SP, "tp"),
        P(SP, "tp"),
        P(),
        P(),
        P(),
        P(SP_TP, None),
        P(SP_TP),
        P(SP_TP, None),
        P(SP_TP, None, None),
        P(SP_TP, None, None),
        P(SP_TP, None, None),
    )
    out_specs = P(SP_TP, None)
    return jax.shard_map(local, mesh=torus, in_specs=in_specs, out_specs=out_specs, check_vma=False)
```

```python
import jax
import jax.numpy as jnp
from jax import lax
from jax.experimental import pallas as pl
from jax.experimental.pallas import tpu as pltpu
from jax.sharding import Mesh
from jax.sharding import PartitionSpec as P

KEY_DIM = 64
VALUE_DIM = 128
BLOCK = 64
RING = 4
SP = ("sp_0", "sp_1", "sp_2")
SP_TP = ("sp_0", "sp_1", "sp_2", "tp")


VMEM_SPEC = pl.BlockSpec(memory_space=pltpu.VMEM)
SMEM_SPEC = pl.BlockSpec(memory_space=pltpu.SMEM)
HBM_SPEC = pl.BlockSpec(memory_space=pl.ANY)
SUB = 16
LANES = 128
SWAP = SUB * SUB


def swap_matrix():
    row = lax.broadcasted_iota(jnp.int32, (SWAP, SWAP), 0)
    column = lax.broadcasted_iota(jnp.int32, (SWAP, SWAP), 1)
    partner = (row & (SUB - 1)) * SUB + (row >> 4)
    return (partner == column).astype(jnp.float32).astype(jnp.bfloat16)


def exchange(swap, blocks):
    turned = jnp.dot(swap, jnp.concatenate(blocks, axis=1), preferred_element_type=jnp.float32)
    return [turned[:, k * LANES : (k + 1) * LANES] for k in range(len(blocks))]


def stack_chunks(ref, g):
    width = ref.shape[1]
    return jnp.concatenate(
        [ref[g * SUB : (g + 1) * SUB, j * LANES : (j + 1) * LANES] for j in range(width // LANES)], axis=0
    )


def routing_kernel(routes_ref, group_ref, expert_ref, slots_ref, owners_ref, weights_ref):
    choices, rows = routes_ref.shape
    capacity = 3
    bf16 = jnp.bfloat16
    expert = lax.broadcasted_iota(jnp.int32, (LANES, rows), 0)
    token = lax.broadcasted_iota(jnp.int32, (LANES, rows), 1)
    named = [expert == routes_ref[k : k + 1] for k in range(choices)]
    named = [one.astype(jnp.float32) for one in named]
    source = lax.broadcasted_iota(jnp.int32, (rows, rows), 0)
    target = lax.broadcasted_iota(jnp.int32, (rows, rows), 1)
    before = (source < target).astype(jnp.float32).astype(bf16)
    used = jnp.dot(sum(named).astype(bf16), before, preferred_element_type=jnp.float32)
    place = lax.broadcasted_iota(jnp.int32, (8, rows), 0).astype(jnp.float32)
    name = lax.broadcasted_iota(jnp.int32, (8, rows), 1).astype(jnp.float32)
    owners = jnp.zeros((8, LANES), jnp.float32)
    for k in range(choices):
        rank = jnp.sum(named[k] * used, axis=0, keepdims=True)
        slots_ref[k : k + 1] = routes_ref[k : k + 1] * capacity + rank.astype(jnp.int32)
        owned = jnp.where(place == rank, name, 0.0).astype(bf16)
        owners = owners + lax.dot_general(
            owned, named[k].astype(bf16), (((1,), (1,)), ((), ())), preferred_element_type=jnp.float32
        )
    owners_ref[...] = owners.astype(jnp.int32)
    score = expert_ref[...]
    weights = group_ref[...] * score / jnp.sum(score, axis=0, keepdims=True)
    for k in range(choices):
        spread = jnp.broadcast_to(weights[k : k + 1], (LANES, rows))
        weights_ref[k] = spread.T


def routing(routes, group_score, expert_score):
    rows, choices = routes.shape
    return call(
        routing_kernel,
        "routing",
        (
            shape_of((choices, rows), jnp.int32),
            shape_of((8, LANES), jnp.int32),
            shape_of((choices, rows, LANES), jnp.float32),
        ),
        (routes.T, group_score.reshape(1, rows), expert_score.T),
        room=2,
    )


def experts_kernel(rows_ref, gate, up, down, out_ref, rows_in, inner, served):
    swap = swap_matrix()
    count, width = rows_in.shape
    hidden = inner.shape[1]
    groups = count // SUB
    for g in range(0, groups, 2):
        blocks = [rows_ref[k * SUB : (k + 1) * SUB].reshape(SWAP, LANES) for k in (g, g + 1)]
        for k, turned in zip((g, g + 1), exchange(swap, blocks)):
            turned = turned.astype(jnp.bfloat16)
            for j in range(width // LANES):
                rows_in[k * SUB : (k + 1) * SUB, j * LANES : (j + 1) * LANES] = turned[j * SUB : (j + 1) * SUB]
    tile = 256
    for n in range(hidden // tile):
        part = slice(n * tile, (n + 1) * tile)
        gated = jnp.dot(rows_in[...], gate[0, :, part], preferred_element_type=jnp.float32)
        lifted = jnp.dot(rows_in[...], up[0, :, part], preferred_element_type=jnp.float32)
        inner[:, part] = (gated / (1.0 + jnp.exp(-gated)) * lifted).astype(jnp.bfloat16)
    for n in range(width // tile):
        part = slice(n * tile, (n + 1) * tile)
        served[:, part] = jnp.dot(inner[...], down[0, :, part], preferred_element_type=jnp.float32).astype(jnp.bfloat16)
    for g in range(0, groups, 2):
        blocks = [stack_chunks(served, k) for k in (g, g + 1)]
        for k, turned in zip((g, g + 1), exchange(swap, blocks)):
            out_ref[k * SUB : (k + 1) * SUB] = turned.astype(jnp.bfloat16).reshape(SUB, SUB, LANES)


def experts(arrived, gate_weight, up_weight, down_weight):
    count = arrived.shape[0]
    width, hidden = gate_weight.shape[1:]
    return pl.pallas_call(
        experts_kernel,
        out_shape=jax.ShapeDtypeStruct(arrived.shape, jnp.bfloat16),
        in_specs=[VMEM_SPEC] * 4,
        out_specs=VMEM_SPEC,
        scratch_shapes=[
            pltpu.VMEM((count, width), jnp.bfloat16),
            pltpu.VMEM((count, hidden), jnp.bfloat16),
            pltpu.VMEM((count, width), jnp.bfloat16),
        ],
        compiler_params=limited(16),
        name="experts",
    )(arrived, gate_weight, up_weight, down_weight)


def combine_kernel(slots_ref, returned_ref, merged_ref, weights_ref, out_ref, picked):
    swap = swap_matrix()
    rows, width = merged_ref.shape

    def copy_row(i, carry):
        picked[0, i] = returned_ref[slots_ref[0, i]]
        picked[1, i] = returned_ref[slots_ref[1, i]]
        return carry

    lax.fori_loop(0, rows, copy_row, 0, unroll=8)
    for g in range(rows // SUB):
        group = slice(g * SUB, (g + 1) * SUB)
        first, second = exchange(swap, [picked[k, group].reshape(SWAP, LANES) for k in range(2)])
        for j in range(width // LANES):
            lanes = slice(j * LANES, (j + 1) * LANES)
            part = slice(j * SUB, (j + 1) * SUB)
            total = weights_ref[0, group] * first[part] + weights_ref[1, group] * second[part]
            out_ref[group, lanes] = (merged_ref[group, lanes].astype(jnp.float32) + total).astype(jnp.bfloat16)


def combine(slots, returned, merged, weights):
    rows = merged.shape[0]
    return call(
        combine_kernel,
        "combine",
        shape_of(merged.shape, jnp.bfloat16),
        (slots, returned, merged, weights),
        1,
        [pltpu.VMEM((2, rows, SUB, LANES), jnp.bfloat16)],
        room=8,
    )


def pieces(value, count):
    parts = []
    for _ in range(count):
        part = value.astype(jnp.bfloat16)
        parts.append(part)
        value = value - part.astype(jnp.float32)
    return parts


def product(left, right, left_dim=1, right_dim=0):
    return lax.dot_general(
        left, right, (((left_dim,), (right_dim,)), ((), ())), preferred_element_type=jnp.float32
    )


def state_kernel(keys_hbm, values_hbm, logits_hbm, running_ref, states_ref, message_ref, keys_ref, values_ref, logits_ref, sems):
    copies = [
        pltpu.make_async_copy(source, target, sems.at[k])
        for k, (source, target) in enumerate(
            ((logits_hbm, logits_ref), (keys_hbm, keys_ref), (values_hbm, values_ref))
        )
    ]
    for copy in copies:
        copy.start()
    copies[0].wait()
    length, channels = keys_ref.shape
    blocks = length // BLOCK
    pairs = channels // LANES
    wide = 2 * VALUE_DIM
    logits = logits_ref[...].astype(jnp.float32)
    decay_log = (jnp.minimum(logits, 0.0) - jnp.log1p(jnp.exp(-jnp.abs(logits)))) / 16.0
    parts = pieces(decay_log, 3)
    row = lax.broadcasted_iota(jnp.int32, (length, length), 0)
    column = lax.broadcasted_iota(jnp.int32, (length, length), 1)
    earlier = (row >= column) & (row // BLOCK == column // BLOCK)
    earlier = earlier.astype(jnp.float32).astype(jnp.bfloat16)
    running = sum(product(earlier, part) for part in parts)
    running_ref[...] = running
    token = lax.broadcasted_iota(jnp.int32, (length, blocks * LANES), 0)
    lane = lax.broadcasted_iota(jnp.int32, (length, blocks * LANES), 1)
    member = (token // BLOCK == lane // LANES).astype(jnp.float32).astype(jnp.bfloat16)
    block_decay = jnp.exp(sum(product(part, member, 0, 0) for part in parts))
    copies[1].wait()
    copies[2].wait()
    states = [jnp.zeros((LANES, VALUE_DIM), jnp.float32)] * pairs
    total = jnp.zeros((1, channels), jnp.float32)
    for n in range(blocks):
        rows = slice(n * BLOCK, (n + 1) * BLOCK)
        closing = running[(n + 1) * BLOCK - 1 : (n + 1) * BLOCK]
        total = total + closing
        key_closing = keys_ref[rows].astype(jnp.float32) * jnp.exp(closing - running[rows])
        key_closing = key_closing.astype(jnp.bfloat16)
        for p in range(pairs):
            states_ref[p, n] = states[p].astype(jnp.bfloat16)
            grown = product(
                key_closing[:, p * LANES : (p + 1) * LANES], values_ref[rows, p * wide : (p + 1) * wide], 0, 0
            )
            grown = jnp.concatenate([grown[:KEY_DIM, :VALUE_DIM], grown[KEY_DIM:, VALUE_DIM:]], axis=0)
            decay = block_decay[p * LANES : (p + 1) * LANES, n * LANES : (n + 1) * LANES]
            states[p] = decay * states[p] + grown
    for p in range(pairs):
        message_ref[p * LANES : (p + 1) * LANES] = states[p].astype(jnp.bfloat16)
    message_ref[channels:] = pack_decay(jnp.exp(total))


def pack_decay(decay):
    pairs = decay.shape[1] // LANES
    place = lax.broadcasted_iota(jnp.int32, (SUB, LANES), 0)
    high, low = pieces(decay, 2)
    packed = jnp.zeros((SUB, LANES), jnp.float32)
    for p in range(pairs):
        lanes = slice(p * LANES, (p + 1) * LANES)
        packed = jnp.where(place == p, high[:, lanes].astype(jnp.float32), packed)
        packed = jnp.where(place == pairs + p, low[:, lanes].astype(jnp.float32), packed)
    return packed.astype(jnp.bfloat16)


def unpack_decay(message_ref):
    channels = message_ref.shape[0] - SUB
    pairs = channels // LANES
    packed = message_ref[channels:].astype(jnp.float32)
    diagonal = lax.broadcasted_iota(jnp.int32, (LANES, LANES), 0) == lax.broadcasted_iota(
        jnp.int32, (LANES, LANES), 1
    )
    ones = jnp.ones((LANES, VALUE_DIM), jnp.bfloat16)
    spread = []
    for p in range(pairs):
        both = [jnp.where(diagonal, packed[k : k + 1], 0.0).astype(jnp.bfloat16) for k in (p, pairs + p)]
        spread.append(product(both[0], ones) + product(both[1], ones))
    line = jnp.concatenate([packed[p : p + 1] + packed[pairs + p : pairs + p + 1] for p in range(pairs)], axis=1)
    return line, jnp.concatenate(spread, axis=0)


def stage_kernel(place_ref, own_ref, back1_ref, back2_ref, back3_ref, before_ref, decay_ref, message_ref):
    place = place_ref[0]
    channels = own_ref.shape[0] - SUB
    received = []
    for ref in (back1_ref, back2_ref, back3_ref):
        line, spread = unpack_decay(ref)
        received.append((line, spread, ref[:channels].astype(jnp.float32)))
    own_line, own_spread = unpack_decay(own_ref)
    before = jnp.zeros((channels, VALUE_DIM), jnp.float32)
    decay = jnp.ones((channels, VALUE_DIM), jnp.float32)
    for k in (3, 2, 1):
        valid = place >= k
        _, spread, state = received[k - 1]
        before = jnp.where(valid, spread * before + state, before)
        decay = jnp.where(valid, spread * decay, decay)
    before_ref[...] = before
    decay_ref[...] = decay
    total = own_spread * before + own_ref[:channels].astype(jnp.float32)
    for k in (3, 2, 1):
        later = place < k
        _, spread, state = received[k - 1]
        total = jnp.where(later, spread * total + state, total)
    message_ref[:channels] = total.astype(jnp.bfloat16)
    line = own_line * received[0][0] * received[1][0] * received[2][0]
    message_ref[channels:] = pack_decay(line)


def masked_heads(rows):
    lane = lax.broadcasted_iota(jnp.int32, rows.shape, 1)
    return jnp.concatenate(
        [jnp.where(lane < KEY_DIM, rows, 0.0), jnp.where(lane >= KEY_DIM, rows, 0.0)], axis=0
    ).astype(jnp.bfloat16)


def within_kernel(queries_ref, keys_ref, values_ref, running_ref, states_ref, partial_ref, reach_ref):
    length, channels = keys_ref.shape
    blocks = length // BLOCK
    pairs = channels // LANES
    lead = jnp.zeros((1, channels), jnp.float32)
    row = lax.broadcasted_iota(jnp.int32, (2 * BLOCK, BLOCK), 0)
    column = lax.broadcasted_iota(jnp.int32, (2 * BLOCK, BLOCK), 1)
    causal = (row & (BLOCK - 1)) >= column
    for n in range(blocks):
        rows = slice(n * BLOCK, (n + 1) * BLOCK)
        running = running_ref[rows]
        query_scaled = queries_ref[rows].astype(jnp.float32) * KEY_DIM ** (-0.5) * jnp.exp(running)
        key_inverse = (keys_ref[rows].astype(jnp.float32) * jnp.exp(-running)).astype(jnp.bfloat16)
        reach_ref[rows] = query_scaled * jnp.exp(lead)
        lead = lead + running[BLOCK - 1 : BLOCK]
        for p in range(pairs):
            lanes = slice(p * LANES, (p + 1) * LANES)
            masked = masked_heads(query_scaled[:, lanes])
            scores = jnp.where(causal, product(masked, key_inverse[:, lanes], 1, 1), 0.0).astype(jnp.bfloat16)
            carried = product(masked, states_ref[p, n])
            for h in range(2):
                place = slice((2 * p + h) * VALUE_DIM, (2 * p + h + 1) * VALUE_DIM)
                part = slice(h * BLOCK, (h + 1) * BLOCK)
                partial_ref[rows, place] = product(scores[part], values_ref[rows, place]) + carried[part]


def finish_kernel(
    place_ref, back1_ref, back2_ref, back3_ref, before_y_ref, decay_y_ref, before_x_ref, decay_x_ref,
    partial_ref, reach_ref, head_gain_ref, out_gate_ref, kept_ref, given_ref, whole,
):
    core = place_ref[0]
    length, channels = reach_ref.shape
    pairs = channels // LANES
    state = jnp.zeros((channels, VALUE_DIM), jnp.float32)
    for ref in (back3_ref, back2_ref, back1_ref):
        state = unpack_decay(ref)[1] * state + ref[:channels].astype(jnp.float32)
    state = before_y_ref[...] + decay_y_ref[...] * state
    state = (before_x_ref[...] + decay_x_ref[...] * state).astype(jnp.bfloat16)
    half = length // 2
    for p in range(pairs):
        lanes = slice(p * LANES, (p + 1) * LANES)
        carried = product(masked_heads(reach_ref[:, lanes]), state[lanes])
        for h in range(2):
            place = slice((2 * p + h) * VALUE_DIM, (2 * p + h + 1) * VALUE_DIM)
            attended = partial_ref[:, place] + carried[h * length : (h + 1) * length]
            scale = lax.rsqrt(jnp.mean(attended * attended, axis=1, keepdims=True) + 1e-06)
            gate = out_gate_ref[:, place].astype(jnp.float32)
            result = attended * scale * head_gain_ref[...] * (gate / (1.0 + jnp.exp(-gate)))
            result = result.astype(jnp.bfloat16)
            whole[0, :, place] = result[:half]
            whole[1, :, place] = result[half:]
    kept_ref[...] = whole[core]
    given_ref[...] = whole[1 - core]


def project_kernel(
    place_ref, owners_ref, kept_ref, taken_ref, weight_ref, residual_ref, norm_gain_ref, merged_ref, outgoing_ref,
    chunked,
):
    core = place_ref[0]
    rows, width = residual_ref.shape
    depth = kept_ref.shape[1]
    tile = 256
    own = pl.ds(pl.multiple_of(core * depth, depth), depth)
    other = pl.ds(pl.multiple_of((1 - core) * depth, depth), depth)
    square = jnp.zeros((rows, 1), jnp.float32)
    for n in range(width // tile):
        part = slice(n * tile, (n + 1) * tile)
        projected = product(kept_ref[...], weight_ref[own, part]) + product(taken_ref[...], weight_ref[other, part])
        merged = (residual_ref[:, part].astype(jnp.float32) + projected).astype(jnp.bfloat16)
        merged_ref[:, part] = merged
        widened = merged.astype(jnp.float32)
        square = square + jnp.sum(widened * widened, axis=1, keepdims=True)
    scale = lax.rsqrt(square / width + 1e-06)
    swap = swap_matrix()
    for g in range(0, rows // SUB, 2):
        blocks = []
        for k in (g, g + 1):
            group = slice(k * SUB, (k + 1) * SUB)
            stacked = []
            for j in range(width // LANES):
                lanes = slice(j * LANES, (j + 1) * LANES)
                widened = merged_ref[group, lanes].astype(jnp.float32)
                stacked.append((widened * scale[group] * norm_gain_ref[:, lanes]).astype(jnp.bfloat16))
            blocks.append(jnp.concatenate(stacked, axis=0))
        for k, turned in zip((g, g + 1), exchange(swap, blocks)):
            chunked[k * SUB : (k + 1) * SUB] = turned.astype(jnp.bfloat16).reshape(SUB, SUB, LANES)

    experts_total = owners_ref.shape[1]
    capacity = outgoing_ref.shape[0] // experts_total

    def copy_rows(expert, carry):
        for place in range(capacity):
            outgoing_ref[capacity * expert + place] = chunked[owners_ref[place, expert]]
        return carry

    lax.fori_loop(0, experts_total, copy_rows, 0, unroll=8)


def shape_of(shape, dtype):
    return jax.ShapeDtypeStruct(shape, dtype)


def limited(mebibytes):
    return pltpu.CompilerParams(vmem_limit_bytes=int(mebibytes * 1048576))


def call(kernel, name, outs, operands, scalars=0, scratch=(), cost=10000000, room=6, far=False):
    return pl.pallas_call(
        kernel,
        out_shape=outs,
        in_specs=[SMEM_SPEC] * scalars + [HBM_SPEC if far else VMEM_SPEC] * (len(operands) - scalars),
        out_specs=jax.tree.map(lambda _: VMEM_SPEC, outs),
        scratch_shapes=list(scratch),
        cost_estimate=pl.CostEstimate(flops=cost * 400, bytes_accessed=cost, transcendentals=0),
        compiler_params=limited(room),
        name=name,
    )(*operands)


def from_behind(message, axis, wrap):
    return [
        lax.ppermute(
            message, axis, [(i, (i + k) % RING) for i in range(RING) if wrap or i + k < RING]
        )
        for k in range(1, RING)
    ]


def local(
    residual,
    queries,
    key_rows,
    value_rows,
    out_gate,
    gate_logits,
    head_gain,
    out_weight,
    norm_gain,
    routes,
    group_score,
    expert_score,
    gate_weight,
    up_weight,
    down_weight,
):
    row_count, model_width = residual.shape
    length, channels = queries.shape
    values = value_rows.shape[1]
    blocks = length // BLOCK
    pairs = channels // LANES
    f32, bf16 = jnp.float32, jnp.bfloat16
    z, y, x, core = (lax.axis_index(axis).astype(jnp.int32).reshape(1) for axis in SP_TP)
    message_shape = shape_of((channels + SUB, VALUE_DIM), bf16)
    state_shape = shape_of((channels, VALUE_DIM), f32)
    running, states, message = call(
        state_kernel,
        "local_state",
        (
            shape_of((length, channels), f32),
            shape_of((pairs, blocks, LANES, VALUE_DIM), bf16),
            message_shape,
        ),
        (key_rows, value_rows, gate_logits),
        scratch=[
            pltpu.VMEM(key_rows.shape, bf16),
            pltpu.VMEM(value_rows.shape, bf16),
            pltpu.VMEM(gate_logits.shape, bf16),
            pltpu.SemaphoreType.DMA((3,)),
        ],
        room=53.8,
        far=True,
    )
    experts_total = lax.axis_size(SP_TP)
    capacity = 3 * row_count // experts_total
    slots, owners, weights = routing(routes, group_score, expert_score)
    behind = from_behind(message, "sp_2", True)
    slots, owners, weights, *behind = lax.optimization_barrier((slots, owners, weights, *behind))
    before_x, decay_x, message_x = call(
        stage_kernel, "stage_x", (state_shape, state_shape, message_shape), (x, message, *behind), 1
    )
    partial, reach = call(
        within_kernel,
        "within",
        (shape_of((length, values), f32), shape_of((length, channels), f32)),
        (queries, key_rows, value_rows, running, states),
    )
    behind = from_behind(message_x, "sp_1", True)
    partial, reach, *behind = lax.optimization_barrier((partial, reach, *behind))
    before_y, decay_y, message_y = call(
        stage_kernel, "stage_y", (state_shape, state_shape, message_shape), (y, message_x, *behind), 1
    )
    behind = from_behind(message_y, "sp_0", False)
    half = shape_of((length // 2, values), bf16)
    kept, given = call(
        finish_kernel,
        "finish",
        (half, half),
        (core, *behind, before_y, decay_y, before_x, decay_x, partial, reach, head_gain.reshape(1, -1), out_gate),
        1,
        [pltpu.VMEM((2, length // 2, values), bf16)],
    )
    taken = lax.ppermute(given, "tp", [(0, 1), (1, 0)])
    merged, outgoing = call(
        project_kernel,
        "project",
        (
            shape_of((row_count, model_width), bf16),
            shape_of((experts_total * capacity, SUB, LANES), bf16),
        ),
        (core, owners, kept, taken, out_weight, residual, norm_gain.reshape(1, -1)),
        2,
        [pltpu.VMEM((row_count, SUB, LANES), bf16)],
        room=14,
    )
    block = (experts_total, capacity * SUB, LANES)
    arrived = lax.all_to_all(outgoing.reshape(block), SP_TP, split_axis=0, concat_axis=0, tiled=True)
    served = experts(arrived.reshape(outgoing.shape), gate_weight, up_weight, down_weight)
    returned = lax.all_to_all(served.reshape(block), SP_TP, split_axis=0, concat_axis=0, tiled=True)
    return combine(slots, returned.reshape(outgoing.shape), merged, weights)


def solution(mesh):
    torus = Mesh(mesh.devices.reshape(4, 4, 4, mesh.shape["tp"]), ("sp_0", "sp_1", "sp_2", "tp"))
    in_specs = (
        P(SP_TP, None),
        P(SP, "tp"),
        P(SP, "tp"),
        P(SP, "tp"),
        P(SP, "tp"),
        P(SP, "tp"),
        P(),
        P(),
        P(),
        P(SP_TP, None),
        P(SP_TP),
        P(SP_TP, None),
        P(SP_TP, None, None),
        P(SP_TP, None, None),
        P(SP_TP, None, None),
    )
    out_specs = P(SP_TP, None)
    return jax.shard_map(local, mesh=torus, in_specs=in_specs, out_specs=out_specs, check_vma=False)
```

```python
import jax
import jax.numpy as jnp
from jax import lax
from jax.experimental import pallas as pl
from jax.experimental.pallas import tpu as pltpu
from jax.sharding import Mesh
from jax.sharding import PartitionSpec as P

KEY_DIM = 64
VALUE_DIM = 128
BLOCK = 64
RING = 4
SP = ("sp_0", "sp_1", "sp_2")
SP_TP = ("sp_0", "sp_1", "sp_2", "tp")


VMEM_SPEC = pl.BlockSpec(memory_space=pltpu.VMEM)
SMEM_SPEC = pl.BlockSpec(memory_space=pltpu.SMEM)
HBM_SPEC = pl.BlockSpec(memory_space=pl.ANY)
SUB = 16
LANES = 128
SWAP = SUB * SUB


def swap_matrix():
    row = lax.broadcasted_iota(jnp.int32, (SWAP, SWAP), 0)
    column = lax.broadcasted_iota(jnp.int32, (SWAP, SWAP), 1)
    partner = (row & (SUB - 1)) * SUB + (row >> 4)
    return (partner == column).astype(jnp.float32).astype(jnp.bfloat16)


def exchange(swap, blocks):
    turned = jnp.dot(swap, jnp.concatenate(blocks, axis=1), preferred_element_type=jnp.float32)
    return [turned[:, k * LANES : (k + 1) * LANES] for k in range(len(blocks))]


def stack_chunks(ref, g):
    width = ref.shape[1]
    return jnp.concatenate(
        [ref[g * SUB : (g + 1) * SUB, j * LANES : (j + 1) * LANES] for j in range(width // LANES)], axis=0
    )


def routing_kernel(routes_ref, group_ref, expert_ref, slots_ref, owners_ref, weights_ref):
    choices, rows = routes_ref.shape
    capacity = 3
    bf16 = jnp.bfloat16
    expert = lax.broadcasted_iota(jnp.int32, (LANES, rows), 0)
    token = lax.broadcasted_iota(jnp.int32, (LANES, rows), 1)
    named = [expert == routes_ref[k : k + 1] for k in range(choices)]
    named = [one.astype(jnp.float32) for one in named]
    source = lax.broadcasted_iota(jnp.int32, (rows, rows), 0)
    target = lax.broadcasted_iota(jnp.int32, (rows, rows), 1)
    before = (source < target).astype(jnp.float32).astype(bf16)
    used = jnp.dot(sum(named).astype(bf16), before, preferred_element_type=jnp.float32)
    place = lax.broadcasted_iota(jnp.int32, (8, rows), 0).astype(jnp.float32)
    name = lax.broadcasted_iota(jnp.int32, (8, rows), 1).astype(jnp.float32)
    owners = jnp.zeros((8, LANES), jnp.float32)
    for k in range(choices):
        rank = jnp.sum(named[k] * used, axis=0, keepdims=True)
        slots_ref[k : k + 1] = routes_ref[k : k + 1] * capacity + rank.astype(jnp.int32)
        owned = jnp.where(place == rank, name, 0.0).astype(bf16)
        owners = owners + lax.dot_general(
            owned, named[k].astype(bf16), (((1,), (1,)), ((), ())), preferred_element_type=jnp.float32
        )
    owners_ref[...] = owners.astype(jnp.int32)
    score = expert_ref[...]
    weights = group_ref[...] * score / jnp.sum(score, axis=0, keepdims=True)
    for k in range(choices):
        spread = jnp.broadcast_to(weights[k : k + 1], (LANES, rows))
        weights_ref[k] = spread.T


def routing(routes, group_score, expert_score):
    rows, choices = routes.shape
    return call(
        routing_kernel,
        (
            shape_of((choices, rows), jnp.int32),
            shape_of((8, LANES), jnp.int32),
            shape_of((choices, rows, LANES), jnp.float32),
        ),
        (routes.T, group_score.reshape(1, rows), expert_score.T),
        room=2,
    )


def experts_kernel(rows_ref, gate, up, down, out_ref, rows_in, inner, served):
    swap = swap_matrix()
    count, width = rows_in.shape
    hidden = inner.shape[1]
    groups = count // SUB
    for g in range(0, groups, 2):
        blocks = [rows_ref[k * SUB : (k + 1) * SUB].reshape(SWAP, LANES) for k in (g, g + 1)]
        for k, turned in zip((g, g + 1), exchange(swap, blocks)):
            turned = turned.astype(jnp.bfloat16)
            for j in range(width // LANES):
                rows_in[k * SUB : (k + 1) * SUB, j * LANES : (j + 1) * LANES] = turned[j * SUB : (j + 1) * SUB]
    tile = 256
    for n in range(hidden // tile):
        part = slice(n * tile, (n + 1) * tile)
        gated = jnp.dot(rows_in[...], gate[0, :, part], preferred_element_type=jnp.float32)
        lifted = jnp.dot(rows_in[...], up[0, :, part], preferred_element_type=jnp.float32)
        inner[:, part] = (gated / (1.0 + jnp.exp(-gated)) * lifted).astype(jnp.bfloat16)
    for n in range(width // tile):
        part = slice(n * tile, (n + 1) * tile)
        served[:, part] = jnp.dot(inner[...], down[0, :, part], preferred_element_type=jnp.float32).astype(jnp.bfloat16)
    for g in range(0, groups, 2):
        blocks = [stack_chunks(served, k) for k in (g, g + 1)]
        for k, turned in zip((g, g + 1), exchange(swap, blocks)):
            out_ref[k * SUB : (k + 1) * SUB] = turned.astype(jnp.bfloat16).reshape(SUB, SUB, LANES)


def experts(arrived, gate_weight, up_weight, down_weight):
    count = arrived.shape[0]
    width, hidden = gate_weight.shape[1:]
    return pl.pallas_call(
        experts_kernel,
        out_shape=jax.ShapeDtypeStruct(arrived.shape, jnp.bfloat16),
        in_specs=[VMEM_SPEC] * 4,
        out_specs=VMEM_SPEC,
        scratch_shapes=[
            pltpu.VMEM((count, width), jnp.bfloat16),
            pltpu.VMEM((count, hidden), jnp.bfloat16),
            pltpu.VMEM((count, width), jnp.bfloat16),
        ],
        compiler_params=limited(16),
        name="experts",
    )(arrived, gate_weight, up_weight, down_weight)


def combine_kernel(slots_ref, returned_ref, merged_ref, weights_ref, out_ref, picked):
    swap = swap_matrix()
    rows, width = merged_ref.shape

    def copy_row(i, carry):
        picked[0, i] = returned_ref[slots_ref[0, i]]
        picked[1, i] = returned_ref[slots_ref[1, i]]
        return carry

    lax.fori_loop(0, rows, copy_row, 0, unroll=8)
    for g in range(rows // SUB):
        group = slice(g * SUB, (g + 1) * SUB)
        first, second = exchange(swap, [picked[k, group].reshape(SWAP, LANES) for k in range(2)])
        for j in range(width // LANES):
            lanes = slice(j * LANES, (j + 1) * LANES)
            part = slice(j * SUB, (j + 1) * SUB)
            total = weights_ref[0, group] * first[part] + weights_ref[1, group] * second[part]
            out_ref[group, lanes] = (merged_ref[group, lanes].astype(jnp.float32) + total).astype(jnp.bfloat16)


def combine(slots, returned, merged, weights):
    rows = merged.shape[0]
    return call(
        combine_kernel,
        shape_of(merged.shape, jnp.bfloat16),
        (slots, returned, merged, weights),
        1,
        [pltpu.VMEM((2, rows, SUB, LANES), jnp.bfloat16)],
        room=8,
    )


def pieces(value, count):
    parts = []
    for _ in range(count):
        part = value.astype(jnp.bfloat16)
        parts.append(part)
        value = value - part.astype(jnp.float32)
    return parts


def product(left, right, left_dim=1, right_dim=0):
    return lax.dot_general(
        left, right, (((left_dim,), (right_dim,)), ((), ())), preferred_element_type=jnp.float32
    )


def running_sums(logits):
    length = logits.shape[0]
    blocks = length // BLOCK
    decay_log = (jnp.minimum(logits, 0.0) - jnp.log1p(jnp.exp(-jnp.abs(logits)))) / 16.0
    parts = pieces(decay_log, 3)
    row = lax.broadcasted_iota(jnp.int32, (length, length), 0)
    column = lax.broadcasted_iota(jnp.int32, (length, length), 1)
    earlier = (row >= column) & (row // BLOCK == column // BLOCK)
    earlier = earlier.astype(jnp.float32).astype(jnp.bfloat16)
    running = sum(product(earlier, part) for part in parts)
    token = lax.broadcasted_iota(jnp.int32, (length, blocks * LANES), 0)
    lane = lax.broadcasted_iota(jnp.int32, (length, blocks * LANES), 1)
    member = (token // BLOCK == lane // LANES).astype(jnp.float32).astype(jnp.bfloat16)
    block_decay = jnp.exp(sum(product(part, member, 0, 0) for part in parts))
    return running, block_decay


def grow(states, n, running, block_decay, keys_ref, values_ref):
    wide = 2 * VALUE_DIM
    rows = slice(n * BLOCK, (n + 1) * BLOCK)
    closing = running[(n + 1) * BLOCK - 1 : (n + 1) * BLOCK]
    key_closing = keys_ref[rows].astype(jnp.float32) * jnp.exp(closing - running[rows])
    key_closing = key_closing.astype(jnp.bfloat16)
    after = []
    for p, state in enumerate(states):
        lanes = slice(p * LANES, (p + 1) * LANES)
        grown = product(key_closing[:, lanes], values_ref[rows, p * wide : (p + 1) * wide], 0, 0)
        grown = jnp.concatenate([grown[:KEY_DIM, :VALUE_DIM], grown[KEY_DIM:, VALUE_DIM:]], axis=0)
        after.append(block_decay[lanes, n * LANES : (n + 1) * LANES] * state + grown)
    return after


def state_kernel(keys_hbm, values_hbm, logits_hbm, message_ref, keys_ref, values_ref, logits_ref, sems):
    copies = [
        pltpu.make_async_copy(source, target, sems.at[k])
        for k, (source, target) in enumerate(
            ((logits_hbm, logits_ref), (keys_hbm, keys_ref), (values_hbm, values_ref))
        )
    ]
    for copy in copies:
        copy.start()
    copies[0].wait()
    length, channels = keys_ref.shape
    blocks = length // BLOCK
    pairs = channels // LANES
    running, block_decay = running_sums(logits_ref[...].astype(jnp.float32))
    copies[1].wait()
    copies[2].wait()
    states = [jnp.zeros((LANES, VALUE_DIM), jnp.float32)] * pairs
    total = jnp.zeros((1, channels), jnp.float32)
    for n in range(blocks):
        total = total + running[(n + 1) * BLOCK - 1 : (n + 1) * BLOCK]
        states = grow(states, n, running, block_decay, keys_ref, values_ref)
    for p in range(pairs):
        message_ref[p * LANES : (p + 1) * LANES] = states[p].astype(jnp.bfloat16)
    message_ref[channels:] = pack_decay(jnp.exp(total))


def pack_decay(decay):
    pairs = decay.shape[1] // LANES
    place = lax.broadcasted_iota(jnp.int32, (SUB, LANES), 0)
    high, low = pieces(decay, 2)
    packed = jnp.zeros((SUB, LANES), jnp.float32)
    for p in range(pairs):
        lanes = slice(p * LANES, (p + 1) * LANES)
        packed = jnp.where(place == p, high[:, lanes].astype(jnp.float32), packed)
        packed = jnp.where(place == pairs + p, low[:, lanes].astype(jnp.float32), packed)
    return packed.astype(jnp.bfloat16)


def unpack_decay(message_ref):
    channels = message_ref.shape[0] - SUB
    pairs = channels // LANES
    packed = message_ref[channels:].astype(jnp.float32)
    diagonal = lax.broadcasted_iota(jnp.int32, (LANES, LANES), 0) == lax.broadcasted_iota(
        jnp.int32, (LANES, LANES), 1
    )
    ones = jnp.ones((LANES, VALUE_DIM), jnp.bfloat16)
    spread = []
    for p in range(pairs):
        both = [jnp.where(diagonal, packed[k : k + 1], 0.0).astype(jnp.bfloat16) for k in (p, pairs + p)]
        spread.append(product(both[0], ones) + product(both[1], ones))
    line = jnp.concatenate([packed[p : p + 1] + packed[pairs + p : pairs + p + 1] for p in range(pairs)], axis=1)
    return line, jnp.concatenate(spread, axis=0)


def stage_kernel(place_ref, own_ref, back1_ref, back2_ref, back3_ref, before_ref, decay_ref, message_ref):
    place = place_ref[0]
    channels = own_ref.shape[0] - SUB
    received = []
    for ref in (back1_ref, back2_ref, back3_ref):
        line, spread = unpack_decay(ref)
        received.append((line, spread, ref[:channels].astype(jnp.float32)))
    own_line, own_spread = unpack_decay(own_ref)
    before = jnp.zeros((channels, VALUE_DIM), jnp.float32)
    decay = jnp.ones((channels, VALUE_DIM), jnp.float32)
    for k in (3, 2, 1):
        valid = place >= k
        _, spread, state = received[k - 1]
        before = jnp.where(valid, spread * before + state, before)
        decay = jnp.where(valid, spread * decay, decay)
    before_ref[...] = before
    decay_ref[...] = decay
    total = own_spread * before + own_ref[:channels].astype(jnp.float32)
    for k in (3, 2, 1):
        later = place < k
        _, spread, state = received[k - 1]
        total = jnp.where(later, spread * total + state, total)
    message_ref[:channels] = total.astype(jnp.bfloat16)
    line = own_line * received[0][0] * received[1][0] * received[2][0]
    message_ref[channels:] = pack_decay(line)


def masked_heads(rows):
    lane = lax.broadcasted_iota(jnp.int32, rows.shape, 1)
    return jnp.concatenate(
        [jnp.where(lane < KEY_DIM, rows, 0.0), jnp.where(lane >= KEY_DIM, rows, 0.0)], axis=0
    ).astype(jnp.bfloat16)


def within_kernel(queries_ref, keys_ref, values_ref, logits_ref, partial_ref, reach_ref):
    length, channels = keys_ref.shape
    blocks = length // BLOCK
    pairs = channels // LANES
    running_all, block_decay = running_sums(logits_ref[...].astype(jnp.float32))
    states = [jnp.zeros((LANES, VALUE_DIM), jnp.float32)] * pairs
    lead = jnp.zeros((1, channels), jnp.float32)
    row = lax.broadcasted_iota(jnp.int32, (2 * BLOCK, BLOCK), 0)
    column = lax.broadcasted_iota(jnp.int32, (2 * BLOCK, BLOCK), 1)
    causal = (row & (BLOCK - 1)) >= column
    for n in range(blocks):
        rows = slice(n * BLOCK, (n + 1) * BLOCK)
        running = running_all[rows]
        query_scaled = queries_ref[rows].astype(jnp.float32) * KEY_DIM ** (-0.5) * jnp.exp(running)
        key_inverse = (keys_ref[rows].astype(jnp.float32) * jnp.exp(-running)).astype(jnp.bfloat16)
        reach_ref[rows] = query_scaled * jnp.exp(lead)
        lead = lead + running[BLOCK - 1 : BLOCK]
        for p in range(pairs):
            lanes = slice(p * LANES, (p + 1) * LANES)
            masked = masked_heads(query_scaled[:, lanes])
            scores = jnp.where(causal, product(masked, key_inverse[:, lanes], 1, 1), 0.0).astype(jnp.bfloat16)
            carried = product(masked, states[p].astype(jnp.bfloat16))
            for h in range(2):
                place = slice((2 * p + h) * VALUE_DIM, (2 * p + h + 1) * VALUE_DIM)
                part = slice(h * BLOCK, (h + 1) * BLOCK)
                partial_ref[rows, place] = product(scores[part], values_ref[rows, place]) + carried[part]
        if n + 1 < blocks:
            states = grow(states, n, running_all, block_decay, keys_ref, values_ref)


def finish_kernel(
    place_ref, back1_ref, back2_ref, back3_ref, before_y_ref, decay_y_ref, before_x_ref, decay_x_ref,
    partial_ref, reach_ref, head_gain_ref, out_gate_ref, kept_ref, given_ref, whole,
):
    core, plane = place_ref[0], place_ref[1]
    length, channels = reach_ref.shape
    pairs = channels // LANES
    state = jnp.zeros((channels, VALUE_DIM), jnp.float32)
    for k, ref in ((3, back3_ref), (2, back2_ref), (1, back1_ref)):
        passed = unpack_decay(ref)[1] * state + ref[:channels].astype(jnp.float32)
        state = jnp.where(plane >= k, passed, state)
    state = before_y_ref[...] + decay_y_ref[...] * state
    state = (before_x_ref[...] + decay_x_ref[...] * state).astype(jnp.bfloat16)
    half = length // 2
    for p in range(pairs):
        lanes = slice(p * LANES, (p + 1) * LANES)
        carried = product(masked_heads(reach_ref[:, lanes]), state[lanes])
        for h in range(2):
            place = slice((2 * p + h) * VALUE_DIM, (2 * p + h + 1) * VALUE_DIM)
            attended = partial_ref[:, place] + carried[h * length : (h + 1) * length]
            scale = lax.rsqrt(jnp.mean(attended * attended, axis=1, keepdims=True) + 1e-06)
            gate = out_gate_ref[:, place].astype(jnp.float32)
            result = attended * scale * head_gain_ref[...] * (gate / (1.0 + jnp.exp(-gate)))
            result = result.astype(jnp.bfloat16)
            whole[0, :, place] = result[:half]
            whole[1, :, place] = result[half:]
    kept_ref[...] = whole[core]
    given_ref[...] = whole[1 - core]


def project_kernel(
    place_ref, owners_ref, kept_ref, taken_ref, weight_ref, residual_ref, norm_gain_ref, merged_ref, outgoing_ref,
    chunked,
):
    core = place_ref[0]
    rows, width = residual_ref.shape
    depth = kept_ref.shape[1]
    tile = 256
    own = pl.ds(pl.multiple_of(core * depth, depth), depth)
    other = pl.ds(pl.multiple_of((1 - core) * depth, depth), depth)
    square = jnp.zeros((rows, 1), jnp.float32)
    for n in range(width // tile):
        part = slice(n * tile, (n + 1) * tile)
        projected = product(kept_ref[...], weight_ref[own, part]) + product(taken_ref[...], weight_ref[other, part])
        merged = (residual_ref[:, part].astype(jnp.float32) + projected).astype(jnp.bfloat16)
        merged_ref[:, part] = merged
        widened = merged.astype(jnp.float32)
        square = square + jnp.sum(widened * widened, axis=1, keepdims=True)
    scale = lax.rsqrt(square / width + 1e-06)
    swap = swap_matrix()
    for g in range(0, rows // SUB, 2):
        blocks = []
        for k in (g, g + 1):
            group = slice(k * SUB, (k + 1) * SUB)
            stacked = []
            for j in range(width // LANES):
                lanes = slice(j * LANES, (j + 1) * LANES)
                widened = merged_ref[group, lanes].astype(jnp.float32)
                stacked.append((widened * scale[group] * norm_gain_ref[:, lanes]).astype(jnp.bfloat16))
            blocks.append(jnp.concatenate(stacked, axis=0))
        for k, turned in zip((g, g + 1), exchange(swap, blocks)):
            chunked[k * SUB : (k + 1) * SUB] = turned.astype(jnp.bfloat16).reshape(SUB, SUB, LANES)

    experts_total = owners_ref.shape[1]
    capacity = outgoing_ref.shape[0] // experts_total

    def copy_rows(expert, carry):
        for place in range(capacity):
            outgoing_ref[capacity * expert + place] = chunked[owners_ref[place, expert]]
        return carry

    lax.fori_loop(0, experts_total, copy_rows, 0, unroll=8)


def shape_of(shape, dtype):
    return jax.ShapeDtypeStruct(shape, dtype)


def limited(mebibytes):
    return pltpu.CompilerParams(vmem_limit_bytes=int(mebibytes * 1048576))


def call(kernel, outs, operands, scalars=0, scratch=(), cost=10000000, room=6, far=False):
    return pl.pallas_call(
        kernel,
        out_shape=outs,
        in_specs=[SMEM_SPEC] * scalars + [HBM_SPEC if far else VMEM_SPEC] * (len(operands) - scalars),
        out_specs=jax.tree.map(lambda _: VMEM_SPEC, outs),
        scratch_shapes=list(scratch),
        cost_estimate=pl.CostEstimate(flops=cost * 400, bytes_accessed=cost, transcendentals=0),
        compiler_params=limited(room),
    )(*operands)


def from_behind(message, axis):
    moved = []
    for k in range(1, RING):
        moved.append(lax.ppermute(message, axis, [(i, (i + k) % RING) for i in range(RING)]))
    return moved


def local(
    residual,
    queries,
    key_rows,
    value_rows,
    out_gate,
    gate_logits,
    head_gain,
    out_weight,
    norm_gain,
    routes,
    group_score,
    expert_score,
    gate_weight,
    up_weight,
    down_weight,
):
    row_count, model_width = residual.shape
    length, channels = queries.shape
    values = value_rows.shape[1]
    f32, bf16 = jnp.float32, jnp.bfloat16
    z, y, x, core = (lax.axis_index(axis).astype(jnp.int32).reshape(1) for axis in SP_TP)
    message_shape = shape_of((channels + SUB, VALUE_DIM), bf16)
    state_shape = shape_of((channels, VALUE_DIM), f32)
    message = call(
        state_kernel,
        message_shape,
        (key_rows, value_rows, gate_logits),
        scratch=[
            pltpu.VMEM(key_rows.shape, bf16),
            pltpu.VMEM(value_rows.shape, bf16),
            pltpu.VMEM(gate_logits.shape, bf16),
            pltpu.SemaphoreType.DMA((3,)),
        ],
        room=53.8,
        far=True,
    )
    experts_total = lax.axis_size(SP_TP)
    capacity = 3 * row_count // experts_total
    slots, owners, weights = routing(routes, group_score, expert_score)
    behind = from_behind(message, "sp_2")
    slots, owners, weights, *behind = lax.optimization_barrier((slots, owners, weights, *behind))
    before_x, decay_x, message_x = call(
        stage_kernel, (state_shape, state_shape, message_shape), (x, message, *behind), 1
    )
    partial, reach = call(
        within_kernel,
        (shape_of((length, values), f32), shape_of((length, channels), f32)),
        (queries, key_rows, value_rows, gate_logits),
    )
    behind = from_behind(message_x, "sp_1")
    partial, reach, *behind = lax.optimization_barrier((partial, reach, *behind))
    before_y, decay_y, message_y = call(
        stage_kernel, (state_shape, state_shape, message_shape), (y, message_x, *behind), 1
    )
    behind = from_behind(message_y, "sp_0")
    half = shape_of((length // 2, values), bf16)
    kept, given = call(
        finish_kernel,
        (half, half),
        (jnp.concatenate([core, z]), *behind, before_y, decay_y, before_x, decay_x, partial, reach, head_gain.reshape(1, -1), out_gate),
        1,
        [pltpu.VMEM((2, length // 2, values), bf16)],
    )
    taken = lax.ppermute(given, "tp", [(0, 1), (1, 0)])
    merged, outgoing = call(
        project_kernel,
        (
            shape_of((row_count, model_width), bf16),
            shape_of((experts_total * capacity, SUB, LANES), bf16),
        ),
        (core, owners, kept, taken, out_weight, residual, norm_gain.reshape(1, -1)),
        2,
        [pltpu.VMEM((row_count, SUB, LANES), bf16)],
        room=14,
    )
    block = (experts_total, capacity * SUB, LANES)
    arrived = lax.all_to_all(outgoing.reshape(block), SP_TP, split_axis=0, concat_axis=0, tiled=True)
    served = experts(arrived.reshape(outgoing.shape), gate_weight, up_weight, down_weight)
    returned = lax.all_to_all(served.reshape(block), SP_TP, split_axis=0, concat_axis=0, tiled=True)
    return combine(slots, returned.reshape(outgoing.shape), merged, weights)


def solution(mesh):
    torus = Mesh(mesh.devices.reshape(4, 4, 4, mesh.shape["tp"]), ("sp_0", "sp_1", "sp_2", "tp"))
    in_specs = (
        P(SP_TP, None),
        P(SP, "tp"),
        P(SP, "tp"),
        P(SP, "tp"),
        P(SP, "tp"),
        P(SP, "tp"),
        P(),
        P(),
        P(),
        P(SP_TP, None),
        P(SP_TP),
        P(SP_TP, None),
        P(SP_TP, None, None),
        P(SP_TP, None, None),
        P(SP_TP, None, None),
    )
    out_specs = P(SP_TP, None)
    return jax.shard_map(local, mesh=torus, in_specs=in_specs, out_specs=out_specs, check_vma=False)
```

```python
import jax
import jax.numpy as jnp
from jax import lax
from jax.experimental import pallas as pl
from jax.experimental.pallas import tpu as pltpu
from jax.sharding import Mesh
from jax.sharding import PartitionSpec as P

KEY_DIM = 64
VALUE_DIM = 128
BLOCK = 64
RING = 4
SP = ("sp_0", "sp_1", "sp_2")
SP_TP = ("sp_0", "sp_1", "sp_2", "tp")


VMEM_SPEC = pl.BlockSpec(memory_space=pltpu.VMEM)
SMEM_SPEC = pl.BlockSpec(memory_space=pltpu.SMEM)
HBM_SPEC = pl.BlockSpec(memory_space=pl.ANY)
SUB = 16
LANES = 128
SWAP = SUB * SUB


def swap_matrix():
    row = lax.broadcasted_iota(jnp.int32, (SWAP, SWAP), 0)
    column = lax.broadcasted_iota(jnp.int32, (SWAP, SWAP), 1)
    partner = (row & (SUB - 1)) * SUB + (row >> 4)
    return (partner == column).astype(jnp.float32).astype(jnp.bfloat16)


def exchange(swap, blocks):
    turned = jnp.dot(swap, jnp.concatenate(blocks, axis=1), preferred_element_type=jnp.float32)
    return [turned[:, k * LANES : (k + 1) * LANES] for k in range(len(blocks))]


def stack_chunks(ref, g):
    width = ref.shape[1]
    return jnp.concatenate(
        [ref[g * SUB : (g + 1) * SUB, j * LANES : (j + 1) * LANES] for j in range(width // LANES)], axis=0
    )


def routing_kernel(routes_ref, group_ref, expert_ref, slots_ref, owners_ref, weights_ref):
    choices, rows = routes_ref.shape
    capacity = 3
    bf16 = jnp.bfloat16
    expert = lax.broadcasted_iota(jnp.int32, (LANES, rows), 0)
    token = lax.broadcasted_iota(jnp.int32, (LANES, rows), 1)
    named = [expert == routes_ref[k : k + 1] for k in range(choices)]
    named = [one.astype(jnp.float32) for one in named]
    source = lax.broadcasted_iota(jnp.int32, (rows, rows), 0)
    target = lax.broadcasted_iota(jnp.int32, (rows, rows), 1)
    before = (source < target).astype(jnp.float32).astype(bf16)
    used = jnp.dot(sum(named).astype(bf16), before, preferred_element_type=jnp.float32)
    place = lax.broadcasted_iota(jnp.int32, (8, rows), 0).astype(jnp.float32)
    name = lax.broadcasted_iota(jnp.int32, (8, rows), 1).astype(jnp.float32)
    owners = jnp.zeros((8, LANES), jnp.float32)
    for k in range(choices):
        rank = jnp.sum(named[k] * used, axis=0, keepdims=True)
        slots_ref[k : k + 1] = routes_ref[k : k + 1] * capacity + rank.astype(jnp.int32)
        owned = jnp.where(place == rank, name, 0.0).astype(bf16)
        owners = owners + lax.dot_general(
            owned, named[k].astype(bf16), (((1,), (1,)), ((), ())), preferred_element_type=jnp.float32
        )
    owners_ref[...] = owners.astype(jnp.int32)
    score = expert_ref[...]
    weights = group_ref[...] * score / jnp.sum(score, axis=0, keepdims=True)
    for k in range(choices):
        spread = jnp.broadcast_to(weights[k : k + 1], (LANES, rows))
        weights_ref[k] = spread.T


def routing(routes, group_score, expert_score):
    rows, choices = routes.shape
    return call(
        routing_kernel,
        (
            shape_of((choices, rows), jnp.int32),
            shape_of((8, LANES), jnp.int32),
            shape_of((choices, rows, LANES), jnp.float32),
        ),
        (routes.T, group_score.reshape(1, rows), expert_score.T),
        room=2,
    )


def experts_kernel(rows_ref, gate, up, down, out_ref, rows_in, inner, served):
    swap = swap_matrix()
    count, width = rows_in.shape
    hidden = inner.shape[1]
    groups = count // SUB
    for g in range(0, groups, 2):
        blocks = [rows_ref[k * SUB : (k + 1) * SUB].reshape(SWAP, LANES) for k in (g, g + 1)]
        for k, turned in zip((g, g + 1), exchange(swap, blocks)):
            turned = turned.astype(jnp.bfloat16)
            for j in range(width // LANES):
                rows_in[k * SUB : (k + 1) * SUB, j * LANES : (j + 1) * LANES] = turned[j * SUB : (j + 1) * SUB]
    tile = 256
    for n in range(hidden // tile):
        part = slice(n * tile, (n + 1) * tile)
        gated = jnp.dot(rows_in[...], gate[0, :, part], preferred_element_type=jnp.float32)
        lifted = jnp.dot(rows_in[...], up[0, :, part], preferred_element_type=jnp.float32)
        inner[:, part] = (gated / (1.0 + jnp.exp(-gated)) * lifted).astype(jnp.bfloat16)
    for n in range(width // tile):
        part = slice(n * tile, (n + 1) * tile)
        served[:, part] = jnp.dot(inner[...], down[0, :, part], preferred_element_type=jnp.float32).astype(jnp.bfloat16)
    for g in range(0, groups, 2):
        blocks = [stack_chunks(served, k) for k in (g, g + 1)]
        for k, turned in zip((g, g + 1), exchange(swap, blocks)):
            out_ref[k * SUB : (k + 1) * SUB] = turned.astype(jnp.bfloat16).reshape(SUB, SUB, LANES)


def experts(arrived, gate_weight, up_weight, down_weight):
    count = arrived.shape[0]
    width, hidden = gate_weight.shape[1:]
    return pl.pallas_call(
        experts_kernel,
        out_shape=jax.ShapeDtypeStruct(arrived.shape, jnp.bfloat16),
        in_specs=[VMEM_SPEC] * 4,
        out_specs=VMEM_SPEC,
        scratch_shapes=[
            pltpu.VMEM((count, width), jnp.bfloat16),
            pltpu.VMEM((count, hidden), jnp.bfloat16),
            pltpu.VMEM((count, width), jnp.bfloat16),
        ],
        compiler_params=limited(16),
        name="experts",
    )(arrived, gate_weight, up_weight, down_weight)


def combine_kernel(slots_ref, returned_ref, merged_ref, weights_ref, out_ref, picked):
    swap = swap_matrix()
    rows, width = merged_ref.shape

    def copy_row(i, carry):
        picked[0, i] = returned_ref[slots_ref[0, i]]
        picked[1, i] = returned_ref[slots_ref[1, i]]
        return carry

    lax.fori_loop(0, rows, copy_row, 0, unroll=8)
    for g in range(rows // SUB):
        group = slice(g * SUB, (g + 1) * SUB)
        first, second = exchange(swap, [picked[k, group].reshape(SWAP, LANES) for k in range(2)])
        for j in range(width // LANES):
            lanes = slice(j * LANES, (j + 1) * LANES)
            part = slice(j * SUB, (j + 1) * SUB)
            total = weights_ref[0, group] * first[part] + weights_ref[1, group] * second[part]
            out_ref[group, lanes] = (merged_ref[group, lanes].astype(jnp.float32) + total).astype(jnp.bfloat16)


def combine(slots, returned, merged, weights):
    rows = merged.shape[0]
    return call(
        combine_kernel,
        shape_of(merged.shape, jnp.bfloat16),
        (slots, returned, merged, weights),
        1,
        [pltpu.VMEM((2, rows, SUB, LANES), jnp.bfloat16)],
        room=8,
    )


def pieces(value, count):
    parts = []
    for _ in range(count):
        part = value.astype(jnp.bfloat16)
        parts.append(part)
        value = value - part.astype(jnp.float32)
    return parts


def product(left, right, left_dim=1, right_dim=0):
    return lax.dot_general(
        left, right, (((left_dim,), (right_dim,)), ((), ())), preferred_element_type=jnp.float32
    )


def running_sums(logits):
    length = logits.shape[0]
    blocks = length // BLOCK
    decay_log = (jnp.minimum(logits, 0.0) - jnp.log1p(jnp.exp(-jnp.abs(logits)))) / 16.0
    parts = pieces(decay_log, 3)
    row = lax.broadcasted_iota(jnp.int32, (length, length), 0)
    column = lax.broadcasted_iota(jnp.int32, (length, length), 1)
    earlier = (row >= column) & (row // BLOCK == column // BLOCK)
    earlier = earlier.astype(jnp.float32).astype(jnp.bfloat16)
    running = sum(product(earlier, part) for part in parts)
    token = lax.broadcasted_iota(jnp.int32, (length, blocks * LANES), 0)
    lane = lax.broadcasted_iota(jnp.int32, (length, blocks * LANES), 1)
    member = (token // BLOCK == lane // LANES).astype(jnp.float32).astype(jnp.bfloat16)
    block_decay = jnp.exp(sum(product(part, member, 0, 0) for part in parts))
    return running, block_decay


def grow(states, n, running, block_decay, keys_ref, values_ref):
    wide = 2 * VALUE_DIM
    rows = slice(n * BLOCK, (n + 1) * BLOCK)
    closing = running[(n + 1) * BLOCK - 1 : (n + 1) * BLOCK]
    key_closing = keys_ref[rows].astype(jnp.float32) * jnp.exp(closing - running[rows])
    key_closing = key_closing.astype(jnp.bfloat16)
    after = []
    for p, state in enumerate(states):
        lanes = slice(p * LANES, (p + 1) * LANES)
        grown = product(key_closing[:, lanes], values_ref[rows, p * wide : (p + 1) * wide], 0, 0)
        grown = jnp.concatenate([grown[:KEY_DIM, :VALUE_DIM], grown[KEY_DIM:, VALUE_DIM:]], axis=0)
        after.append(block_decay[lanes, n * LANES : (n + 1) * LANES] * state + grown)
    return after


def state_kernel(keys_hbm, values_hbm, logits_hbm, message_ref, keys_ref, values_ref, logits_ref, sems):
    copies = [
        pltpu.make_async_copy(source, target, sems.at[k])
        for k, (source, target) in enumerate(
            ((logits_hbm, logits_ref), (keys_hbm, keys_ref), (values_hbm, values_ref))
        )
    ]
    for copy in copies:
        copy.start()
    copies[0].wait()
    length, channels = keys_ref.shape
    blocks = length // BLOCK
    pairs = channels // LANES
    running, block_decay = running_sums(logits_ref[...].astype(jnp.float32))
    copies[1].wait()
    copies[2].wait()
    states = [jnp.zeros((LANES, VALUE_DIM), jnp.float32)] * pairs
    total = jnp.zeros((1, channels), jnp.float32)
    for n in range(blocks):
        total = total + running[(n + 1) * BLOCK - 1 : (n + 1) * BLOCK]
        states = grow(states, n, running, block_decay, keys_ref, values_ref)
    for p in range(pairs):
        message_ref[p * LANES : (p + 1) * LANES] = states[p].astype(jnp.bfloat16)
    message_ref[channels:] = pack_decay(jnp.exp(total))


def pack_decay(decay):
    pairs = decay.shape[1] // LANES
    place = lax.broadcasted_iota(jnp.int32, (SUB, LANES), 0)
    high, low = pieces(decay, 2)
    packed = jnp.zeros((SUB, LANES), jnp.float32)
    for p in range(pairs):
        lanes = slice(p * LANES, (p + 1) * LANES)
        packed = jnp.where(place == p, high[:, lanes].astype(jnp.float32), packed)
        packed = jnp.where(place == pairs + p, low[:, lanes].astype(jnp.float32), packed)
    return packed.astype(jnp.bfloat16)


def unpack_decay(message_ref):
    channels = message_ref.shape[0] - SUB
    pairs = channels // LANES
    packed = message_ref[channels:].astype(jnp.float32)
    diagonal = lax.broadcasted_iota(jnp.int32, (LANES, LANES), 0) == lax.broadcasted_iota(
        jnp.int32, (LANES, LANES), 1
    )
    ones = jnp.ones((LANES, VALUE_DIM), jnp.bfloat16)
    spread = []
    for p in range(pairs):
        both = [jnp.where(diagonal, packed[k : k + 1], 0.0).astype(jnp.bfloat16) for k in (p, pairs + p)]
        spread.append(product(both[0], ones) + product(both[1], ones))
    line = jnp.concatenate([packed[p : p + 1] + packed[pairs + p : pairs + p + 1] for p in range(pairs)], axis=1)
    return line, jnp.concatenate(spread, axis=0)


def stage_kernel(place_ref, own_ref, back1_ref, back2_ref, back3_ref, before_ref, decay_ref, message_ref):
    place = place_ref[0]
    channels = own_ref.shape[0] - SUB
    received = []
    for ref in (back1_ref, back2_ref, back3_ref):
        line, spread = unpack_decay(ref)
        received.append((line, spread, ref[:channels].astype(jnp.float32)))
    own_line, own_spread = unpack_decay(own_ref)
    before = jnp.zeros((channels, VALUE_DIM), jnp.float32)
    decay = jnp.ones((channels, VALUE_DIM), jnp.float32)
    for k in (3, 2, 1):
        valid = place >= k
        _, spread, state = received[k - 1]
        before = jnp.where(valid, spread * before + state, before)
        decay = jnp.where(valid, spread * decay, decay)
    before_ref[...] = before
    decay_ref[...] = decay
    total = own_spread * before + own_ref[:channels].astype(jnp.float32)
    for k in (3, 2, 1):
        later = place < k
        _, spread, state = received[k - 1]
        total = jnp.where(later, spread * total + state, total)
    message_ref[:channels] = total.astype(jnp.bfloat16)
    line = own_line * received[0][0] * received[1][0] * received[2][0]
    message_ref[channels:] = pack_decay(line)


def masked_heads(rows):
    lane = lax.broadcasted_iota(jnp.int32, rows.shape, 1)
    return jnp.concatenate(
        [jnp.where(lane < KEY_DIM, rows, 0.0), jnp.where(lane >= KEY_DIM, rows, 0.0)], axis=0
    ).astype(jnp.bfloat16)


def within_kernel(queries_ref, keys_ref, values_ref, logits_ref, partial_ref, reach_ref):
    length, channels = keys_ref.shape
    blocks = length // BLOCK
    pairs = channels // LANES
    running_all, block_decay = running_sums(logits_ref[...].astype(jnp.float32))
    states = [jnp.zeros((LANES, VALUE_DIM), jnp.float32)] * pairs
    lead = jnp.zeros((1, channels), jnp.float32)
    row = lax.broadcasted_iota(jnp.int32, (2 * BLOCK, BLOCK), 0)
    column = lax.broadcasted_iota(jnp.int32, (2 * BLOCK, BLOCK), 1)
    causal = (row & (BLOCK - 1)) >= column
    for n in range(blocks):
        rows = slice(n * BLOCK, (n + 1) * BLOCK)
        running = running_all[rows]
        query_scaled = queries_ref[rows].astype(jnp.float32) * KEY_DIM ** (-0.5) * jnp.exp(running)
        key_inverse = (keys_ref[rows].astype(jnp.float32) * jnp.exp(-running)).astype(jnp.bfloat16)
        reach_ref[rows] = query_scaled * jnp.exp(lead)
        lead = lead + running[BLOCK - 1 : BLOCK]
        for p in range(pairs):
            lanes = slice(p * LANES, (p + 1) * LANES)
            masked = masked_heads(query_scaled[:, lanes])
            scores = jnp.where(causal, product(masked, key_inverse[:, lanes], 1, 1), 0.0).astype(jnp.bfloat16)
            carried = product(masked, states[p].astype(jnp.bfloat16))
            for h in range(2):
                place = slice((2 * p + h) * VALUE_DIM, (2 * p + h + 1) * VALUE_DIM)
                part = slice(h * BLOCK, (h + 1) * BLOCK)
                partial_ref[rows, place] = product(scores[part], values_ref[rows, place]) + carried[part]
        if n + 1 < blocks:
            states = grow(states, n, running_all, block_decay, keys_ref, values_ref)


def finish_kernel(
    place_ref, plane_ref, back1_ref, back2_ref, back3_ref, before_y_ref, decay_y_ref, before_x_ref, decay_x_ref,
    partial_ref, reach_ref, head_gain_ref, out_gate_ref, kept_ref, given_ref, whole,
):
    core, plane = place_ref[0], plane_ref[0]
    length, channels = reach_ref.shape
    pairs = channels // LANES
    state = jnp.zeros((channels, VALUE_DIM), jnp.float32)
    for k, ref in ((3, back3_ref), (2, back2_ref), (1, back1_ref)):
        passed = unpack_decay(ref)[1] * state + ref[:channels].astype(jnp.float32)
        state = jnp.where(plane >= k, passed, state)
    state = before_y_ref[...] + decay_y_ref[...] * state
    state = (before_x_ref[...] + decay_x_ref[...] * state).astype(jnp.bfloat16)
    half = length // 2
    for p in range(pairs):
        lanes = slice(p * LANES, (p + 1) * LANES)
        carried = product(masked_heads(reach_ref[:, lanes]), state[lanes])
        for h in range(2):
            place = slice((2 * p + h) * VALUE_DIM, (2 * p + h + 1) * VALUE_DIM)
            attended = partial_ref[:, place] + carried[h * length : (h + 1) * length]
            scale = lax.rsqrt(jnp.mean(attended * attended, axis=1, keepdims=True) + 1e-06)
            gate = out_gate_ref[:, place].astype(jnp.float32)
            result = attended * scale * head_gain_ref[...] * (gate / (1.0 + jnp.exp(-gate)))
            result = result.astype(jnp.bfloat16)
            whole[0, :, place] = result[:half]
            whole[1, :, place] = result[half:]
    kept_ref[...] = whole[core]
    given_ref[...] = whole[1 - core]


def project_kernel(
    place_ref, owners_ref, kept_ref, taken_ref, weight_ref, residual_ref, norm_gain_ref, merged_ref, outgoing_ref,
    chunked,
):
    core = place_ref[0]
    rows, width = residual_ref.shape
    depth = kept_ref.shape[1]
    tile = 256
    own = pl.ds(pl.multiple_of(core * depth, depth), depth)
    other = pl.ds(pl.multiple_of((1 - core) * depth, depth), depth)
    square = jnp.zeros((rows, 1), jnp.float32)
    for n in range(width // tile):
        part = slice(n * tile, (n + 1) * tile)
        projected = product(kept_ref[...], weight_ref[own, part]) + product(taken_ref[...], weight_ref[other, part])
        merged = (residual_ref[:, part].astype(jnp.float32) + projected).astype(jnp.bfloat16)
        merged_ref[:, part] = merged
        widened = merged.astype(jnp.float32)
        square = square + jnp.sum(widened * widened, axis=1, keepdims=True)
    scale = lax.rsqrt(square / width + 1e-06)
    swap = swap_matrix()
    for g in range(0, rows // SUB, 2):
        blocks = []
        for k in (g, g + 1):
            group = slice(k * SUB, (k + 1) * SUB)
            stacked = []
            for j in range(width // LANES):
                lanes = slice(j * LANES, (j + 1) * LANES)
                widened = merged_ref[group, lanes].astype(jnp.float32)
                stacked.append((widened * scale[group] * norm_gain_ref[:, lanes]).astype(jnp.bfloat16))
            blocks.append(jnp.concatenate(stacked, axis=0))
        for k, turned in zip((g, g + 1), exchange(swap, blocks)):
            chunked[k * SUB : (k + 1) * SUB] = turned.astype(jnp.bfloat16).reshape(SUB, SUB, LANES)

    experts_total = owners_ref.shape[1]
    capacity = outgoing_ref.shape[0] // experts_total

    def copy_rows(expert, carry):
        for place in range(capacity):
            outgoing_ref[capacity * expert + place] = chunked[owners_ref[place, expert]]
        return carry

    lax.fori_loop(0, experts_total, copy_rows, 0, unroll=8)


def shape_of(shape, dtype):
    return jax.ShapeDtypeStruct(shape, dtype)


def limited(mebibytes):
    return pltpu.CompilerParams(vmem_limit_bytes=int(mebibytes * 1048576))


def call(kernel, outs, operands, scalars=0, scratch=(), cost=10000000, room=6, far=False):
    return pl.pallas_call(
        kernel,
        out_shape=outs,
        in_specs=[SMEM_SPEC] * scalars + [HBM_SPEC if far else VMEM_SPEC] * (len(operands) - scalars),
        out_specs=jax.tree.map(lambda _: VMEM_SPEC, outs),
        scratch_shapes=list(scratch),
        cost_estimate=pl.CostEstimate(flops=cost * 400, bytes_accessed=cost, transcendentals=0),
        compiler_params=limited(room),
    )(*operands)


def from_behind(message, axis):
    moved = []
    for k in range(1, RING):
        moved.append(lax.ppermute(message, axis, [(i, (i + k) % RING) for i in range(RING)]))
    return moved


def local(
    residual,
    queries,
    key_rows,
    value_rows,
    out_gate,
    gate_logits,
    head_gain,
    out_weight,
    norm_gain,
    routes,
    group_score,
    expert_score,
    gate_weight,
    up_weight,
    down_weight,
):
    row_count, model_width = residual.shape
    length, channels = queries.shape
    values = value_rows.shape[1]
    f32, bf16 = jnp.float32, jnp.bfloat16
    z, y, x, core = (lax.axis_index(axis).astype(jnp.int32).reshape(1) for axis in SP_TP)
    message_shape = shape_of((channels + SUB, VALUE_DIM), bf16)
    state_shape = shape_of((channels, VALUE_DIM), f32)
    message = call(
        state_kernel,
        message_shape,
        (key_rows, value_rows, gate_logits),
        scratch=[
            pltpu.VMEM(key_rows.shape, bf16),
            pltpu.VMEM(value_rows.shape, bf16),
            pltpu.VMEM(gate_logits.shape, bf16),
            pltpu.SemaphoreType.DMA((3,)),
        ],
        room=53.8,
        far=True,
    )
    experts_total = lax.axis_size(SP_TP)
    capacity = 3 * row_count // experts_total
    slots, owners, weights = routing(routes, group_score, expert_score)
    behind = from_behind(message, "sp_2")
    slots, owners, weights, *behind = lax.optimization_barrier((slots, owners, weights, *behind))
    before_x, decay_x, message_x = call(
        stage_kernel, (state_shape, state_shape, message_shape), (x, message, *behind), 1
    )
    partial, reach = call(
        within_kernel,
        (shape_of((length, values), f32), shape_of((length, channels), f32)),
        (queries, key_rows, value_rows, gate_logits),
    )
    behind = from_behind(message_x, "sp_1")
    partial, reach, *behind = lax.optimization_barrier((partial, reach, *behind))
    before_y, decay_y, message_y = call(
        stage_kernel, (state_shape, state_shape, message_shape), (y, message_x, *behind), 1
    )
    behind = from_behind(message_y, "sp_0")
    half = shape_of((length // 2, values), bf16)
    kept, given = call(
        finish_kernel,
        (half, half),
        (core, z, *behind, before_y, decay_y, before_x, decay_x, partial, reach, head_gain.reshape(1, -1), out_gate),
        2,
        [pltpu.VMEM((2, length // 2, values), bf16)],
    )
    taken = lax.ppermute(given, "tp", [(0, 1), (1, 0)])
    merged, outgoing = call(
        project_kernel,
        (
            shape_of((row_count, model_width), bf16),
            shape_of((experts_total * capacity, SUB, LANES), bf16),
        ),
        (core, owners, kept, taken, out_weight, residual, norm_gain.reshape(1, -1)),
        2,
        [pltpu.VMEM((row_count, SUB, LANES), bf16)],
        room=14,
    )
    block = (experts_total, capacity * SUB, LANES)
    arrived = lax.all_to_all(outgoing.reshape(block), SP_TP, split_axis=0, concat_axis=0, tiled=True)
    served = experts(arrived.reshape(outgoing.shape), gate_weight, up_weight, down_weight)
    returned = lax.all_to_all(served.reshape(block), SP_TP, split_axis=0, concat_axis=0, tiled=True)
    return combine(slots, returned.reshape(outgoing.shape), merged, weights)


def solution(mesh):
    torus = Mesh(mesh.devices.reshape(4, 4, 4, mesh.shape["tp"]), ("sp_0", "sp_1", "sp_2", "tp"))
    in_specs = (
        P(SP_TP, None),
        P(SP, "tp"),
        P(SP, "tp"),
        P(SP, "tp"),
        P(SP, "tp"),
        P(SP, "tp"),
        P(),
        P(),
        P(),
        P(SP_TP, None),
        P(SP_TP),
        P(SP_TP, None),
        P(SP_TP, None, None),
        P(SP_TP, None, None),
        P(SP_TP, None, None),
    )
    out_specs = P(SP_TP, None)
    return jax.shard_map(local, mesh=torus, in_specs=in_specs, out_specs=out_specs, check_vma=False)
```

```python
import jax
import jax.numpy as jnp
from jax import lax
from jax.experimental import pallas as pl
from jax.experimental.pallas import tpu as pltpu
from jax.sharding import Mesh
from jax.sharding import PartitionSpec as P

KEY_DIM = 64
VALUE_DIM = 128
BLOCK = 64
RING = 4
SP = ("sp_0", "sp_1", "sp_2")
SP_TP = ("sp_0", "sp_1", "sp_2", "tp")


VMEM_SPEC = pl.BlockSpec(memory_space=pltpu.VMEM)
SMEM_SPEC = pl.BlockSpec(memory_space=pltpu.SMEM)
ANY_SPEC = pl.BlockSpec(memory_space=pl.ANY)
SUB = 16
LANES = 128
SWAP = SUB * SUB


def swap_matrix():
    row = lax.broadcasted_iota(jnp.int32, (SWAP, SWAP), 0)
    column = lax.broadcasted_iota(jnp.int32, (SWAP, SWAP), 1)
    partner = (row & (SUB - 1)) * SUB + (row >> 4)
    return (partner == column).astype(jnp.float32).astype(jnp.bfloat16)


def exchange(swap, blocks):
    turned = jnp.dot(swap, jnp.concatenate(blocks, axis=1), preferred_element_type=jnp.float32)
    return [turned[:, k * LANES : (k + 1) * LANES] for k in range(len(blocks))]


def stack_chunks(ref, g):
    width = ref.shape[1]
    return jnp.concatenate(
        [ref[g * SUB : (g + 1) * SUB, j * LANES : (j + 1) * LANES] for j in range(width // LANES)], axis=0
    )


def routing_kernel(routes_ref, group_ref, expert_ref, slots_ref, owners_ref, weights_ref):
    choices, rows = routes_ref.shape
    capacity = 3
    bf16 = jnp.bfloat16
    expert = lax.broadcasted_iota(jnp.int32, (LANES, rows), 0)
    token = lax.broadcasted_iota(jnp.int32, (LANES, rows), 1)
    named = [expert == routes_ref[k : k + 1] for k in range(choices)]
    named = [one.astype(jnp.float32) for one in named]
    source = lax.broadcasted_iota(jnp.int32, (rows, rows), 0)
    target = lax.broadcasted_iota(jnp.int32, (rows, rows), 1)
    before = (source < target).astype(jnp.float32).astype(bf16)
    used = jnp.dot(sum(named).astype(bf16), before, preferred_element_type=jnp.float32)
    place = lax.broadcasted_iota(jnp.int32, (8, rows), 0).astype(jnp.float32)
    name = lax.broadcasted_iota(jnp.int32, (8, rows), 1).astype(jnp.float32)
    owners = jnp.zeros((8, LANES), jnp.float32)
    for k in range(choices):
        rank = jnp.sum(named[k] * used, axis=0, keepdims=True)
        slots_ref[k : k + 1] = routes_ref[k : k + 1] * capacity + rank.astype(jnp.int32)
        owned = jnp.where(place == rank, name, 0.0).astype(bf16)
        owners = owners + lax.dot_general(
            owned, named[k].astype(bf16), (((1,), (1,)), ((), ())), preferred_element_type=jnp.float32
        )
    owners_ref[...] = owners.astype(jnp.int32)
    score = expert_ref[...]
    weights = group_ref[...] * score / jnp.sum(score, axis=0, keepdims=True)
    for k in range(choices):
        spread = jnp.broadcast_to(weights[k : k + 1], (LANES, rows))
        weights_ref[k] = spread.T


def routing(routes, group_score, expert_score):
    rows, choices = routes.shape
    return call(
        routing_kernel,
        (
            shape_of((choices, rows), jnp.int32),
            shape_of((8, LANES), jnp.int32),
            shape_of((choices, rows, LANES), jnp.float32),
        ),
        (routes.T, group_score.reshape(1, rows), expert_score.T),
        room=2,
    )


def experts_kernel(rows_ref, gate, up, down, out_ref, rows_in, inner, served):
    swap = swap_matrix()
    count, width = rows_in.shape
    hidden = inner.shape[1]
    groups = count // SUB
    for g in range(0, groups, 2):
        blocks = [rows_ref[k * SUB : (k + 1) * SUB].reshape(SWAP, LANES) for k in (g, g + 1)]
        for k, turned in zip((g, g + 1), exchange(swap, blocks)):
            turned = turned.astype(jnp.bfloat16)
            for j in range(width // LANES):
                rows_in[k * SUB : (k + 1) * SUB, j * LANES : (j + 1) * LANES] = turned[j * SUB : (j + 1) * SUB]
    tile = 256
    for n in range(hidden // tile):
        part = slice(n * tile, (n + 1) * tile)
        gated = jnp.dot(rows_in[...], gate[0, :, part], preferred_element_type=jnp.float32)
        lifted = jnp.dot(rows_in[...], up[0, :, part], preferred_element_type=jnp.float32)
        inner[:, part] = (gated / (1.0 + jnp.exp(-gated)) * lifted).astype(jnp.bfloat16)
    for n in range(width // tile):
        part = slice(n * tile, (n + 1) * tile)
        served[:, part] = jnp.dot(inner[...], down[0, :, part], preferred_element_type=jnp.float32).astype(jnp.bfloat16)
    for g in range(0, groups, 2):
        blocks = [stack_chunks(served, k) for k in (g, g + 1)]
        for k, turned in zip((g, g + 1), exchange(swap, blocks)):
            out_ref[k * SUB : (k + 1) * SUB] = turned.astype(jnp.bfloat16).reshape(SUB, SUB, LANES)


def experts(arrived, gate_weight, up_weight, down_weight):
    count = arrived.shape[0]
    width, hidden = gate_weight.shape[1:]
    return pl.pallas_call(
        experts_kernel,
        out_shape=jax.ShapeDtypeStruct(arrived.shape, jnp.bfloat16),
        in_specs=[VMEM_SPEC] * 4,
        out_specs=VMEM_SPEC,
        scratch_shapes=[
            pltpu.VMEM((count, width), jnp.bfloat16),
            pltpu.VMEM((count, hidden), jnp.bfloat16),
            pltpu.VMEM((count, width), jnp.bfloat16),
        ],
        compiler_params=limited(16),
        name="experts",
    )(arrived, gate_weight, up_weight, down_weight)


def combine_kernel(slots_vmem, returned_ref, merged_ref, weights_ref, out_hbm, out_ref, slots_ref, sem, sems):
    indices = pltpu.make_async_copy(slots_vmem, slots_ref, sem.at[0])
    indices.start()
    swap = swap_matrix()
    rows, width = merged_ref.shape
    indices.wait()
    copies = []
    for g in range(rows // SUB):
        group = slice(g * SUB, (g + 1) * SUB)
        picked = [
            jnp.concatenate([returned_ref[slots_ref[k, g * SUB + i]] for i in range(SUB)], axis=0) for k in range(2)
        ]
        first, second = exchange(swap, picked)
        for j in range(width // LANES):
            lanes = slice(j * LANES, (j + 1) * LANES)
            part = slice(j * SUB, (j + 1) * SUB)
            total = weights_ref[0, group] * first[part] + weights_ref[1, group] * second[part]
            out_ref[group, lanes] = (merged_ref[group, lanes].astype(jnp.float32) + total).astype(jnp.bfloat16)
        if g % 2 == 1:
            both = pl.ds((g - 1) * SUB, 2 * SUB)
            copies.append(pltpu.make_async_copy(out_ref.at[both], out_hbm.at[both], sems.at[g // 2]))
            copies[-1].start()
    for copy in copies:
        copy.wait()


def combine(slots, returned, merged, weights):
    rows = merged.shape[0]
    return pl.pallas_call(
        combine_kernel,
        out_shape=shape_of(merged.shape, jnp.bfloat16),
        in_specs=[VMEM_SPEC] * 4,
        out_specs=ANY_SPEC,
        scratch_shapes=[
            pltpu.VMEM(merged.shape, jnp.bfloat16),
            pltpu.SMEM(slots.shape, jnp.int32),
            pltpu.SemaphoreType.DMA((1,)),
            pltpu.SemaphoreType.DMA((rows // SUB // 2,)),
        ],
        compiler_params=limited(8),
        name="combine",
    )(slots, returned, merged, weights)


def pieces(value, count):
    parts = []
    for _ in range(count):
        part = value.astype(jnp.bfloat16)
        parts.append(part)
        value = value - part.astype(jnp.float32)
    return parts


def product(left, right, left_dim=1, right_dim=0):
    return lax.dot_general(
        left, right, (((left_dim,), (right_dim,)), ((), ())), preferred_element_type=jnp.float32
    )


def running_sums(logits):
    length = logits.shape[0]
    decay_log = (jnp.minimum(logits, 0.0) - jnp.log1p(jnp.exp(-jnp.abs(logits)))) / 16.0
    parts = pieces(decay_log, 3)
    row = lax.broadcasted_iota(jnp.int32, (length, length), 0)
    column = lax.broadcasted_iota(jnp.int32, (length, length), 1)
    earlier = (row >= column) & (row // BLOCK == column // BLOCK)
    earlier = earlier.astype(jnp.float32).astype(jnp.bfloat16)
    return sum(product(earlier, part) for part in parts)


def grow(states, n, running, keys_ref, values_ref):
    wide = 2 * VALUE_DIM
    rows = slice(n * BLOCK, (n + 1) * BLOCK)
    closing = running[(n + 1) * BLOCK - 1 : (n + 1) * BLOCK]
    key_closing = keys_ref[rows].astype(jnp.float32) * jnp.exp(closing - running[rows])
    key_closing = key_closing.astype(jnp.bfloat16)
    decay = jnp.exp(closing)
    lane = lax.broadcasted_iota(jnp.int32, (VALUE_DIM, LANES), 1)
    after = []
    for p, state in enumerate(states):
        lanes = slice(p * LANES, (p + 1) * LANES)
        grown = product(values_ref[rows, p * wide : (p + 1) * wide], key_closing[:, lanes], 0, 0)
        grown = jnp.where(lane < KEY_DIM, grown[:VALUE_DIM], grown[VALUE_DIM:])
        after.append(decay[:, lanes] * state + grown)
    return after


def state_kernel(keys_hbm, values_hbm, logits_hbm, message_ref, keys_ref, values_ref, logits_ref, sems):
    copies = [
        pltpu.make_async_copy(source, target, sems.at[k])
        for k, (source, target) in enumerate(
            ((logits_hbm, logits_ref), (keys_hbm, keys_ref), (values_hbm, values_ref))
        )
    ]
    for copy in copies:
        copy.start()
    copies[0].wait()
    length, channels = keys_ref.shape
    blocks = length // BLOCK
    pairs = channels // LANES
    running = running_sums(logits_ref[...].astype(jnp.float32))
    copies[1].wait()
    copies[2].wait()
    states = [jnp.zeros((VALUE_DIM, LANES), jnp.float32)] * pairs
    total = jnp.zeros((1, channels), jnp.float32)
    for n in range(blocks):
        total = total + running[(n + 1) * BLOCK - 1 : (n + 1) * BLOCK]
        states = grow(states, n, running, keys_ref, values_ref)
    for p in range(pairs):
        message_ref[p * VALUE_DIM : (p + 1) * VALUE_DIM] = states[p].astype(jnp.bfloat16)
    message_ref[pairs * VALUE_DIM :] = pack_decay(jnp.exp(total))


def pack_decay(decay):
    pairs = decay.shape[1] // LANES
    place = lax.broadcasted_iota(jnp.int32, (SUB, LANES), 0)
    high, low = pieces(decay, 2)
    packed = jnp.zeros((SUB, LANES), jnp.float32)
    for p in range(pairs):
        lanes = slice(p * LANES, (p + 1) * LANES)
        packed = jnp.where(place == p, high[:, lanes].astype(jnp.float32), packed)
        packed = jnp.where(place == pairs + p, low[:, lanes].astype(jnp.float32), packed)
    return packed.astype(jnp.bfloat16)


def unpack(message_ref):
    states = message_ref.shape[0] - SUB
    pairs = states // VALUE_DIM
    packed = message_ref[states:].astype(jnp.float32)
    decays = [packed[p : p + 1] + packed[pairs + p : pairs + p + 1] for p in range(pairs)]
    return decays, [message_ref[p * VALUE_DIM : (p + 1) * VALUE_DIM].astype(jnp.float32) for p in range(pairs)]


def stage_kernel(place_ref, own_ref, back1_ref, back2_ref, back3_ref, before_ref, decay_ref, message_ref):
    place = place_ref[0]
    own_decays, own_states = unpack(own_ref)
    pairs = len(own_decays)
    received = [unpack(ref) for ref in (back1_ref, back2_ref, back3_ref)]
    whole = []
    for p in range(pairs):
        rows = slice(p * VALUE_DIM, (p + 1) * VALUE_DIM)
        before = jnp.zeros((VALUE_DIM, LANES), jnp.float32)
        decay = jnp.ones((1, LANES), jnp.float32)
        for k in (3, 2, 1):
            valid = place >= k
            passed, state = received[k - 1][0][p], received[k - 1][1][p]
            before = jnp.where(valid, passed * before + state, before)
            decay = jnp.where(valid, passed * decay, decay)
        before_ref[rows] = before
        decay_ref[p * 8 : (p + 1) * 8] = jnp.broadcast_to(decay, (8, LANES))
        total = own_decays[p] * before + own_states[p]
        for k in (3, 2, 1):
            later = place < k
            passed, state = received[k - 1][0][p], received[k - 1][1][p]
            total = jnp.where(later, passed * total + state, total)
        message_ref[rows] = total.astype(jnp.bfloat16)
        whole.append(own_decays[p] * received[0][0][p] * received[1][0][p] * received[2][0][p])
    message_ref[pairs * VALUE_DIM :] = pack_decay(jnp.concatenate(whole, axis=1))


def masked_heads(rows):
    lane = lax.broadcasted_iota(jnp.int32, rows.shape, 1)
    return jnp.concatenate(
        [jnp.where(lane < KEY_DIM, rows, 0.0), jnp.where(lane >= KEY_DIM, rows, 0.0)], axis=0
    ).astype(jnp.bfloat16)


def within_kernel(
    queries_ref, keys_ref, values_ref, logits_ref, head_gain_ref, out_gate_ref, partial_ref, reach_ref, gating_ref
):
    for h in range(out_gate_ref.shape[1] // VALUE_DIM):
        place = slice(h * VALUE_DIM, (h + 1) * VALUE_DIM)
        gate = out_gate_ref[:, place].astype(jnp.float32)
        gating_ref[:, place] = head_gain_ref[...] * (gate / (1.0 + jnp.exp(-gate)))
    length, channels = keys_ref.shape
    blocks = length // BLOCK
    pairs = channels // LANES
    running_all = running_sums(logits_ref[...].astype(jnp.float32))
    states = [jnp.zeros((VALUE_DIM, LANES), jnp.float32)] * pairs
    lead = jnp.zeros((1, channels), jnp.float32)
    row = lax.broadcasted_iota(jnp.int32, (2 * BLOCK, BLOCK), 0)
    column = lax.broadcasted_iota(jnp.int32, (2 * BLOCK, BLOCK), 1)
    causal = (row & (BLOCK - 1)) >= column
    for n in range(blocks):
        rows = slice(n * BLOCK, (n + 1) * BLOCK)
        running = running_all[rows]
        query_scaled = queries_ref[rows].astype(jnp.float32) * KEY_DIM ** (-0.5) * jnp.exp(running)
        key_inverse = (keys_ref[rows].astype(jnp.float32) * jnp.exp(-running)).astype(jnp.bfloat16)
        reach_ref[rows] = query_scaled * jnp.exp(lead)
        lead = lead + running[BLOCK - 1 : BLOCK]
        for p in range(pairs):
            lanes = slice(p * LANES, (p + 1) * LANES)
            masked = masked_heads(query_scaled[:, lanes])
            scores = jnp.where(causal, product(masked, key_inverse[:, lanes], 1, 1), 0.0).astype(jnp.bfloat16)
            carried = product(masked, states[p].astype(jnp.bfloat16), 1, 1)
            for h in range(2):
                place = slice((2 * p + h) * VALUE_DIM, (2 * p + h + 1) * VALUE_DIM)
                part = slice(h * BLOCK, (h + 1) * BLOCK)
                partial_ref[rows, place] = product(scores[part], values_ref[rows, place]) + carried[part]
        if n + 1 < blocks:
            states = grow(states, n, running_all, keys_ref, values_ref)


def finish_kernel(
    place_ref, plane_ref, back1_ref, back2_ref, back3_ref, before_y_ref, decay_y_ref, before_x_ref, decay_x_ref,
    partial_ref, reach_ref, gating_ref, kept_ref, given_ref, whole,
):
    core, plane = place_ref[0], plane_ref[0]
    length, channels = reach_ref.shape
    pairs = channels // LANES
    received = [unpack(ref) for ref in (back1_ref, back2_ref, back3_ref)]
    half = length // 2
    for p in range(pairs):
        lanes = slice(p * LANES, (p + 1) * LANES)
        rows = slice(p * VALUE_DIM, (p + 1) * VALUE_DIM)
        state = jnp.zeros((VALUE_DIM, LANES), jnp.float32)
        for k in (3, 2, 1):
            decay, grown = received[k - 1][0][p], received[k - 1][1][p]
            state = jnp.where(plane >= k, decay * state + grown, state)
        state = before_y_ref[rows] + decay_y_ref[p * 8 : p * 8 + 1] * state
        state = before_x_ref[rows] + decay_x_ref[p * 8 : p * 8 + 1] * state
        carried = product(masked_heads(reach_ref[:, lanes]), state.astype(jnp.bfloat16), 1, 1)
        for h in range(2):
            place = slice((2 * p + h) * VALUE_DIM, (2 * p + h + 1) * VALUE_DIM)
            attended = partial_ref[:, place] + carried[h * length : (h + 1) * length]
            scale = lax.rsqrt(jnp.mean(attended * attended, axis=1, keepdims=True) + 1e-06)
            result = (attended * scale * gating_ref[:, place]).astype(jnp.bfloat16)
            whole[0, :, place] = result[:half]
            whole[1, :, place] = result[half:]
    kept_ref[...] = whole[core]
    given_ref[...] = whole[1 - core]


def project_kernel(
    place_ref, owners_vmem, kept_ref, taken_ref, weight_ref, residual_ref, norm_gain_ref, merged_ref, outgoing_ref,
    chunked, owners_ref, sem,
):
    indices = pltpu.make_async_copy(owners_vmem, owners_ref, sem.at[0])
    indices.start()
    core = place_ref[0]
    rows, width = residual_ref.shape
    depth = kept_ref.shape[1]
    tile = 256
    own = pl.ds(pl.multiple_of(core * depth, depth), depth)
    other = pl.ds(pl.multiple_of((1 - core) * depth, depth), depth)
    square = jnp.zeros((rows, 1), jnp.float32)
    for n in range(width // tile):
        part = slice(n * tile, (n + 1) * tile)
        projected = product(kept_ref[...], weight_ref[own, part]) + product(taken_ref[...], weight_ref[other, part])
        merged = (residual_ref[:, part].astype(jnp.float32) + projected).astype(jnp.bfloat16)
        merged_ref[:, part] = merged
        widened = merged.astype(jnp.float32)
        square = square + jnp.sum(widened * widened, axis=1, keepdims=True)
    scale = lax.rsqrt(square / width + 1e-06)
    swap = swap_matrix()
    for g in range(0, rows // SUB, 2):
        blocks = []
        for k in (g, g + 1):
            group = slice(k * SUB, (k + 1) * SUB)
            stacked = []
            for j in range(width // LANES):
                lanes = slice(j * LANES, (j + 1) * LANES)
                widened = merged_ref[group, lanes].astype(jnp.float32)
                stacked.append((widened * scale[group] * norm_gain_ref[:, lanes]).astype(jnp.bfloat16))
            blocks.append(jnp.concatenate(stacked, axis=0))
        for k, turned in zip((g, g + 1), exchange(swap, blocks)):
            chunked[k * SUB : (k + 1) * SUB] = turned.astype(jnp.bfloat16).reshape(SUB, SUB, LANES)

    experts_total = owners_ref.shape[1]
    capacity = outgoing_ref.shape[0] // experts_total

    batch = 8
    indices.wait()

    def copy_rows(step, carry):
        first = step * batch
        rows = [chunked[owners_ref[place, first + k]] for k in range(batch) for place in range(capacity)]
        for k, row in enumerate(rows):
            outgoing_ref[capacity * first + k] = row
        return carry

    lax.fori_loop(0, experts_total // batch, copy_rows, 0, unroll=2)


def shape_of(shape, dtype):
    return jax.ShapeDtypeStruct(shape, dtype)


def limited(mebibytes):
    return pltpu.CompilerParams(vmem_limit_bytes=int(mebibytes * 1048576))


def call(kernel, outs, operands, scalars=0, scratch=(), cost=10000000, room=6, far=False):
    return pl.pallas_call(
        kernel,
        out_shape=outs,
        in_specs=[SMEM_SPEC] * scalars + [ANY_SPEC if far else VMEM_SPEC] * (len(operands) - scalars),
        out_specs=jax.tree.map(lambda _: VMEM_SPEC, outs),
        scratch_shapes=list(scratch),
        cost_estimate=pl.CostEstimate(flops=cost * 400, bytes_accessed=cost, transcendentals=0),
        compiler_params=limited(room),
    )(*operands)


def from_behind(message, axis):
    moved = []
    for k in range(1, RING):
        moved.append(lax.ppermute(message, axis, [(i, (i + k) % RING) for i in range(RING)]))
    return moved


def local(
    residual,
    queries,
    key_rows,
    value_rows,
    out_gate,
    gate_logits,
    head_gain,
    out_weight,
    norm_gain,
    routes,
    group_score,
    expert_score,
    gate_weight,
    up_weight,
    down_weight,
):
    row_count, model_width = residual.shape
    length, channels = queries.shape
    values = value_rows.shape[1]
    f32, bf16 = jnp.float32, jnp.bfloat16
    z, y, x, core = (lax.axis_index(axis).astype(jnp.int32).reshape(1) for axis in SP_TP)
    pairs = channels // LANES
    message_shape = shape_of((pairs * VALUE_DIM + SUB, LANES), bf16)
    state_shape = shape_of((pairs * VALUE_DIM, LANES), f32)
    decay_shape = shape_of((pairs * 8, LANES), f32)
    message = call(
        state_kernel,
        message_shape,
        (key_rows, value_rows, gate_logits),
        scratch=[
            pltpu.VMEM(key_rows.shape, bf16),
            pltpu.VMEM(value_rows.shape, bf16),
            pltpu.VMEM(gate_logits.shape, bf16),
            pltpu.SemaphoreType.DMA((3,)),
        ],
        room=53.8,
        far=True,
    )
    experts_total = lax.axis_size(SP_TP)
    capacity = 3 * row_count // experts_total
    slots, owners, weights = routing(routes, group_score, expert_score)
    behind = from_behind(message, "sp_2")
    slots, owners, weights, *behind = lax.optimization_barrier((slots, owners, weights, *behind))
    before_x, decay_x, message_x = call(
        stage_kernel, (state_shape, decay_shape, message_shape), (x, message, *behind), 1
    )
    partial, reach, gating = call(
        within_kernel,
        (shape_of((length, values), f32), shape_of((length, channels), f32), shape_of((length, values), f32)),
        (queries, key_rows, value_rows, gate_logits, head_gain.reshape(1, -1), out_gate),
    )
    behind = from_behind(message_x, "sp_1")
    partial, reach, gating, *behind = lax.optimization_barrier((partial, reach, gating, *behind))
    before_y, decay_y, message_y = call(
        stage_kernel, (state_shape, decay_shape, message_shape), (y, message_x, *behind), 1
    )
    behind = from_behind(message_y, "sp_0")
    half = shape_of((length // 2, values), bf16)
    kept, given = call(
        finish_kernel,
        (half, half),
        (core, z, *behind, before_y, decay_y, before_x, decay_x, partial, reach, gating),
        2,
        [pltpu.VMEM((2, length // 2, values), bf16)],
    )
    taken = lax.ppermute(given, "tp", [(0, 1), (1, 0)])
    merged, outgoing = call(
        project_kernel,
        (
            shape_of((row_count, model_width), bf16),
            shape_of((experts_total * capacity, SUB, LANES), bf16),
        ),
        (core, owners, kept, taken, out_weight, residual, norm_gain.reshape(1, -1)),
        1,
        [
            pltpu.VMEM((row_count, SUB, LANES), bf16),
            pltpu.SMEM(owners.shape, jnp.int32),
            pltpu.SemaphoreType.DMA((1,)),
        ],
        room=14,
    )
    block = (experts_total, capacity * SUB, LANES)
    arrived = lax.all_to_all(outgoing.reshape(block), SP_TP, split_axis=0, concat_axis=0, tiled=True)
    served = experts(arrived.reshape(outgoing.shape), gate_weight, up_weight, down_weight)
    returned = lax.all_to_all(served.reshape(block), SP_TP, split_axis=0, concat_axis=0, tiled=True)
    return combine(slots, returned.reshape(outgoing.shape), merged, weights)


def solution(mesh):
    torus = Mesh(mesh.devices.reshape(4, 4, 4, mesh.shape["tp"]), ("sp_0", "sp_1", "sp_2", "tp"))
    in_specs = (
        P(SP_TP, None),
        P(SP, "tp"),
        P(SP, "tp"),
        P(SP, "tp"),
        P(SP, "tp"),
        P(SP, "tp"),
        P(),
        P(),
        P(),
        P(SP_TP, None),
        P(SP_TP),
        P(SP_TP, None),
        P(SP_TP, None, None),
        P(SP_TP, None, None),
        P(SP_TP, None, None),
    )
    out_specs = P(SP_TP, None)
    return jax.shard_map(local, mesh=torus, in_specs=in_specs, out_specs=out_specs, check_vma=False)
```

```python
import jax
import jax.numpy as jnp
from jax import lax
from jax.experimental import pallas as pl
from jax.experimental.pallas import tpu as pltpu
from jax.sharding import Mesh
from jax.sharding import PartitionSpec as P

KEY_DIM = 64
VALUE_DIM = 128
BLOCK = 64
RING = 4
SP = ("sp_0", "sp_1", "sp_2")
SP_TP = ("sp_0", "sp_1", "sp_2", "tp")


VMEM_SPEC = pl.BlockSpec(memory_space=pltpu.VMEM)
SMEM_SPEC = pl.BlockSpec(memory_space=pltpu.SMEM)
ANY_SPEC = pl.BlockSpec(memory_space=pl.ANY)
SUB = 16
LANES = 128
SWAP = SUB * SUB


def swap_matrix():
    row = lax.broadcasted_iota(jnp.int32, (SWAP, SWAP), 0)
    column = lax.broadcasted_iota(jnp.int32, (SWAP, SWAP), 1)
    partner = (row & (SUB - 1)) * SUB + (row >> 4)
    return (partner == column).astype(jnp.float32).astype(jnp.bfloat16)


def exchange(swap, blocks):
    turned = jnp.dot(swap, jnp.concatenate(blocks, axis=1), preferred_element_type=jnp.float32)
    return [turned[:, k * LANES : (k + 1) * LANES] for k in range(len(blocks))]


def stack_chunks(ref, g):
    width = ref.shape[1]
    return jnp.concatenate(
        [ref[g * SUB : (g + 1) * SUB, j * LANES : (j + 1) * LANES] for j in range(width // LANES)], axis=0
    )


def routing_kernel(routes_ref, group_ref, expert_ref, slots_ref, owners_ref, weights_ref):
    choices, rows = routes_ref.shape
    capacity = 3
    bf16 = jnp.bfloat16
    expert = lax.broadcasted_iota(jnp.int32, (LANES, rows), 0)
    token = lax.broadcasted_iota(jnp.int32, (LANES, rows), 1)
    named = [expert == routes_ref[k : k + 1] for k in range(choices)]
    named = [one.astype(jnp.float32) for one in named]
    source = lax.broadcasted_iota(jnp.int32, (rows, rows), 0)
    target = lax.broadcasted_iota(jnp.int32, (rows, rows), 1)
    before = (source < target).astype(jnp.float32).astype(bf16)
    used = jnp.dot(sum(named).astype(bf16), before, preferred_element_type=jnp.float32)
    place = lax.broadcasted_iota(jnp.int32, (8, rows), 0).astype(jnp.float32)
    name = lax.broadcasted_iota(jnp.int32, (8, rows), 1).astype(jnp.float32)
    owners = jnp.zeros((8, LANES), jnp.float32)
    for k in range(choices):
        rank = jnp.sum(named[k] * used, axis=0, keepdims=True)
        slots_ref[k : k + 1] = routes_ref[k : k + 1] * capacity + rank.astype(jnp.int32)
        owned = jnp.where(place == rank, name, 0.0).astype(bf16)
        owners = owners + lax.dot_general(
            owned, named[k].astype(bf16), (((1,), (1,)), ((), ())), preferred_element_type=jnp.float32
        )
    owners_ref[...] = owners.astype(jnp.int32)
    score = expert_ref[...]
    weights = group_ref[...] * score / jnp.sum(score, axis=0, keepdims=True)
    for k in range(choices):
        spread = jnp.broadcast_to(weights[k : k + 1], (LANES, rows))
        weights_ref[k] = spread.T


def routing(routes, group_score, expert_score):
    rows, choices = routes.shape
    return call(
        routing_kernel,
        (
            shape_of((choices, rows), jnp.int32),
            shape_of((8, LANES), jnp.int32),
            shape_of((choices, rows, LANES), jnp.float32),
        ),
        (routes.T, group_score.reshape(1, rows), expert_score.T),
        room=2,
    )


def experts_kernel(rows_ref, gate, up, down, out_ref, rows_in, inner, served):
    swap = swap_matrix()
    count, width = rows_in.shape
    hidden = inner.shape[1]
    groups = count // SUB
    for g in range(0, groups, 2):
        blocks = [rows_ref[k * SUB : (k + 1) * SUB].reshape(SWAP, LANES) for k in (g, g + 1)]
        for k, turned in zip((g, g + 1), exchange(swap, blocks)):
            turned = turned.astype(jnp.bfloat16)
            for j in range(width // LANES):
                rows_in[k * SUB : (k + 1) * SUB, j * LANES : (j + 1) * LANES] = turned[j * SUB : (j + 1) * SUB]
    tile = 256
    for n in range(hidden // tile):
        part = slice(n * tile, (n + 1) * tile)
        gated = jnp.dot(rows_in[...], gate[0, :, part], preferred_element_type=jnp.float32)
        lifted = jnp.dot(rows_in[...], up[0, :, part], preferred_element_type=jnp.float32)
        inner[:, part] = (gated / (1.0 + jnp.exp(-gated)) * lifted).astype(jnp.bfloat16)
    for n in range(width // tile):
        part = slice(n * tile, (n + 1) * tile)
        served[:, part] = jnp.dot(inner[...], down[0, :, part], preferred_element_type=jnp.float32).astype(jnp.bfloat16)
    for g in range(0, groups, 2):
        blocks = [stack_chunks(served, k) for k in (g, g + 1)]
        for k, turned in zip((g, g + 1), exchange(swap, blocks)):
            out_ref[k * SUB : (k + 1) * SUB] = turned.astype(jnp.bfloat16).reshape(SUB, SUB, LANES)


def experts(arrived, gate_weight, up_weight, down_weight):
    count = arrived.shape[0]
    width, hidden = gate_weight.shape[1:]
    return pl.pallas_call(
        experts_kernel,
        out_shape=jax.ShapeDtypeStruct(arrived.shape, jnp.bfloat16),
        in_specs=[VMEM_SPEC] * 4,
        out_specs=VMEM_SPEC,
        scratch_shapes=[
            pltpu.VMEM((count, width), jnp.bfloat16),
            pltpu.VMEM((count, hidden), jnp.bfloat16),
            pltpu.VMEM((count, width), jnp.bfloat16),
        ],
        compiler_params=limited(16),
        name="experts",
    )(arrived, gate_weight, up_weight, down_weight)


def combine_kernel(slots_vmem, returned_ref, merged_ref, weights_ref, out_hbm, out_ref, slots_ref, sem, sems):
    indices = pltpu.make_async_copy(slots_vmem, slots_ref, sem.at[0])
    indices.start()
    swap = swap_matrix()
    rows, width = merged_ref.shape
    indices.wait()
    copies = []
    for g in range(rows // SUB):
        group = slice(g * SUB, (g + 1) * SUB)
        picked = [
            jnp.concatenate([returned_ref[slots_ref[k, g * SUB + i]] for i in range(SUB)], axis=0) for k in range(2)
        ]
        first, second = exchange(swap, picked)
        for j in range(width // LANES):
            lanes = slice(j * LANES, (j + 1) * LANES)
            part = slice(j * SUB, (j + 1) * SUB)
            total = weights_ref[0, group] * first[part] + weights_ref[1, group] * second[part]
            out_ref[group, lanes] = (merged_ref[group, lanes].astype(jnp.float32) + total).astype(jnp.bfloat16)
        if g % 2 == 1:
            both = pl.ds((g - 1) * SUB, 2 * SUB)
            copies.append(pltpu.make_async_copy(out_ref.at[both], out_hbm.at[both], sems.at[g // 2]))
            copies[-1].start()
    for copy in copies:
        copy.wait()


def combine(slots, returned, merged, weights):
    rows = merged.shape[0]
    return pl.pallas_call(
        combine_kernel,
        out_shape=shape_of(merged.shape, jnp.bfloat16),
        in_specs=[VMEM_SPEC] * 4,
        out_specs=ANY_SPEC,
        scratch_shapes=[
            pltpu.VMEM(merged.shape, jnp.bfloat16),
            pltpu.SMEM(slots.shape, jnp.int32),
            pltpu.SemaphoreType.DMA((1,)),
            pltpu.SemaphoreType.DMA((rows // SUB // 2,)),
        ],
        compiler_params=limited(8),
        name="combine",
    )(slots, returned, merged, weights)


def pieces(value, count):
    parts = []
    for _ in range(count):
        part = value.astype(jnp.bfloat16)
        parts.append(part)
        value = value - part.astype(jnp.float32)
    return parts


def product(left, right, left_dim=1, right_dim=0):
    return lax.dot_general(
        left, right, (((left_dim,), (right_dim,)), ((), ())), preferred_element_type=jnp.float32
    )


def running_sums(logits):
    length = logits.shape[0]
    decay_log = (jnp.minimum(logits, 0.0) - jnp.log1p(jnp.exp(-jnp.abs(logits)))) / 16.0
    parts = pieces(decay_log, 3)
    row = lax.broadcasted_iota(jnp.int32, (length, length), 0)
    column = lax.broadcasted_iota(jnp.int32, (length, length), 1)
    earlier = (row >= column) & (row // BLOCK == column // BLOCK)
    earlier = earlier.astype(jnp.float32).astype(jnp.bfloat16)
    return sum(product(earlier, part) for part in parts)


def grow(states, n, running, keys_ref, values_ref):
    wide = 2 * VALUE_DIM
    rows = slice(n * BLOCK, (n + 1) * BLOCK)
    closing = running[(n + 1) * BLOCK - 1 : (n + 1) * BLOCK]
    key_closing = keys_ref[rows].astype(jnp.float32) * jnp.exp(closing - running[rows])
    key_closing = key_closing.astype(jnp.bfloat16)
    decay = jnp.exp(closing)
    lane = lax.broadcasted_iota(jnp.int32, (VALUE_DIM, LANES), 1)
    after = []
    for p, state in enumerate(states):
        lanes = slice(p * LANES, (p + 1) * LANES)
        grown = product(values_ref[rows, p * wide : (p + 1) * wide], key_closing[:, lanes], 0, 0)
        grown = jnp.where(lane < KEY_DIM, grown[:VALUE_DIM], grown[VALUE_DIM:])
        after.append(decay[:, lanes] * state + grown)
    return after


def state_kernel(keys_hbm, values_hbm, logits_hbm, message_ref, keys_ref, values_ref, logits_ref, sems):
    copies = [
        pltpu.make_async_copy(source, target, sems.at[k])
        for k, (source, target) in enumerate(
            ((logits_hbm, logits_ref), (keys_hbm, keys_ref), (values_hbm, values_ref))
        )
    ]
    for copy in copies:
        copy.start()
    copies[0].wait()
    length, channels = keys_ref.shape
    blocks = length // BLOCK
    pairs = channels // LANES
    running = running_sums(logits_ref[...].astype(jnp.float32))
    copies[1].wait()
    copies[2].wait()
    states = [jnp.zeros((VALUE_DIM, LANES), jnp.float32)] * pairs
    total = jnp.zeros((1, channels), jnp.float32)
    for n in range(blocks):
        total = total + running[(n + 1) * BLOCK - 1 : (n + 1) * BLOCK]
        states = grow(states, n, running, keys_ref, values_ref)
    for p in range(pairs):
        message_ref[p * VALUE_DIM : (p + 1) * VALUE_DIM] = states[p].astype(jnp.bfloat16)
    message_ref[pairs * VALUE_DIM :] = pack_decay(jnp.exp(total))


def pack_decay(decay):
    pairs = decay.shape[1] // LANES
    place = lax.broadcasted_iota(jnp.int32, (SUB, LANES), 0)
    high, low = pieces(decay, 2)
    packed = jnp.zeros((SUB, LANES), jnp.float32)
    for p in range(pairs):
        lanes = slice(p * LANES, (p + 1) * LANES)
        packed = jnp.where(place == p, high[:, lanes].astype(jnp.float32), packed)
        packed = jnp.where(place == pairs + p, low[:, lanes].astype(jnp.float32), packed)
    return packed.astype(jnp.bfloat16)


def unpack(message_ref):
    states = message_ref.shape[0] - SUB
    pairs = states // VALUE_DIM
    packed = message_ref[states:].astype(jnp.float32)
    decays = [packed[p : p + 1] + packed[pairs + p : pairs + p + 1] for p in range(pairs)]
    return decays, [message_ref[p * VALUE_DIM : (p + 1) * VALUE_DIM].astype(jnp.float32) for p in range(pairs)]


def stage_kernel(place_ref, own_ref, back1_ref, back2_ref, back3_ref, before_ref, decay_ref, message_ref):
    place = place_ref[0]
    own_decays, own_states = unpack(own_ref)
    pairs = len(own_decays)
    received = [unpack(ref) for ref in (back1_ref, back2_ref, back3_ref)]
    whole = []
    for p in range(pairs):
        rows = slice(p * VALUE_DIM, (p + 1) * VALUE_DIM)
        before = jnp.zeros((VALUE_DIM, LANES), jnp.float32)
        decay = jnp.ones((1, LANES), jnp.float32)
        for k in (3, 2, 1):
            valid = place >= k
            passed, state = received[k - 1][0][p], received[k - 1][1][p]
            before = jnp.where(valid, passed * before + state, before)
            decay = jnp.where(valid, passed * decay, decay)
        before_ref[rows] = before
        decay_ref[p * 8 : (p + 1) * 8] = jnp.broadcast_to(decay, (8, LANES))
        total = own_decays[p] * before + own_states[p]
        for k in (3, 2, 1):
            later = place < k
            passed, state = received[k - 1][0][p], received[k - 1][1][p]
            total = jnp.where(later, passed * total + state, total)
        message_ref[rows] = total.astype(jnp.bfloat16)
        whole.append(own_decays[p] * received[0][0][p] * received[1][0][p] * received[2][0][p])
    message_ref[pairs * VALUE_DIM :] = pack_decay(jnp.concatenate(whole, axis=1))


def masked_heads(rows):
    lane = lax.broadcasted_iota(jnp.int32, rows.shape, 1)
    return jnp.concatenate(
        [jnp.where(lane < KEY_DIM, rows, 0.0), jnp.where(lane >= KEY_DIM, rows, 0.0)], axis=0
    ).astype(jnp.bfloat16)


def within_kernel(
    queries_ref, keys_ref, values_ref, logits_ref, head_gain_ref, out_gate_ref, partial_ref, reach_ref, gating_ref
):
    for h in range(out_gate_ref.shape[1] // VALUE_DIM):
        place = slice(h * VALUE_DIM, (h + 1) * VALUE_DIM)
        gate = out_gate_ref[:, place].astype(jnp.float32)
        gating_ref[:, place] = head_gain_ref[...] * (gate / (1.0 + jnp.exp(-gate)))
    length, channels = keys_ref.shape
    blocks = length // BLOCK
    pairs = channels // LANES
    running_all = running_sums(logits_ref[...].astype(jnp.float32))
    states = [jnp.zeros((VALUE_DIM, LANES), jnp.float32)] * pairs
    lead = jnp.zeros((1, channels), jnp.float32)
    row = lax.broadcasted_iota(jnp.int32, (2 * BLOCK, BLOCK), 0)
    column = lax.broadcasted_iota(jnp.int32, (2 * BLOCK, BLOCK), 1)
    causal = (row & (BLOCK - 1)) >= column
    for n in range(blocks):
        rows = slice(n * BLOCK, (n + 1) * BLOCK)
        running = running_all[rows]
        query_scaled = queries_ref[rows].astype(jnp.float32) * KEY_DIM ** (-0.5) * jnp.exp(running)
        key_inverse = (keys_ref[rows].astype(jnp.float32) * jnp.exp(-running)).astype(jnp.bfloat16)
        reach_ref[rows] = query_scaled * jnp.exp(lead)
        lead = lead + running[BLOCK - 1 : BLOCK]
        for p in range(pairs):
            lanes = slice(p * LANES, (p + 1) * LANES)
            masked = masked_heads(query_scaled[:, lanes])
            scores = jnp.where(causal, product(masked, key_inverse[:, lanes], 1, 1), 0.0).astype(jnp.bfloat16)
            carried = product(masked, states[p].astype(jnp.bfloat16), 1, 1)
            for h in range(2):
                place = slice((2 * p + h) * VALUE_DIM, (2 * p + h + 1) * VALUE_DIM)
                part = slice(h * BLOCK, (h + 1) * BLOCK)
                partial_ref[rows, place] = product(scores[part], values_ref[rows, place]) + carried[part]
        if n + 1 < blocks:
            states = grow(states, n, running_all, keys_ref, values_ref)


def finish_kernel(
    place_ref, plane_ref, back1_ref, back2_ref, back3_ref, before_y_ref, decay_y_ref, before_x_ref, decay_x_ref,
    partial_ref, reach_ref, gating_ref, kept_ref, given_ref, whole,
):
    core, plane = place_ref[0], plane_ref[0]
    length, channels = reach_ref.shape
    pairs = channels // LANES
    received = [unpack(ref) for ref in (back1_ref, back2_ref, back3_ref)]
    half = length // 2
    for p in range(pairs):
        lanes = slice(p * LANES, (p + 1) * LANES)
        rows = slice(p * VALUE_DIM, (p + 1) * VALUE_DIM)
        state = jnp.zeros((VALUE_DIM, LANES), jnp.float32)
        for k in (3, 2, 1):
            decay, grown = received[k - 1][0][p], received[k - 1][1][p]
            state = jnp.where(plane >= k, decay * state + grown, state)
        state = before_y_ref[rows] + decay_y_ref[p * 8 : p * 8 + 1] * state
        state = before_x_ref[rows] + decay_x_ref[p * 8 : p * 8 + 1] * state
        carried = product(masked_heads(reach_ref[:, lanes]), state.astype(jnp.bfloat16), 1, 1)
        for h in range(2):
            place = slice((2 * p + h) * VALUE_DIM, (2 * p + h + 1) * VALUE_DIM)
            attended = partial_ref[:, place] + carried[h * length : (h + 1) * length]
            scale = lax.rsqrt(jnp.mean(attended * attended, axis=1, keepdims=True) + 1e-06)
            result = (attended * scale * gating_ref[:, place]).astype(jnp.bfloat16)
            whole[0, :, place] = result[:half]
            whole[1, :, place] = result[half:]
    kept_ref[...] = whole[core]
    given_ref[...] = whole[1 - core]


def own_kernel(place_ref, kept_ref, weight_ref, residual_ref, partial_ref):
    core = place_ref[0]
    depth = kept_ref.shape[1]
    tile = 256
    own = pl.ds(pl.multiple_of(core * depth, depth), depth)
    for n in range(residual_ref.shape[1] // tile):
        part = slice(n * tile, (n + 1) * tile)
        partial_ref[:, part] = residual_ref[:, part].astype(jnp.float32) + product(kept_ref[...], weight_ref[own, part])


def project_kernel(
    place_ref, owners_vmem, taken_ref, weight_ref, partial_ref, norm_gain_ref, merged_ref, outgoing_ref,
    chunked, owners_ref, sem,
):
    indices = pltpu.make_async_copy(owners_vmem, owners_ref, sem.at[0])
    indices.start()
    core = place_ref[0]
    rows, width = partial_ref.shape
    depth = taken_ref.shape[1]
    tile = 256
    other = pl.ds(pl.multiple_of((1 - core) * depth, depth), depth)
    square = jnp.zeros((rows, 1), jnp.float32)
    for n in range(width // tile):
        part = slice(n * tile, (n + 1) * tile)
        merged = (partial_ref[:, part] + product(taken_ref[...], weight_ref[other, part])).astype(jnp.bfloat16)
        merged_ref[:, part] = merged
        widened = merged.astype(jnp.float32)
        square = square + jnp.sum(widened * widened, axis=1, keepdims=True)
    scale = lax.rsqrt(square / width + 1e-06)
    swap = swap_matrix()
    for g in range(0, rows // SUB, 2):
        blocks = []
        for k in (g, g + 1):
            group = slice(k * SUB, (k + 1) * SUB)
            stacked = []
            for j in range(width // LANES):
                lanes = slice(j * LANES, (j + 1) * LANES)
                widened = merged_ref[group, lanes].astype(jnp.float32)
                stacked.append((widened * scale[group] * norm_gain_ref[:, lanes]).astype(jnp.bfloat16))
            blocks.append(jnp.concatenate(stacked, axis=0))
        for k, turned in zip((g, g + 1), exchange(swap, blocks)):
            chunked[k * SUB : (k + 1) * SUB] = turned.astype(jnp.bfloat16).reshape(SUB, SUB, LANES)

    experts_total = owners_ref.shape[1]
    capacity = outgoing_ref.shape[0] // experts_total

    indices.wait()
    batch = 8
    for first in range(0, experts_total, batch):
        rows = [chunked[owners_ref[place, first + k]] for k in range(batch) for place in range(capacity)]
        for k, row in enumerate(rows):
            outgoing_ref[capacity * first + k] = row


def shape_of(shape, dtype):
    return jax.ShapeDtypeStruct(shape, dtype)


def limited(mebibytes):
    return pltpu.CompilerParams(vmem_limit_bytes=int(mebibytes * 1048576))


def call(kernel, outs, operands, scalars=0, scratch=(), cost=10000000, room=6, far=False):
    return pl.pallas_call(
        kernel,
        out_shape=outs,
        in_specs=[SMEM_SPEC] * scalars + [ANY_SPEC if far else VMEM_SPEC] * (len(operands) - scalars),
        out_specs=jax.tree.map(lambda _: VMEM_SPEC, outs),
        scratch_shapes=list(scratch),
        cost_estimate=pl.CostEstimate(flops=cost * 400, bytes_accessed=cost, transcendentals=0),
        compiler_params=limited(room),
    )(*operands)


def from_behind(message, axis):
    moved = []
    for k in range(1, RING):
        moved.append(lax.ppermute(message, axis, [(i, (i + k) % RING) for i in range(RING)]))
    return moved


def local(
    residual,
    queries,
    key_rows,
    value_rows,
    out_gate,
    gate_logits,
    head_gain,
    out_weight,
    norm_gain,
    routes,
    group_score,
    expert_score,
    gate_weight,
    up_weight,
    down_weight,
):
    row_count, model_width = residual.shape
    length, channels = queries.shape
    values = value_rows.shape[1]
    f32, bf16 = jnp.float32, jnp.bfloat16
    z, y, x, core = (lax.axis_index(axis).astype(jnp.int32).reshape(1) for axis in SP_TP)
    pairs = channels // LANES
    message_shape = shape_of((pairs * VALUE_DIM + SUB, LANES), bf16)
    state_shape = shape_of((pairs * VALUE_DIM, LANES), f32)
    decay_shape = shape_of((pairs * 8, LANES), f32)
    message = call(
        state_kernel,
        message_shape,
        (key_rows, value_rows, gate_logits),
        scratch=[
            pltpu.VMEM(key_rows.shape, bf16),
            pltpu.VMEM(value_rows.shape, bf16),
            pltpu.VMEM(gate_logits.shape, bf16),
            pltpu.SemaphoreType.DMA((3,)),
        ],
        room=53.8,
        far=True,
    )
    experts_total = lax.axis_size(SP_TP)
    capacity = 3 * row_count // experts_total
    slots, owners, weights = routing(routes, group_score, expert_score)
    behind = from_behind(message, "sp_2")
    slots, owners, weights, *behind = lax.optimization_barrier((slots, owners, weights, *behind))
    before_x, decay_x, message_x = call(
        stage_kernel, (state_shape, decay_shape, message_shape), (x, message, *behind), 1
    )
    behind = from_behind(message_x, "sp_1")
    before_y, decay_y, message_y = call(
        stage_kernel, (state_shape, decay_shape, message_shape), (y, message_x, *behind), 1
    )
    behind = from_behind(message_y, "sp_0")
    message_y, queries, key_rows = lax.optimization_barrier((message_y, queries, key_rows))
    partial, reach, gating = call(
        within_kernel,
        (shape_of((length, values), f32), shape_of((length, channels), f32), shape_of((length, values), f32)),
        (queries, key_rows, value_rows, gate_logits, head_gain.reshape(1, -1), out_gate),
    )
    partial, reach, gating, *behind = lax.optimization_barrier((partial, reach, gating, *behind))
    half = shape_of((length // 2, values), bf16)
    kept, given = call(
        finish_kernel,
        (half, half),
        (core, z, *behind, before_y, decay_y, before_x, decay_x, partial, reach, gating),
        2,
        [pltpu.VMEM((2, length // 2, values), bf16)],
        cost=300000,
    )
    taken = lax.ppermute(given, "tp", [(0, 1), (1, 0)])
    projected = call(own_kernel, shape_of((row_count, model_width), f32), (core, kept, out_weight, residual), 1, room=8)
    projected, taken = lax.optimization_barrier((projected, taken))
    merged, outgoing = call(
        project_kernel,
        (
            shape_of((row_count, model_width), bf16),
            shape_of((experts_total * capacity, SUB, LANES), bf16),
        ),
        (core, owners, taken, out_weight, projected, norm_gain.reshape(1, -1)),
        1,
        [
            pltpu.VMEM((row_count, SUB, LANES), bf16),
            pltpu.SMEM(owners.shape, jnp.int32),
            pltpu.SemaphoreType.DMA((1,)),
        ],
        room=14,
    )
    block = (experts_total, capacity * SUB, LANES)
    arrived = lax.all_to_all(outgoing.reshape(block), SP_TP, split_axis=0, concat_axis=0, tiled=True)
    served = experts(arrived.reshape(outgoing.shape), gate_weight, up_weight, down_weight)
    returned = lax.all_to_all(served.reshape(block), SP_TP, split_axis=0, concat_axis=0, tiled=True)
    return combine(slots, returned.reshape(outgoing.shape), merged, weights)


def solution(mesh):
    torus = Mesh(mesh.devices.reshape(4, 4, 4, mesh.shape["tp"]), ("sp_0", "sp_1", "sp_2", "tp"))
    in_specs = (
        P(SP_TP, None),
        P(SP, "tp"),
        P(SP, "tp"),
        P(SP, "tp"),
        P(SP, "tp"),
        P(SP, "tp"),
        P(),
        P(),
        P(),
        P(SP_TP, None),
        P(SP_TP),
        P(SP_TP, None),
        P(SP_TP, None, None),
        P(SP_TP, None, None),
        P(SP_TP, None, None),
    )
    out_specs = P(SP_TP, None)
    return jax.shard_map(local, mesh=torus, in_specs=in_specs, out_specs=out_specs, check_vma=False)
```

```python
import jax
import jax.numpy as jnp
from jax import lax
from jax.experimental import pallas as pl
from jax.experimental.pallas import tpu as pltpu
from jax.sharding import Mesh
from jax.sharding import PartitionSpec as P

KEY_DIM = 64
VALUE_DIM = 128
BLOCK = 64
RING = 4
SP = ("sp_0", "sp_1", "sp_2")
SP_TP = ("sp_0", "sp_1", "sp_2", "tp")


VMEM_SPEC = pl.BlockSpec(memory_space=pltpu.VMEM)
SMEM_SPEC = pl.BlockSpec(memory_space=pltpu.SMEM)
ANY_SPEC = pl.BlockSpec(memory_space=pl.ANY)
SUB = 16
LANES = 128
SWAP = SUB * SUB


def swap_matrix():
    row = lax.broadcasted_iota(jnp.int32, (SWAP, SWAP), 0)
    column = lax.broadcasted_iota(jnp.int32, (SWAP, SWAP), 1)
    partner = (row & (SUB - 1)) * SUB + (row >> 4)
    return (partner == column).astype(jnp.float32).astype(jnp.bfloat16)


def exchange(swap, blocks):
    turned = jnp.dot(swap, jnp.concatenate(blocks, axis=1), preferred_element_type=jnp.float32)
    return [turned[:, k * LANES : (k + 1) * LANES] for k in range(len(blocks))]


def turn(block):
    return jnp.transpose(block.reshape(SUB, SUB, LANES), (1, 0, 2)).reshape(SWAP, LANES)


def swap_groups(swap, blocks, by_matmul):
    return exchange(swap, blocks) if by_matmul else [turn(block) for block in blocks]


def stack_chunks(ref, g):
    width = ref.shape[1]
    return jnp.concatenate(
        [ref[g * SUB : (g + 1) * SUB, j * LANES : (j + 1) * LANES] for j in range(width // LANES)], axis=0
    )


def routing_kernel(routes_ref, group_ref, expert_ref, slots_ref, owners_ref, weights_ref):
    choices, rows = routes_ref.shape
    capacity = 3
    bf16 = jnp.bfloat16
    expert = lax.broadcasted_iota(jnp.int32, (LANES, rows), 0)
    token = lax.broadcasted_iota(jnp.int32, (LANES, rows), 1)
    named = [expert == routes_ref[k : k + 1] for k in range(choices)]
    named = [one.astype(jnp.float32) for one in named]
    source = lax.broadcasted_iota(jnp.int32, (rows, rows), 0)
    target = lax.broadcasted_iota(jnp.int32, (rows, rows), 1)
    before = (source < target).astype(jnp.float32).astype(bf16)
    used = jnp.dot(sum(named).astype(bf16), before, preferred_element_type=jnp.float32)
    place = lax.broadcasted_iota(jnp.int32, (8, rows), 0).astype(jnp.float32)
    name = lax.broadcasted_iota(jnp.int32, (8, rows), 1).astype(jnp.float32)
    owners = jnp.zeros((8, LANES), jnp.float32)
    for k in range(choices):
        rank = jnp.sum(named[k] * used, axis=0, keepdims=True)
        slots_ref[k : k + 1] = routes_ref[k : k + 1] * capacity + rank.astype(jnp.int32)
        owned = jnp.where(place == rank, name, 0.0).astype(bf16)
        owners = owners + lax.dot_general(
            owned, named[k].astype(bf16), (((1,), (1,)), ((), ())), preferred_element_type=jnp.float32
        )
    owners_ref[...] = owners.astype(jnp.int32)
    score = expert_ref[...]
    weights = group_ref[...] * score / jnp.sum(score, axis=0, keepdims=True)
    for k in range(choices):
        spread = jnp.broadcast_to(weights[k : k + 1], (LANES, rows))
        weights_ref[k] = spread.T


def routing(routes, group_score, expert_score):
    rows, choices = routes.shape
    return call(
        routing_kernel,
        (
            shape_of((choices, rows), jnp.int32),
            shape_of((8, LANES), jnp.int32),
            shape_of((choices, rows, LANES), jnp.float32),
        ),
        (routes.T, group_score.reshape(1, rows), expert_score.T),
        room=2,
    )


def experts_kernel(rows_ref, gate, up, down, out_ref, rows_in, inner, served):
    swap = swap_matrix()
    count, width = rows_in.shape
    hidden = inner.shape[1]
    groups = count // SUB
    for g in range(0, groups, 2):
        blocks = [rows_ref[k * SUB : (k + 1) * SUB].reshape(SWAP, LANES) for k in (g, g + 1)]
        for k, turned in zip((g, g + 1), swap_groups(swap, blocks, False)):
            turned = turned.astype(jnp.bfloat16)
            for j in range(width // LANES):
                rows_in[k * SUB : (k + 1) * SUB, j * LANES : (j + 1) * LANES] = turned[j * SUB : (j + 1) * SUB]
    tile = 256
    for n in range(hidden // tile):
        part = slice(n * tile, (n + 1) * tile)
        gated = jnp.dot(rows_in[...], gate[0, :, part], preferred_element_type=jnp.float32)
        lifted = jnp.dot(rows_in[...], up[0, :, part], preferred_element_type=jnp.float32)
        inner[:, part] = (gated / (1.0 + jnp.exp(-gated)) * lifted).astype(jnp.bfloat16)
    for n in range(width // tile):
        part = slice(n * tile, (n + 1) * tile)
        served[:, part] = jnp.dot(inner[...], down[0, :, part], preferred_element_type=jnp.float32).astype(jnp.bfloat16)
    for g in range(0, groups, 2):
        blocks = [stack_chunks(served, k) for k in (g, g + 1)]
        for k, turned in zip((g, g + 1), swap_groups(swap, blocks, False)):
            out_ref[k * SUB : (k + 1) * SUB] = turned.astype(jnp.bfloat16).reshape(SUB, SUB, LANES)


def experts(arrived, gate_weight, up_weight, down_weight):
    count = arrived.shape[0]
    width, hidden = gate_weight.shape[1:]
    return pl.pallas_call(
        experts_kernel,
        out_shape=jax.ShapeDtypeStruct(arrived.shape, jnp.bfloat16),
        in_specs=[VMEM_SPEC] * 4,
        out_specs=VMEM_SPEC,
        scratch_shapes=[
            pltpu.VMEM((count, width), jnp.bfloat16),
            pltpu.VMEM((count, hidden), jnp.bfloat16),
            pltpu.VMEM((count, width), jnp.bfloat16),
        ],
        compiler_params=limited(16),
        name="experts",
    )(arrived, gate_weight, up_weight, down_weight)


def combine_kernel(slots_vmem, returned_ref, merged_ref, weights_ref, out_hbm, out_ref, slots_ref, sem, sems):
    indices = pltpu.make_async_copy(slots_vmem, slots_ref, sem.at[0])
    indices.start()
    swap = swap_matrix()
    rows, width = merged_ref.shape
    indices.wait()
    copies = []
    for g in range(rows // SUB):
        group = slice(g * SUB, (g + 1) * SUB)
        picked = [
            jnp.concatenate([returned_ref[slots_ref[k, g * SUB + i]] for i in range(SUB)], axis=0) for k in range(2)
        ]
        first, second = exchange(swap, picked)
        for j in range(width // LANES):
            lanes = slice(j * LANES, (j + 1) * LANES)
            part = slice(j * SUB, (j + 1) * SUB)
            total = weights_ref[0, group] * first[part] + weights_ref[1, group] * second[part]
            out_ref[group, lanes] = (merged_ref[group, lanes].astype(jnp.float32) + total).astype(jnp.bfloat16)
        if g % 2 == 1:
            both = pl.ds((g - 1) * SUB, 2 * SUB)
            copies.append(pltpu.make_async_copy(out_ref.at[both], out_hbm.at[both], sems.at[g // 2]))
            copies[-1].start()
    for copy in copies:
        copy.wait()


def combine(slots, returned, merged, weights):
    rows = merged.shape[0]
    return pl.pallas_call(
        combine_kernel,
        out_shape=shape_of(merged.shape, jnp.bfloat16),
        in_specs=[VMEM_SPEC] * 4,
        out_specs=ANY_SPEC,
        scratch_shapes=[
            pltpu.VMEM(merged.shape, jnp.bfloat16),
            pltpu.SMEM(slots.shape, jnp.int32),
            pltpu.SemaphoreType.DMA((1,)),
            pltpu.SemaphoreType.DMA((rows // SUB // 2,)),
        ],
        compiler_params=limited(8),
        name="combine",
    )(slots, returned, merged, weights)


def pieces(value, count):
    parts = []
    for _ in range(count):
        part = value.astype(jnp.bfloat16)
        parts.append(part)
        value = value - part.astype(jnp.float32)
    return parts


def product(left, right, left_dim=1, right_dim=0):
    return lax.dot_general(
        left, right, (((left_dim,), (right_dim,)), ((), ())), preferred_element_type=jnp.float32
    )


def running_sums(logits):
    length = logits.shape[0]
    decay_log = (jnp.minimum(logits, 0.0) - jnp.log1p(jnp.exp(-jnp.abs(logits)))) / 16.0
    parts = pieces(decay_log, 3)
    row = lax.broadcasted_iota(jnp.int32, (length, length), 0)
    column = lax.broadcasted_iota(jnp.int32, (length, length), 1)
    earlier = (row >= column) & (row // BLOCK == column // BLOCK)
    earlier = earlier.astype(jnp.float32).astype(jnp.bfloat16)
    return sum(product(earlier, part) for part in parts)


def grow(states, n, running, keys_ref, values_ref):
    wide = 2 * VALUE_DIM
    rows = slice(n * BLOCK, (n + 1) * BLOCK)
    closing = running[(n + 1) * BLOCK - 1 : (n + 1) * BLOCK]
    key_closing = keys_ref[rows].astype(jnp.float32) * jnp.exp(closing - running[rows])
    key_closing = key_closing.astype(jnp.bfloat16)
    decay = jnp.exp(closing)
    lane = lax.broadcasted_iota(jnp.int32, (VALUE_DIM, LANES), 1)
    after = []
    for p, state in enumerate(states):
        lanes = slice(p * LANES, (p + 1) * LANES)
        grown = product(values_ref[rows, p * wide : (p + 1) * wide], key_closing[:, lanes], 0, 0)
        grown = jnp.where(lane < KEY_DIM, grown[:VALUE_DIM], grown[VALUE_DIM:])
        after.append(decay[:, lanes] * state + grown)
    return after


def state_kernel(keys_hbm, values_hbm, logits_hbm, message_ref, keys_ref, values_ref, logits_ref, sems):
    copies = [
        pltpu.make_async_copy(source, target, sems.at[k])
        for k, (source, target) in enumerate(
            ((logits_hbm, logits_ref), (keys_hbm, keys_ref), (values_hbm, values_ref))
        )
    ]
    for copy in copies:
        copy.start()
    copies[0].wait()
    length, channels = keys_ref.shape
    blocks = length // BLOCK
    pairs = channels // LANES
    running = running_sums(logits_ref[...].astype(jnp.float32))
    copies[1].wait()
    copies[2].wait()
    states = [jnp.zeros((VALUE_DIM, LANES), jnp.float32)] * pairs
    total = jnp.zeros((1, channels), jnp.float32)
    for n in range(blocks):
        total = total + running[(n + 1) * BLOCK - 1 : (n + 1) * BLOCK]
        states = grow(states, n, running, keys_ref, values_ref)
    for p in range(pairs):
        message_ref[p * VALUE_DIM : (p + 1) * VALUE_DIM] = states[p].astype(jnp.bfloat16)
    message_ref[pairs * VALUE_DIM :] = pack_decay(jnp.exp(total))


def pack_decay(decay):
    pairs = decay.shape[1] // LANES
    place = lax.broadcasted_iota(jnp.int32, (SUB, LANES), 0)
    high, low = pieces(decay, 2)
    packed = jnp.zeros((SUB, LANES), jnp.float32)
    for p in range(pairs):
        lanes = slice(p * LANES, (p + 1) * LANES)
        packed = jnp.where(place == p, high[:, lanes].astype(jnp.float32), packed)
        packed = jnp.where(place == pairs + p, low[:, lanes].astype(jnp.float32), packed)
    return packed.astype(jnp.bfloat16)


def unpack(message_ref):
    states = message_ref.shape[0] - SUB
    pairs = states // VALUE_DIM
    packed = message_ref[states:].astype(jnp.float32)
    decays = [packed[p : p + 1] + packed[pairs + p : pairs + p + 1] for p in range(pairs)]
    return decays, [message_ref[p * VALUE_DIM : (p + 1) * VALUE_DIM].astype(jnp.float32) for p in range(pairs)]


def stage_kernel(place_ref, own_ref, back1_ref, back2_ref, back3_ref, before_ref, decay_ref, message_ref):
    place = place_ref[0]
    own_decays, own_states = unpack(own_ref)
    pairs = len(own_decays)
    received = [unpack(ref) for ref in (back1_ref, back2_ref, back3_ref)]
    whole = []
    for p in range(pairs):
        rows = slice(p * VALUE_DIM, (p + 1) * VALUE_DIM)
        before = jnp.zeros((VALUE_DIM, LANES), jnp.float32)
        decay = jnp.ones((1, LANES), jnp.float32)
        for k in (3, 2, 1):
            valid = place >= k
            passed, state = received[k - 1][0][p], received[k - 1][1][p]
            before = jnp.where(valid, passed * before + state, before)
            decay = jnp.where(valid, passed * decay, decay)
        before_ref[rows] = before
        decay_ref[p * 8 : (p + 1) * 8] = jnp.broadcast_to(decay, (8, LANES))
        total = own_decays[p] * before + own_states[p]
        for k in (3, 2, 1):
            later = place < k
            passed, state = received[k - 1][0][p], received[k - 1][1][p]
            total = jnp.where(later, passed * total + state, total)
        message_ref[rows] = total.astype(jnp.bfloat16)
        whole.append(own_decays[p] * received[0][0][p] * received[1][0][p] * received[2][0][p])
    message_ref[pairs * VALUE_DIM :] = pack_decay(jnp.concatenate(whole, axis=1))


def masked_heads(rows):
    lane = lax.broadcasted_iota(jnp.int32, rows.shape, 1)
    return jnp.concatenate(
        [jnp.where(lane < KEY_DIM, rows, 0.0), jnp.where(lane >= KEY_DIM, rows, 0.0)], axis=0
    ).astype(jnp.bfloat16)


def within_kernel(
    queries_ref, keys_ref, values_ref, logits_ref, head_gain_ref, out_gate_ref, partial_ref, reach_ref, gating_ref
):
    for h in range(out_gate_ref.shape[1] // VALUE_DIM):
        place = slice(h * VALUE_DIM, (h + 1) * VALUE_DIM)
        gate = out_gate_ref[:, place].astype(jnp.float32)
        gating_ref[:, place] = head_gain_ref[...] * (gate / (1.0 + jnp.exp(-gate)))
    length, channels = keys_ref.shape
    blocks = length // BLOCK
    pairs = channels // LANES
    running_all = running_sums(logits_ref[...].astype(jnp.float32))
    states = [jnp.zeros((VALUE_DIM, LANES), jnp.float32)] * pairs
    lead = jnp.zeros((1, channels), jnp.float32)
    row = lax.broadcasted_iota(jnp.int32, (2 * BLOCK, BLOCK), 0)
    column = lax.broadcasted_iota(jnp.int32, (2 * BLOCK, BLOCK), 1)
    causal = (row & (BLOCK - 1)) >= column
    for n in range(blocks):
        rows = slice(n * BLOCK, (n + 1) * BLOCK)
        running = running_all[rows]
        query_scaled = queries_ref[rows].astype(jnp.float32) * KEY_DIM ** (-0.5) * jnp.exp(running)
        key_inverse = (keys_ref[rows].astype(jnp.float32) * jnp.exp(-running)).astype(jnp.bfloat16)
        reach_ref[rows] = query_scaled * jnp.exp(lead)
        lead = lead + running[BLOCK - 1 : BLOCK]
        for p in range(pairs):
            lanes = slice(p * LANES, (p + 1) * LANES)
            masked = masked_heads(query_scaled[:, lanes])
            scores = jnp.where(causal, product(masked, key_inverse[:, lanes], 1, 1), 0.0).astype(jnp.bfloat16)
            carried = product(masked, states[p].astype(jnp.bfloat16), 1, 1)
            for h in range(2):
                place = slice((2 * p + h) * VALUE_DIM, (2 * p + h + 1) * VALUE_DIM)
                part = slice(h * BLOCK, (h + 1) * BLOCK)
                partial_ref[rows, place] = product(scores[part], values_ref[rows, place]) + carried[part]
        if n + 1 < blocks:
            states = grow(states, n, running_all, keys_ref, values_ref)


def finish_kernel(
    place_ref, plane_ref, back1_ref, back2_ref, back3_ref, before_y_ref, decay_y_ref, before_x_ref, decay_x_ref,
    partial_ref, reach_ref, gating_ref, kept_ref, given_ref, whole,
):
    core, plane = place_ref[0], plane_ref[0]
    length, channels = reach_ref.shape
    pairs = channels // LANES
    received = [unpack(ref) for ref in (back1_ref, back2_ref, back3_ref)]
    half = length // 2
    for p in range(pairs):
        lanes = slice(p * LANES, (p + 1) * LANES)
        rows = slice(p * VALUE_DIM, (p + 1) * VALUE_DIM)
        state = jnp.zeros((VALUE_DIM, LANES), jnp.float32)
        for k in (3, 2, 1):
            decay, grown = received[k - 1][0][p], received[k - 1][1][p]
            state = jnp.where(plane >= k, decay * state + grown, state)
        state = before_y_ref[rows] + decay_y_ref[p * 8 : p * 8 + 1] * state
        state = before_x_ref[rows] + decay_x_ref[p * 8 : p * 8 + 1] * state
        carried = product(masked_heads(reach_ref[:, lanes]), state.astype(jnp.bfloat16), 1, 1)
        for h in range(2):
            place = slice((2 * p + h) * VALUE_DIM, (2 * p + h + 1) * VALUE_DIM)
            attended = partial_ref[:, place] + carried[h * length : (h + 1) * length]
            scale = lax.rsqrt(jnp.mean(attended * attended, axis=1, keepdims=True) + 1e-06)
            result = (attended * scale * gating_ref[:, place]).astype(jnp.bfloat16)
            whole[0, :, place] = result[:half]
            whole[1, :, place] = result[half:]
    kept_ref[...] = whole[core]
    given_ref[...] = whole[1 - core]


def own_kernel(place_ref, kept_ref, weight_ref, residual_ref, partial_ref):
    core = place_ref[0]
    depth = kept_ref.shape[1]
    tile = 256
    own = pl.ds(pl.multiple_of(core * depth, depth), depth)
    for n in range(residual_ref.shape[1] // tile):
        part = slice(n * tile, (n + 1) * tile)
        partial_ref[:, part] = residual_ref[:, part].astype(jnp.float32) + product(kept_ref[...], weight_ref[own, part])


def project_kernel(
    place_ref, owners_vmem, taken_ref, weight_ref, partial_ref, norm_gain_ref, merged_ref, outgoing_ref,
    chunked, owners_ref, sem,
):
    indices = pltpu.make_async_copy(owners_vmem, owners_ref, sem.at[0])
    indices.start()
    core = place_ref[0]
    rows, width = partial_ref.shape
    depth = taken_ref.shape[1]
    tile = 256
    other = pl.ds(pl.multiple_of((1 - core) * depth, depth), depth)
    square = jnp.zeros((rows, 1), jnp.float32)
    for n in range(width // tile):
        part = slice(n * tile, (n + 1) * tile)
        merged = (partial_ref[:, part] + product(taken_ref[...], weight_ref[other, part])).astype(jnp.bfloat16)
        merged_ref[:, part] = merged
        widened = merged.astype(jnp.float32)
        square = square + jnp.sum(widened * widened, axis=1, keepdims=True)
    scale = lax.rsqrt(square / width + 1e-06)
    swap = swap_matrix()
    for g in range(0, rows // SUB, 2):
        blocks = []
        for k in (g, g + 1):
            group = slice(k * SUB, (k + 1) * SUB)
            stacked = []
            for j in range(width // LANES):
                lanes = slice(j * LANES, (j + 1) * LANES)
                widened = merged_ref[group, lanes].astype(jnp.float32)
                stacked.append((widened * scale[group] * norm_gain_ref[:, lanes]).astype(jnp.bfloat16))
            blocks.append(jnp.concatenate(stacked, axis=0))
        for k, turned in zip((g, g + 1), swap_groups(swap, blocks, False)):
            chunked[k * SUB : (k + 1) * SUB] = turned.astype(jnp.bfloat16).reshape(SUB, SUB, LANES)

    experts_total = owners_ref.shape[1]
    capacity = outgoing_ref.shape[0] // experts_total

    indices.wait()
    batch = 8
    for first in range(0, experts_total, batch):
        rows = [chunked[owners_ref[place, first + k]] for k in range(batch) for place in range(capacity)]
        for k, row in enumerate(rows):
            outgoing_ref[capacity * first + k] = row


def shape_of(shape, dtype):
    return jax.ShapeDtypeStruct(shape, dtype)


def limited(mebibytes):
    return pltpu.CompilerParams(vmem_limit_bytes=int(mebibytes * 1048576))


def call(kernel, outs, operands, scalars=0, scratch=(), cost=10000000, room=6, far=False):
    return pl.pallas_call(
        kernel,
        out_shape=outs,
        in_specs=[SMEM_SPEC] * scalars + [ANY_SPEC if far else VMEM_SPEC] * (len(operands) - scalars),
        out_specs=jax.tree.map(lambda _: VMEM_SPEC, outs),
        scratch_shapes=list(scratch),
        cost_estimate=pl.CostEstimate(flops=cost * 400, bytes_accessed=cost, transcendentals=0),
        compiler_params=limited(room),
    )(*operands)


def from_behind(message, axis):
    moved = []
    for k in range(1, RING):
        moved.append(lax.ppermute(message, axis, [(i, (i + k) % RING) for i in range(RING)]))
    return moved


def local(
    residual,
    queries,
    key_rows,
    value_rows,
    out_gate,
    gate_logits,
    head_gain,
    out_weight,
    norm_gain,
    routes,
    group_score,
    expert_score,
    gate_weight,
    up_weight,
    down_weight,
):
    row_count, model_width = residual.shape
    length, channels = queries.shape
    values = value_rows.shape[1]
    f32, bf16 = jnp.float32, jnp.bfloat16
    z, y, x, core = (lax.axis_index(axis).astype(jnp.int32).reshape(1) for axis in SP_TP)
    pairs = channels // LANES
    message_shape = shape_of((pairs * VALUE_DIM + SUB, LANES), bf16)
    state_shape = shape_of((pairs * VALUE_DIM, LANES), f32)
    decay_shape = shape_of((pairs * 8, LANES), f32)
    message = call(
        state_kernel,
        message_shape,
        (key_rows, value_rows, gate_logits),
        scratch=[
            pltpu.VMEM(key_rows.shape, bf16),
            pltpu.VMEM(value_rows.shape, bf16),
            pltpu.VMEM(gate_logits.shape, bf16),
            pltpu.SemaphoreType.DMA((3,)),
        ],
        room=53.8,
        far=True,
    )
    experts_total = lax.axis_size(SP_TP)
    capacity = 3 * row_count // experts_total
    slots, owners, weights = routing(routes, group_score, expert_score)
    behind = from_behind(message, "sp_2")
    slots, owners, weights, *behind = lax.optimization_barrier((slots, owners, weights, *behind))
    before_x, decay_x, message_x = call(
        stage_kernel, (state_shape, decay_shape, message_shape), (x, message, *behind), 1
    )
    behind = from_behind(message_x, "sp_1")
    before_y, decay_y, message_y = call(
        stage_kernel, (state_shape, decay_shape, message_shape), (y, message_x, *behind), 1
    )
    behind = from_behind(message_y, "sp_0")
    message_y, queries, key_rows = lax.optimization_barrier((message_y, queries, key_rows))
    partial, reach, gating = call(
        within_kernel,
        (shape_of((length, values), f32), shape_of((length, channels), f32), shape_of((length, values), f32)),
        (queries, key_rows, value_rows, gate_logits, head_gain.reshape(1, -1), out_gate),
    )
    partial, reach, gating, *behind = lax.optimization_barrier((partial, reach, gating, *behind))
    half = shape_of((length // 2, values), bf16)
    kept, given = call(
        finish_kernel,
        (half, half),
        (core, z, *behind, before_y, decay_y, before_x, decay_x, partial, reach, gating),
        2,
        [pltpu.VMEM((2, length // 2, values), bf16)],
        cost=300000,
    )
    taken = lax.ppermute(given, "tp", [(0, 1), (1, 0)])
    projected = call(own_kernel, shape_of((row_count, model_width), f32), (core, kept, out_weight, residual), 1, room=8)
    projected, taken = lax.optimization_barrier((projected, taken))
    merged, outgoing = call(
        project_kernel,
        (
            shape_of((row_count, model_width), bf16),
            shape_of((experts_total * capacity, SUB, LANES), bf16),
        ),
        (core, owners, taken, out_weight, projected, norm_gain.reshape(1, -1)),
        1,
        [
            pltpu.VMEM((row_count, SUB, LANES), bf16),
            pltpu.SMEM(owners.shape, jnp.int32),
            pltpu.SemaphoreType.DMA((1,)),
        ],
        room=14,
    )
    block = (experts_total, capacity * SUB, LANES)
    arrived = lax.all_to_all(outgoing.reshape(block), SP_TP, split_axis=0, concat_axis=0, tiled=True)
    served = experts(arrived.reshape(outgoing.shape), gate_weight, up_weight, down_weight)
    returned = lax.all_to_all(served.reshape(block), SP_TP, split_axis=0, concat_axis=0, tiled=True)
    return combine(slots, returned.reshape(outgoing.shape), merged, weights)


def solution(mesh):
    torus = Mesh(mesh.devices.reshape(4, 4, 4, mesh.shape["tp"]), ("sp_0", "sp_1", "sp_2", "tp"))
    in_specs = (
        P(SP_TP, None),
        P(SP, "tp"),
        P(SP, "tp"),
        P(SP, "tp"),
        P(SP, "tp"),
        P(SP, "tp"),
        P(),
        P(),
        P(),
        P(SP_TP, None),
        P(SP_TP),
        P(SP_TP, None),
        P(SP_TP, None, None),
        P(SP_TP, None, None),
        P(SP_TP, None, None),
    )
    out_specs = P(SP_TP, None)
    return jax.shard_map(local, mesh=torus, in_specs=in_specs, out_specs=out_specs, check_vma=False)
```

```python
import jax
import jax.numpy as jnp
from jax import lax
from jax.experimental import pallas as pl
from jax.experimental.pallas import tpu as pltpu
from jax.sharding import Mesh
from jax.sharding import PartitionSpec as P

KEY_DIM = 64
VALUE_DIM = 128
BLOCK = 64
RING = 4
SP = ("sp_0", "sp_1", "sp_2")
SP_TP = ("sp_0", "sp_1", "sp_2", "tp")


VMEM_SPEC = pl.BlockSpec(memory_space=pltpu.VMEM)
SMEM_SPEC = pl.BlockSpec(memory_space=pltpu.SMEM)
ANY_SPEC = pl.BlockSpec(memory_space=pl.ANY)
SUB = 16
LANES = 128
SWAP = SUB * SUB


def swap_matrix():
    row = lax.broadcasted_iota(jnp.int32, (SWAP, SWAP), 0)
    column = lax.broadcasted_iota(jnp.int32, (SWAP, SWAP), 1)
    partner = (row & (SUB - 1)) * SUB + (row >> 4)
    return (partner == column).astype(jnp.float32).astype(jnp.bfloat16)


def exchange(swap, blocks):
    turned = jnp.dot(swap, jnp.concatenate(blocks, axis=1), preferred_element_type=jnp.float32)
    return [turned[:, k * LANES : (k + 1) * LANES] for k in range(len(blocks))]


def turn(block):
    return jnp.transpose(block.reshape(SUB, SUB, LANES), (1, 0, 2)).reshape(SWAP, LANES)


def swap_groups(swap, blocks, by_matmul):
    return exchange(swap, blocks) if by_matmul else [turn(block) for block in blocks]


def stack_chunks(ref, g):
    width = ref.shape[1]
    return jnp.concatenate(
        [ref[g * SUB : (g + 1) * SUB, j * LANES : (j + 1) * LANES] for j in range(width // LANES)], axis=0
    )


def routing_kernel(routes_ref, group_ref, expert_ref, slots_ref, owners_ref, weights_ref):
    choices, rows = routes_ref.shape
    capacity = 3
    bf16 = jnp.bfloat16
    expert = lax.broadcasted_iota(jnp.int32, (LANES, rows), 0)
    token = lax.broadcasted_iota(jnp.int32, (LANES, rows), 1)
    named = [expert == routes_ref[k : k + 1] for k in range(choices)]
    named = [one.astype(jnp.float32) for one in named]
    source = lax.broadcasted_iota(jnp.int32, (rows, rows), 0)
    target = lax.broadcasted_iota(jnp.int32, (rows, rows), 1)
    before = (source < target).astype(jnp.float32).astype(bf16)
    used = jnp.dot(sum(named).astype(bf16), before, preferred_element_type=jnp.float32)
    place = lax.broadcasted_iota(jnp.int32, (8, rows), 0).astype(jnp.float32)
    name = lax.broadcasted_iota(jnp.int32, (8, rows), 1).astype(jnp.float32)
    owners = jnp.zeros((8, LANES), jnp.float32)
    for k in range(choices):
        rank = jnp.sum(named[k] * used, axis=0, keepdims=True)
        slots_ref[k : k + 1] = routes_ref[k : k + 1] * capacity + rank.astype(jnp.int32)
        owned = jnp.where(place == rank, name, 0.0).astype(bf16)
        owners = owners + lax.dot_general(
            owned, named[k].astype(bf16), (((1,), (1,)), ((), ())), preferred_element_type=jnp.float32
        )
    owners_ref[...] = owners.astype(jnp.int32)
    score = expert_ref[...]
    weights = group_ref[...] * score / jnp.sum(score, axis=0, keepdims=True)
    for k in range(choices):
        spread = jnp.broadcast_to(weights[k : k + 1], (LANES, rows))
        weights_ref[k] = spread.T


def routing(routes, group_score, expert_score):
    rows, choices = routes.shape
    return call(
        routing_kernel,
        (
            shape_of((choices, rows), jnp.int32),
            shape_of((8, LANES), jnp.int32),
            shape_of((choices, rows, LANES), jnp.float32),
        ),
        (routes.T, group_score.reshape(1, rows), expert_score.T),
        room=2,
    )


def experts_kernel(rows_ref, gate, up, down, out_ref, rows_in, inner, served):
    swap = swap_matrix()
    count, width = rows_in.shape
    hidden = inner.shape[1]
    groups = count // SUB
    for g in range(0, groups, 2):
        blocks = [rows_ref[k * SUB : (k + 1) * SUB].reshape(SWAP, LANES) for k in (g, g + 1)]
        for k, turned in zip((g, g + 1), swap_groups(swap, blocks, False)):
            turned = turned.astype(jnp.bfloat16)
            for j in range(width // LANES):
                rows_in[k * SUB : (k + 1) * SUB, j * LANES : (j + 1) * LANES] = turned[j * SUB : (j + 1) * SUB]
    tile = 256
    for n in range(hidden // tile):
        part = slice(n * tile, (n + 1) * tile)
        gated = jnp.dot(rows_in[...], gate[0, :, part], preferred_element_type=jnp.float32)
        lifted = jnp.dot(rows_in[...], up[0, :, part], preferred_element_type=jnp.float32)
        inner[:, part] = (gated / (1.0 + jnp.exp(-gated)) * lifted).astype(jnp.bfloat16)
    for n in range(width // tile):
        part = slice(n * tile, (n + 1) * tile)
        served[:, part] = jnp.dot(inner[...], down[0, :, part], preferred_element_type=jnp.float32).astype(jnp.bfloat16)
    for g in range(0, groups, 2):
        blocks = [stack_chunks(served, k) for k in (g, g + 1)]
        for k, turned in zip((g, g + 1), swap_groups(swap, blocks, False)):
            out_ref[k * SUB : (k + 1) * SUB] = turned.astype(jnp.bfloat16).reshape(SUB, SUB, LANES)


def experts(arrived, gate_weight, up_weight, down_weight):
    count = arrived.shape[0]
    width, hidden = gate_weight.shape[1:]
    return pl.pallas_call(
        experts_kernel,
        out_shape=jax.ShapeDtypeStruct(arrived.shape, jnp.bfloat16),
        in_specs=[VMEM_SPEC] * 4,
        out_specs=VMEM_SPEC,
        scratch_shapes=[
            pltpu.VMEM((count, width), jnp.bfloat16),
            pltpu.VMEM((count, hidden), jnp.bfloat16),
            pltpu.VMEM((count, width), jnp.bfloat16),
        ],
        compiler_params=limited(16),
        name="experts",
    )(arrived, gate_weight, up_weight, down_weight)


def combine_kernel(slots_vmem, returned_ref, merged_ref, weights_ref, out_hbm, out_ref, slots_ref, sem, sems):
    indices = pltpu.make_async_copy(slots_vmem, slots_ref, sem.at[0])
    indices.start()
    swap = swap_matrix()
    rows, width = merged_ref.shape
    indices.wait()
    copies = []
    for g in range(rows // SUB):
        group = slice(g * SUB, (g + 1) * SUB)
        picked = [
            jnp.concatenate([returned_ref[slots_ref[k, g * SUB + i]] for i in range(SUB)], axis=0) for k in range(2)
        ]
        first, second = exchange(swap, picked)
        for j in range(width // LANES):
            lanes = slice(j * LANES, (j + 1) * LANES)
            part = slice(j * SUB, (j + 1) * SUB)
            total = weights_ref[0, group] * first[part] + weights_ref[1, group] * second[part]
            out_ref[group, lanes] = (merged_ref[group, lanes].astype(jnp.float32) + total).astype(jnp.bfloat16)
        if g % 2 == 1:
            both = pl.ds((g - 1) * SUB, 2 * SUB)
            copies.append(pltpu.make_async_copy(out_ref.at[both], out_hbm.at[both], sems.at[g // 2]))
            copies[-1].start()
    for copy in copies:
        copy.wait()


def combine(slots, returned, merged, weights):
    rows = merged.shape[0]
    return pl.pallas_call(
        combine_kernel,
        out_shape=shape_of(merged.shape, jnp.bfloat16),
        in_specs=[VMEM_SPEC] * 4,
        out_specs=ANY_SPEC,
        scratch_shapes=[
            pltpu.VMEM(merged.shape, jnp.bfloat16),
            pltpu.SMEM(slots.shape, jnp.int32),
            pltpu.SemaphoreType.DMA((1,)),
            pltpu.SemaphoreType.DMA((rows // SUB // 2,)),
        ],
        compiler_params=limited(8),
        name="combine",
    )(slots, returned, merged, weights)


def pieces(value, count):
    parts = []
    for _ in range(count):
        part = value.astype(jnp.bfloat16)
        parts.append(part)
        value = value - part.astype(jnp.float32)
    return parts


def product(left, right, left_dim=1, right_dim=0):
    return lax.dot_general(
        left, right, (((left_dim,), (right_dim,)), ((), ())), preferred_element_type=jnp.float32
    )


def decay_parts(logits):
    decay_log = (jnp.minimum(logits, 0.0) - jnp.log1p(jnp.exp(-jnp.abs(logits)))) / 16.0
    return decay_log, pieces(decay_log, 3)


def ordered(length):
    row = lax.broadcasted_iota(jnp.int32, (length, length), 0)
    column = lax.broadcasted_iota(jnp.int32, (length, length), 1)
    return row, column


def running_sums(logits):
    _, parts = decay_parts(logits)
    row, column = ordered(logits.shape[0])
    earlier = (row >= column) & (row // BLOCK == column // BLOCK)
    earlier = earlier.astype(jnp.float32).astype(jnp.bfloat16)
    return sum(product(earlier, part) for part in parts)


def grow(states, n, running, keys_ref, values_ref):
    wide = 2 * VALUE_DIM
    rows = slice(n * BLOCK, (n + 1) * BLOCK)
    closing = running[(n + 1) * BLOCK - 1 : (n + 1) * BLOCK]
    key_closing = keys_ref[rows].astype(jnp.float32) * jnp.exp(closing - running[rows])
    key_closing = pieces(key_closing, 2)
    decay = jnp.exp(closing)
    lane = lax.broadcasted_iota(jnp.int32, (VALUE_DIM, LANES), 1)
    after = []
    for p, state in enumerate(states):
        lanes = slice(p * LANES, (p + 1) * LANES)
        value = values_ref[rows, p * wide : (p + 1) * wide]
        grown = product(value, key_closing[0][:, lanes], 0, 0) + product(value, key_closing[1][:, lanes], 0, 0)
        grown = jnp.where(lane < KEY_DIM, grown[:VALUE_DIM], grown[VALUE_DIM:])
        after.append(decay[:, lanes] * state + grown)
    return after


def state_kernel(keys_hbm, values_hbm, logits_hbm, message_ref, keys_ref, values_ref, logits_ref, sems):
    copies = [
        pltpu.make_async_copy(source, target, sems.at[k])
        for k, (source, target) in enumerate(
            ((logits_hbm, logits_ref), (keys_hbm, keys_ref), (values_hbm, values_ref))
        )
    ]
    for copy in copies:
        copy.start()
    copies[0].wait()
    length, channels = keys_ref.shape
    pairs = channels // LANES
    wide = 2 * VALUE_DIM
    decay_log, parts = decay_parts(logits_ref[...].astype(jnp.float32))
    row, column = ordered(length)
    later = (row < column).astype(jnp.float32).astype(jnp.bfloat16)
    ahead = sum(product(later, part) for part in parts)
    factor = jnp.exp(ahead)
    total = ahead[0:1] + decay_log[0:1]
    copies[1].wait()
    key_end = (keys_ref[...].astype(jnp.float32) * factor).astype(jnp.bfloat16)
    copies[2].wait()
    lane = lax.broadcasted_iota(jnp.int32, (VALUE_DIM, LANES), 1)
    for p in range(pairs):
        grown = product(values_ref[:, p * wide : (p + 1) * wide], key_end[:, p * LANES : (p + 1) * LANES], 0, 0)
        state = jnp.where(lane < KEY_DIM, grown[:VALUE_DIM], grown[VALUE_DIM:])
        message_ref[p * VALUE_DIM : (p + 1) * VALUE_DIM] = state.astype(jnp.bfloat16)
    message_ref[pairs * VALUE_DIM :] = pack_decay(jnp.exp(total))


def pack_decay(decay):
    pairs = decay.shape[1] // LANES
    place = lax.broadcasted_iota(jnp.int32, (SUB, LANES), 0)
    high, low = pieces(decay, 2)
    packed = jnp.zeros((SUB, LANES), jnp.float32)
    for p in range(pairs):
        lanes = slice(p * LANES, (p + 1) * LANES)
        packed = jnp.where(place == p, high[:, lanes].astype(jnp.float32), packed)
        packed = jnp.where(place == pairs + p, low[:, lanes].astype(jnp.float32), packed)
    return packed.astype(jnp.bfloat16)


def unpack(message_ref):
    states = message_ref.shape[0] - SUB
    pairs = states // VALUE_DIM
    packed = message_ref[states:].astype(jnp.float32)
    decays = [packed[p : p + 1] + packed[pairs + p : pairs + p + 1] for p in range(pairs)]
    return decays, [message_ref[p * VALUE_DIM : (p + 1) * VALUE_DIM].astype(jnp.float32) for p in range(pairs)]


def stage_kernel(place_ref, own_ref, back1_ref, back2_ref, back3_ref, before_ref, decay_ref, message_ref):
    place = place_ref[0]
    own_decays, own_states = unpack(own_ref)
    pairs = len(own_decays)
    received = [unpack(ref) for ref in (back1_ref, back2_ref, back3_ref)]
    whole = []
    for p in range(pairs):
        rows = slice(p * VALUE_DIM, (p + 1) * VALUE_DIM)
        before = jnp.zeros((VALUE_DIM, LANES), jnp.float32)
        decay = jnp.ones((1, LANES), jnp.float32)
        for k in (3, 2, 1):
            valid = place >= k
            passed, state = received[k - 1][0][p], received[k - 1][1][p]
            before = jnp.where(valid, passed * before + state, before)
            decay = jnp.where(valid, passed * decay, decay)
        before_ref[rows] = before
        decay_ref[p * 8 : (p + 1) * 8] = jnp.broadcast_to(decay, (8, LANES))
        total = own_decays[p] * before + own_states[p]
        for k in (3, 2, 1):
            later = place < k
            passed, state = received[k - 1][0][p], received[k - 1][1][p]
            total = jnp.where(later, passed * total + state, total)
        message_ref[rows] = total.astype(jnp.bfloat16)
        whole.append(own_decays[p] * received[0][0][p] * received[1][0][p] * received[2][0][p])
    message_ref[pairs * VALUE_DIM :] = pack_decay(jnp.concatenate(whole, axis=1))


def masked_heads(rows):
    lane = lax.broadcasted_iota(jnp.int32, rows.shape, 1)
    return jnp.concatenate(
        [jnp.where(lane < KEY_DIM, rows, 0.0), jnp.where(lane >= KEY_DIM, rows, 0.0)], axis=0
    ).astype(jnp.bfloat16)


def within_kernel(
    queries_ref, keys_ref, values_ref, logits_ref, head_gain_ref, out_gate_ref, partial_ref, reach_ref, gating_ref
):
    for h in range(out_gate_ref.shape[1] // VALUE_DIM):
        place = slice(h * VALUE_DIM, (h + 1) * VALUE_DIM)
        gate = out_gate_ref[:, place].astype(jnp.float32)
        gating_ref[:, place] = head_gain_ref[...] * (gate / (1.0 + jnp.exp(-gate)))
    length, channels = keys_ref.shape
    blocks = length // BLOCK
    pairs = channels // LANES
    running_all = running_sums(logits_ref[...].astype(jnp.float32))
    states = [jnp.zeros((VALUE_DIM, LANES), jnp.float32)] * pairs
    lead = jnp.zeros((1, channels), jnp.float32)
    row = lax.broadcasted_iota(jnp.int32, (2 * BLOCK, BLOCK), 0)
    column = lax.broadcasted_iota(jnp.int32, (2 * BLOCK, BLOCK), 1)
    causal = (row & (BLOCK - 1)) >= column
    for n in range(blocks):
        rows = slice(n * BLOCK, (n + 1) * BLOCK)
        running = running_all[rows]
        query_scaled = queries_ref[rows].astype(jnp.float32) * KEY_DIM ** (-0.5) * jnp.exp(running)
        key_inverse = pieces(keys_ref[rows].astype(jnp.float32) * jnp.exp(-running), 2)
        reach_ref[rows] = query_scaled * jnp.exp(lead)
        lead = lead + running[BLOCK - 1 : BLOCK]
        for p in range(pairs):
            lanes = slice(p * LANES, (p + 1) * LANES)
            high, low = (masked_heads(part.astype(jnp.float32)) for part in pieces(query_scaled[:, lanes], 2))
            scores = product(high, key_inverse[0][:, lanes], 1, 1)
            scores = scores + product(high, key_inverse[1][:, lanes], 1, 1) + product(low, key_inverse[0][:, lanes], 1, 1)
            scores = pieces(jnp.where(causal, scores, 0.0), 2)
            before = pieces(states[p], 2)
            carried = product(high, before[0], 1, 1) + product(high, before[1], 1, 1) + product(low, before[0], 1, 1)
            for h in range(2):
                place = slice((2 * p + h) * VALUE_DIM, (2 * p + h + 1) * VALUE_DIM)
                part = slice(h * BLOCK, (h + 1) * BLOCK)
                value = values_ref[rows, place]
                partial_ref[rows, place] = product(scores[0][part], value) + product(scores[1][part], value) + carried[part]
        if n + 1 < blocks:
            states = grow(states, n, running_all, keys_ref, values_ref)


def finish_kernel(
    place_ref, plane_ref, back1_ref, back2_ref, back3_ref, before_y_ref, decay_y_ref, before_x_ref, decay_x_ref,
    partial_ref, reach_ref, gating_ref, kept_ref, given_ref, whole,
):
    core, plane = place_ref[0], plane_ref[0]
    length, channels = reach_ref.shape
    pairs = channels // LANES
    received = [unpack(ref) for ref in (back1_ref, back2_ref, back3_ref)]
    half = length // 2
    for p in range(pairs):
        lanes = slice(p * LANES, (p + 1) * LANES)
        rows = slice(p * VALUE_DIM, (p + 1) * VALUE_DIM)
        state = jnp.zeros((VALUE_DIM, LANES), jnp.float32)
        for k in (3, 2, 1):
            decay, grown = received[k - 1][0][p], received[k - 1][1][p]
            state = jnp.where(plane >= k, decay * state + grown, state)
        state = before_y_ref[rows] + decay_y_ref[p * 8 : p * 8 + 1] * state
        state = before_x_ref[rows] + decay_x_ref[p * 8 : p * 8 + 1] * state
        carried = product(masked_heads(reach_ref[:, lanes]), state.astype(jnp.bfloat16), 1, 1)
        for h in range(2):
            place = slice((2 * p + h) * VALUE_DIM, (2 * p + h + 1) * VALUE_DIM)
            attended = partial_ref[:, place] + carried[h * length : (h + 1) * length]
            scale = lax.rsqrt(jnp.mean(attended * attended, axis=1, keepdims=True) + 1e-06)
            result = (attended * scale * gating_ref[:, place]).astype(jnp.bfloat16)
            whole[0, :, place] = result[:half]
            whole[1, :, place] = result[half:]
    kept_ref[...] = whole[core]
    given_ref[...] = whole[1 - core]


def own_kernel(place_ref, kept_ref, weight_ref, residual_ref, partial_ref):
    core = place_ref[0]
    depth = kept_ref.shape[1]
    tile = 256
    own = pl.ds(pl.multiple_of(core * depth, depth), depth)
    for n in range(residual_ref.shape[1] // tile):
        part = slice(n * tile, (n + 1) * tile)
        partial_ref[:, part] = residual_ref[:, part].astype(jnp.float32) + product(kept_ref[...], weight_ref[own, part])


def project_kernel(
    place_ref, owners_vmem, taken_ref, weight_ref, partial_ref, norm_gain_ref, merged_ref, outgoing_ref,
    chunked, owners_ref, sem,
):
    indices = pltpu.make_async_copy(owners_vmem, owners_ref, sem.at[0])
    indices.start()
    core = place_ref[0]
    rows, width = partial_ref.shape
    depth = taken_ref.shape[1]
    tile = 256
    other = pl.ds(pl.multiple_of((1 - core) * depth, depth), depth)
    square = jnp.zeros((rows, 1), jnp.float32)
    for n in range(width // tile):
        part = slice(n * tile, (n + 1) * tile)
        merged = (partial_ref[:, part] + product(taken_ref[...], weight_ref[other, part])).astype(jnp.bfloat16)
        merged_ref[:, part] = merged
        widened = merged.astype(jnp.float32)
        square = square + jnp.sum(widened * widened, axis=1, keepdims=True)
    scale = lax.rsqrt(square / width + 1e-06)
    swap = swap_matrix()
    for g in range(0, rows // SUB, 2):
        blocks = []
        for k in (g, g + 1):
            group = slice(k * SUB, (k + 1) * SUB)
            stacked = []
            for j in range(width // LANES):
                lanes = slice(j * LANES, (j + 1) * LANES)
                widened = merged_ref[group, lanes].astype(jnp.float32)
                stacked.append((widened * scale[group] * norm_gain_ref[:, lanes]).astype(jnp.bfloat16))
            blocks.append(jnp.concatenate(stacked, axis=0))
        for k, turned in zip((g, g + 1), swap_groups(swap, blocks, False)):
            chunked[k * SUB : (k + 1) * SUB] = turned.astype(jnp.bfloat16).reshape(SUB, SUB, LANES)

    experts_total = owners_ref.shape[1]
    capacity = outgoing_ref.shape[0] // experts_total

    indices.wait()
    batch = 8
    for first in range(0, experts_total, batch):
        rows = [chunked[owners_ref[place, first + k]] for k in range(batch) for place in range(capacity)]
        for k, row in enumerate(rows):
            outgoing_ref[capacity * first + k] = row


def shape_of(shape, dtype):
    return jax.ShapeDtypeStruct(shape, dtype)


def limited(mebibytes):
    return pltpu.CompilerParams(vmem_limit_bytes=int(mebibytes * 1048576))


def call(kernel, outs, operands, scalars=0, scratch=(), cost=10000000, room=6, far=False):
    return pl.pallas_call(
        kernel,
        out_shape=outs,
        in_specs=[SMEM_SPEC] * scalars + [ANY_SPEC if far else VMEM_SPEC] * (len(operands) - scalars),
        out_specs=jax.tree.map(lambda _: VMEM_SPEC, outs),
        scratch_shapes=list(scratch),
        cost_estimate=pl.CostEstimate(flops=cost * 400, bytes_accessed=cost, transcendentals=0),
        compiler_params=limited(room),
    )(*operands)


def from_behind(message, axis):
    moved = []
    for k in range(1, RING):
        moved.append(lax.ppermute(message, axis, [(i, (i + k) % RING) for i in range(RING)]))
    return moved


def local(
    residual,
    queries,
    key_rows,
    value_rows,
    out_gate,
    gate_logits,
    head_gain,
    out_weight,
    norm_gain,
    routes,
    group_score,
    expert_score,
    gate_weight,
    up_weight,
    down_weight,
):
    row_count, model_width = residual.shape
    length, channels = queries.shape
    values = value_rows.shape[1]
    f32, bf16 = jnp.float32, jnp.bfloat16
    z, y, x, core = (lax.axis_index(axis).astype(jnp.int32).reshape(1) for axis in SP_TP)
    pairs = channels // LANES
    message_shape = shape_of((pairs * VALUE_DIM + SUB, LANES), bf16)
    state_shape = shape_of((pairs * VALUE_DIM, LANES), f32)
    decay_shape = shape_of((pairs * 8, LANES), f32)
    message = call(
        state_kernel,
        message_shape,
        (key_rows, value_rows, gate_logits),
        scratch=[
            pltpu.VMEM(key_rows.shape, bf16),
            pltpu.VMEM(value_rows.shape, bf16),
            pltpu.VMEM(gate_logits.shape, bf16),
            pltpu.SemaphoreType.DMA((3,)),
        ],
        room=53.8,
        far=True,
    )
    experts_total = lax.axis_size(SP_TP)
    capacity = 3 * row_count // experts_total
    slots, owners, weights = routing(routes, group_score, expert_score)
    behind = from_behind(message, "sp_2")
    slots, owners, weights, *behind = lax.optimization_barrier((slots, owners, weights, *behind))
    before_x, decay_x, message_x = call(
        stage_kernel, (state_shape, decay_shape, message_shape), (x, message, *behind), 1
    )
    behind = from_behind(message_x, "sp_1")
    before_y, decay_y, message_y = call(
        stage_kernel, (state_shape, decay_shape, message_shape), (y, message_x, *behind), 1
    )
    behind = from_behind(message_y, "sp_0")
    message_y, queries, key_rows = lax.optimization_barrier((message_y, queries, key_rows))
    partial, reach, gating = call(
        within_kernel,
        (shape_of((length, values), f32), shape_of((length, channels), f32), shape_of((length, values), f32)),
        (queries, key_rows, value_rows, gate_logits, head_gain.reshape(1, -1), out_gate),
    )
    partial, reach, gating, *behind = lax.optimization_barrier((partial, reach, gating, *behind))
    half = shape_of((length // 2, values), bf16)
    kept, given = call(
        finish_kernel,
        (half, half),
        (core, z, *behind, before_y, decay_y, before_x, decay_x, partial, reach, gating),
        2,
        [pltpu.VMEM((2, length // 2, values), bf16)],
        cost=300000,
    )
    taken = lax.ppermute(given, "tp", [(0, 1), (1, 0)])
    projected = call(own_kernel, shape_of((row_count, model_width), f32), (core, kept, out_weight, residual), 1, room=8)
    projected, taken = lax.optimization_barrier((projected, taken))
    merged, outgoing = call(
        project_kernel,
        (
            shape_of((row_count, model_width), bf16),
            shape_of((experts_total * capacity, SUB, LANES), bf16),
        ),
        (core, owners, taken, out_weight, projected, norm_gain.reshape(1, -1)),
        1,
        [
            pltpu.VMEM((row_count, SUB, LANES), bf16),
            pltpu.SMEM(owners.shape, jnp.int32),
            pltpu.SemaphoreType.DMA((1,)),
        ],
        room=14,
    )
    block = (experts_total, capacity * SUB, LANES)
    arrived = lax.all_to_all(outgoing.reshape(block), SP_TP, split_axis=0, concat_axis=0, tiled=True)
    served = experts(arrived.reshape(outgoing.shape), gate_weight, up_weight, down_weight)
    returned = lax.all_to_all(served.reshape(block), SP_TP, split_axis=0, concat_axis=0, tiled=True)
    return combine(slots, returned.reshape(outgoing.shape), merged, weights)


def solution(mesh):
    torus = Mesh(mesh.devices.reshape(4, 4, 4, mesh.shape["tp"]), ("sp_0", "sp_1", "sp_2", "tp"))
    in_specs = (
        P(SP_TP, None),
        P(SP, "tp"),
        P(SP, "tp"),
        P(SP, "tp"),
        P(SP, "tp"),
        P(SP, "tp"),
        P(),
        P(),
        P(),
        P(SP_TP, None),
        P(SP_TP),
        P(SP_TP, None),
        P(SP_TP, None, None),
        P(SP_TP, None, None),
        P(SP_TP, None, None),
    )
    out_specs = P(SP_TP, None)
    return jax.shard_map(local, mesh=torus, in_specs=in_specs, out_specs=out_specs, check_vma=False)
```

```python
import jax
import jax.numpy as jnp
from jax import lax
from jax.experimental import pallas as pl
from jax.experimental.pallas import tpu as pltpu
from jax.sharding import Mesh
from jax.sharding import PartitionSpec as P

KEY_DIM = 64
VALUE_DIM = 128
BLOCK = 64
RING = 4
SP = ("sp_0", "sp_1", "sp_2")
SP_TP = ("sp_0", "sp_1", "sp_2", "tp")


VMEM_SPEC = pl.BlockSpec(memory_space=pltpu.VMEM)
SMEM_SPEC = pl.BlockSpec(memory_space=pltpu.SMEM)
ANY_SPEC = pl.BlockSpec(memory_space=pl.ANY)
SUB = 16
LANES = 128
SWAP = SUB * SUB


def swap_matrix():
    row = lax.broadcasted_iota(jnp.int32, (SWAP, SWAP), 0)
    column = lax.broadcasted_iota(jnp.int32, (SWAP, SWAP), 1)
    partner = (row & (SUB - 1)) * SUB + (row >> 4)
    return (partner == column).astype(jnp.float32).astype(jnp.bfloat16)


def exchange(swap, blocks):
    turned = jnp.dot(swap, jnp.concatenate(blocks, axis=1), preferred_element_type=jnp.float32)
    return [turned[:, k * LANES : (k + 1) * LANES] for k in range(len(blocks))]


def turn(block):
    return jnp.transpose(block.reshape(SUB, SUB, LANES), (1, 0, 2)).reshape(SWAP, LANES)


def swap_groups(swap, blocks, by_matmul):
    return exchange(swap, blocks) if by_matmul else [turn(block) for block in blocks]


def stack_chunks(ref, g):
    width = ref.shape[1]
    return jnp.concatenate(
        [ref[g * SUB : (g + 1) * SUB, j * LANES : (j + 1) * LANES] for j in range(width // LANES)], axis=0
    )


def routing_kernel(routes_ref, group_ref, expert_ref, slots_ref, owners_ref, weights_ref):
    choices, rows = routes_ref.shape
    capacity = 3
    bf16 = jnp.bfloat16
    expert = lax.broadcasted_iota(jnp.int32, (LANES, rows), 0)
    token = lax.broadcasted_iota(jnp.int32, (LANES, rows), 1)
    named = [expert == routes_ref[k : k + 1] for k in range(choices)]
    named = [one.astype(jnp.float32) for one in named]
    source = lax.broadcasted_iota(jnp.int32, (rows, rows), 0)
    target = lax.broadcasted_iota(jnp.int32, (rows, rows), 1)
    before = (source < target).astype(jnp.float32).astype(bf16)
    used = jnp.dot(sum(named).astype(bf16), before, preferred_element_type=jnp.float32)
    place = lax.broadcasted_iota(jnp.int32, (8, rows), 0).astype(jnp.float32)
    name = lax.broadcasted_iota(jnp.int32, (8, rows), 1).astype(jnp.float32)
    owners = jnp.zeros((8, LANES), jnp.float32)
    for k in range(choices):
        rank = jnp.sum(named[k] * used, axis=0, keepdims=True)
        slots_ref[k : k + 1] = routes_ref[k : k + 1] * capacity + rank.astype(jnp.int32)
        owned = jnp.where(place == rank, name, 0.0).astype(bf16)
        owners = owners + lax.dot_general(
            owned, named[k].astype(bf16), (((1,), (1,)), ((), ())), preferred_element_type=jnp.float32
        )
    owners_ref[...] = owners.astype(jnp.int32)
    score = expert_ref[...]
    weights = group_ref[...] * score / jnp.sum(score, axis=0, keepdims=True)
    for k in range(choices):
        spread = jnp.broadcast_to(weights[k : k + 1], (LANES, rows))
        weights_ref[k] = spread.T


def routing(routes, group_score, expert_score):
    rows, choices = routes.shape
    return call(
        routing_kernel,
        (
            shape_of((choices, rows), jnp.int32),
            shape_of((8, LANES), jnp.int32),
            shape_of((choices, rows, LANES), jnp.float32),
        ),
        (routes.T, group_score.reshape(1, rows), expert_score.T),
        room=2,
    )


def experts_kernel(rows_ref, gate, up, down, out_ref, rows_in, inner, served):
    swap = swap_matrix()
    count, width = rows_in.shape
    hidden = inner.shape[1]
    groups = count // SUB
    for g in range(0, groups, 2):
        blocks = [rows_ref[k * SUB : (k + 1) * SUB].reshape(SWAP, LANES) for k in (g, g + 1)]
        for k, turned in zip((g, g + 1), swap_groups(swap, blocks, False)):
            turned = turned.astype(jnp.bfloat16)
            for j in range(width // LANES):
                rows_in[k * SUB : (k + 1) * SUB, j * LANES : (j + 1) * LANES] = turned[j * SUB : (j + 1) * SUB]
    tile = 256
    for n in range(hidden // tile):
        part = slice(n * tile, (n + 1) * tile)
        gated = jnp.dot(rows_in[...], gate[0, :, part], preferred_element_type=jnp.float32)
        lifted = jnp.dot(rows_in[...], up[0, :, part], preferred_element_type=jnp.float32)
        inner[:, part] = (gated / (1.0 + jnp.exp(-gated)) * lifted).astype(jnp.bfloat16)
    for n in range(width // tile):
        part = slice(n * tile, (n + 1) * tile)
        served[:, part] = jnp.dot(inner[...], down[0, :, part], preferred_element_type=jnp.float32).astype(jnp.bfloat16)
    for g in range(0, groups, 2):
        blocks = [stack_chunks(served, k) for k in (g, g + 1)]
        for k, turned in zip((g, g + 1), swap_groups(swap, blocks, False)):
            out_ref[k * SUB : (k + 1) * SUB] = turned.astype(jnp.bfloat16).reshape(SUB, SUB, LANES)


def experts(arrived, gate_weight, up_weight, down_weight):
    count = arrived.shape[0]
    width, hidden = gate_weight.shape[1:]
    return pl.pallas_call(
        experts_kernel,
        out_shape=jax.ShapeDtypeStruct(arrived.shape, jnp.bfloat16),
        in_specs=[VMEM_SPEC] * 4,
        out_specs=VMEM_SPEC,
        scratch_shapes=[
            pltpu.VMEM((count, width), jnp.bfloat16),
            pltpu.VMEM((count, hidden), jnp.bfloat16),
            pltpu.VMEM((count, width), jnp.bfloat16),
        ],
        compiler_params=limited(16),
        name="experts",
    )(arrived, gate_weight, up_weight, down_weight)


def combine_kernel(slots_vmem, returned_ref, merged_ref, weights_ref, out_hbm, out_ref, slots_ref, sem, sems):
    indices = pltpu.make_async_copy(slots_vmem, slots_ref, sem.at[0])
    indices.start()
    swap = swap_matrix()
    rows, width = merged_ref.shape
    indices.wait()
    copies = []
    for g in range(rows // SUB):
        group = slice(g * SUB, (g + 1) * SUB)
        picked = [
            jnp.concatenate([returned_ref[slots_ref[k, g * SUB + i]] for i in range(SUB)], axis=0) for k in range(2)
        ]
        first, second = exchange(swap, picked)
        for j in range(width // LANES):
            lanes = slice(j * LANES, (j + 1) * LANES)
            part = slice(j * SUB, (j + 1) * SUB)
            total = weights_ref[0, group] * first[part] + weights_ref[1, group] * second[part]
            out_ref[group, lanes] = (merged_ref[group, lanes].astype(jnp.float32) + total).astype(jnp.bfloat16)
        if g % 2 == 1:
            both = pl.ds((g - 1) * SUB, 2 * SUB)
            copies.append(pltpu.make_async_copy(out_ref.at[both], out_hbm.at[both], sems.at[g // 2]))
            copies[-1].start()
    for copy in copies:
        copy.wait()


def combine(slots, returned, merged, weights):
    rows = merged.shape[0]
    return pl.pallas_call(
        combine_kernel,
        out_shape=shape_of(merged.shape, jnp.bfloat16),
        in_specs=[VMEM_SPEC] * 4,
        out_specs=ANY_SPEC,
        scratch_shapes=[
            pltpu.VMEM(merged.shape, jnp.bfloat16),
            pltpu.SMEM(slots.shape, jnp.int32),
            pltpu.SemaphoreType.DMA((1,)),
            pltpu.SemaphoreType.DMA((rows // SUB // 2,)),
        ],
        compiler_params=limited(8),
        name="combine",
    )(slots, returned, merged, weights)


def pieces(value, count):
    parts = []
    for _ in range(count):
        part = value.astype(jnp.bfloat16)
        parts.append(part)
        value = value - part.astype(jnp.float32)
    return parts


def product(left, right, left_dim=1, right_dim=0):
    return lax.dot_general(
        left, right, (((left_dim,), (right_dim,)), ((), ())), preferred_element_type=jnp.float32
    )


def decay_parts(logits):
    decay_log = (jnp.minimum(logits, 0.0) - jnp.log1p(jnp.exp(-jnp.abs(logits)))) / 16.0
    return decay_log, pieces(decay_log, 3)


def ordered(length):
    row = lax.broadcasted_iota(jnp.int32, (length, length), 0)
    column = lax.broadcasted_iota(jnp.int32, (length, length), 1)
    return row, column


def running_sums(logits):
    _, parts = decay_parts(logits)
    row, column = ordered(logits.shape[0])
    earlier = (row >= column) & (row // BLOCK == column // BLOCK)
    earlier = earlier.astype(jnp.float32).astype(jnp.bfloat16)
    return sum(product(earlier, part) for part in parts)


def grow(states, n, running, keys_ref, values_ref):
    wide = 2 * VALUE_DIM
    rows = slice(n * BLOCK, (n + 1) * BLOCK)
    closing = running[(n + 1) * BLOCK - 1 : (n + 1) * BLOCK]
    key_closing = keys_ref[rows].astype(jnp.float32) * jnp.exp(closing - running[rows])
    key_closing = pieces(key_closing, 2)
    decay = jnp.exp(closing)
    lane = lax.broadcasted_iota(jnp.int32, (VALUE_DIM, LANES), 1)
    after = []
    for p, state in enumerate(states):
        lanes = slice(p * LANES, (p + 1) * LANES)
        value = values_ref[rows, p * wide : (p + 1) * wide]
        grown = product(value, key_closing[0][:, lanes], 0, 0) + product(value, key_closing[1][:, lanes], 0, 0)
        grown = jnp.where(lane < KEY_DIM, grown[:VALUE_DIM], grown[VALUE_DIM:])
        after.append(decay[:, lanes] * state + grown)
    return after


def state_kernel(keys_hbm, values_hbm, logits_hbm, message_ref, keys_ref, values_ref, logits_ref, sems):
    copies = [
        pltpu.make_async_copy(source, target, sems.at[k])
        for k, (source, target) in enumerate(
            ((logits_hbm, logits_ref), (keys_hbm, keys_ref), (values_hbm, values_ref))
        )
    ]
    for copy in copies:
        copy.start()
    copies[0].wait()
    length, channels = keys_ref.shape
    pairs = channels // LANES
    wide = 2 * VALUE_DIM
    decay_log, parts = decay_parts(logits_ref[...].astype(jnp.float32))
    row, column = ordered(length)
    later = (row < column).astype(jnp.float32).astype(jnp.bfloat16)
    ahead = sum(product(later, part) for part in parts)
    factor = jnp.exp(ahead)
    total = ahead[0:1] + decay_log[0:1]
    copies[1].wait()
    key_end = (keys_ref[...].astype(jnp.float32) * factor).astype(jnp.bfloat16)
    copies[2].wait()
    lane = lax.broadcasted_iota(jnp.int32, (VALUE_DIM, LANES), 1)
    for p in range(pairs):
        grown = product(values_ref[:, p * wide : (p + 1) * wide], key_end[:, p * LANES : (p + 1) * LANES], 0, 0)
        state = jnp.where(lane < KEY_DIM, grown[:VALUE_DIM], grown[VALUE_DIM:])
        message_ref[p * VALUE_DIM : (p + 1) * VALUE_DIM] = state.astype(jnp.bfloat16)
    message_ref[pairs * VALUE_DIM :] = pack_decay(jnp.exp(total))


def pack_decay(decay):
    pairs = decay.shape[1] // LANES
    place = lax.broadcasted_iota(jnp.int32, (SUB, LANES), 0)
    high, low = pieces(decay, 2)
    packed = jnp.zeros((SUB, LANES), jnp.float32)
    for p in range(pairs):
        lanes = slice(p * LANES, (p + 1) * LANES)
        packed = jnp.where(place == p, high[:, lanes].astype(jnp.float32), packed)
        packed = jnp.where(place == pairs + p, low[:, lanes].astype(jnp.float32), packed)
    return packed.astype(jnp.bfloat16)


def unpack(message_ref):
    states = message_ref.shape[0] - SUB
    pairs = states // VALUE_DIM
    packed = message_ref[states:].astype(jnp.float32)
    decays = [packed[p : p + 1] + packed[pairs + p : pairs + p + 1] for p in range(pairs)]
    return decays, [message_ref[p * VALUE_DIM : (p + 1) * VALUE_DIM].astype(jnp.float32) for p in range(pairs)]


def stage_kernel(place_ref, own_ref, back1_ref, back2_ref, back3_ref, before_ref, decay_ref, message_ref):
    place = place_ref[0]
    own_decays, own_states = unpack(own_ref)
    pairs = len(own_decays)
    received = [unpack(ref) for ref in (back1_ref, back2_ref, back3_ref)]
    whole = []
    for p in range(pairs):
        rows = slice(p * VALUE_DIM, (p + 1) * VALUE_DIM)
        before = jnp.zeros((VALUE_DIM, LANES), jnp.float32)
        decay = jnp.ones((1, LANES), jnp.float32)
        for k in (3, 2, 1):
            valid = place >= k
            passed, state = received[k - 1][0][p], received[k - 1][1][p]
            before = jnp.where(valid, passed * before + state, before)
            decay = jnp.where(valid, passed * decay, decay)
        before_ref[rows] = before
        decay_ref[p * 8 : (p + 1) * 8] = jnp.broadcast_to(decay, (8, LANES))
        total = own_decays[p] * before + own_states[p]
        for k in (3, 2, 1):
            later = place < k
            passed, state = received[k - 1][0][p], received[k - 1][1][p]
            total = jnp.where(later, passed * total + state, total)
        message_ref[rows] = total.astype(jnp.bfloat16)
        whole.append(own_decays[p] * received[0][0][p] * received[1][0][p] * received[2][0][p])
    message_ref[pairs * VALUE_DIM :] = pack_decay(jnp.concatenate(whole, axis=1))


def masked_heads(rows):
    lane = lax.broadcasted_iota(jnp.int32, rows.shape, 1)
    return jnp.concatenate(
        [jnp.where(lane < KEY_DIM, rows, 0.0), jnp.where(lane >= KEY_DIM, rows, 0.0)], axis=0
    ).astype(jnp.bfloat16)


def within_kernel(
    queries_ref, keys_ref, values_ref, logits_ref, head_gain_ref, out_gate_ref, partial_ref, reach_ref, gating_ref
):
    for h in range(out_gate_ref.shape[1] // VALUE_DIM):
        place = slice(h * VALUE_DIM, (h + 1) * VALUE_DIM)
        gate = out_gate_ref[:, place].astype(jnp.float32)
        gating_ref[:, place] = head_gain_ref[...] * (gate / (1.0 + jnp.exp(-gate)))
    length, channels = keys_ref.shape
    blocks = length // BLOCK
    pairs = channels // LANES
    running_all = running_sums(logits_ref[...].astype(jnp.float32))
    states = [jnp.zeros((VALUE_DIM, LANES), jnp.float32)] * pairs
    lead = jnp.zeros((1, channels), jnp.float32)
    row = lax.broadcasted_iota(jnp.int32, (2 * BLOCK, BLOCK), 0)
    column = lax.broadcasted_iota(jnp.int32, (2 * BLOCK, BLOCK), 1)
    causal = (row & (BLOCK - 1)) >= column
    for n in range(blocks):
        rows = slice(n * BLOCK, (n + 1) * BLOCK)
        running = running_all[rows]
        query_scaled = queries_ref[rows].astype(jnp.float32) * KEY_DIM ** (-0.5) * jnp.exp(running)
        key_inverse = pieces(keys_ref[rows].astype(jnp.float32) * jnp.exp(-running), 2)
        reach_ref[rows] = query_scaled * jnp.exp(lead)
        lead = lead + running[BLOCK - 1 : BLOCK]
        for p in range(pairs):
            lanes = slice(p * LANES, (p + 1) * LANES)
            high, low = (masked_heads(part.astype(jnp.float32)) for part in pieces(query_scaled[:, lanes], 2))
            scores = product(high, key_inverse[0][:, lanes], 1, 1)
            scores = scores + product(high, key_inverse[1][:, lanes], 1, 1) + product(low, key_inverse[0][:, lanes], 1, 1)
            scores = pieces(jnp.where(causal, scores, 0.0), 2)
            before = pieces(states[p], 2)
            carried = product(high, before[0], 1, 1) + product(high, before[1], 1, 1) + product(low, before[0], 1, 1)
            for h in range(2):
                place = slice((2 * p + h) * VALUE_DIM, (2 * p + h + 1) * VALUE_DIM)
                part = slice(h * BLOCK, (h + 1) * BLOCK)
                value = values_ref[rows, place]
                partial_ref[rows, place] = product(scores[0][part], value) + product(scores[1][part], value) + carried[part]
        if n + 1 < blocks:
            states = grow(states, n, running_all, keys_ref, values_ref)


def finish_half(core, reach_ref, partial_ref, gating_ref, state_of, result_ref):
    half = result_ref.shape[0]
    tokens = pl.ds(pl.multiple_of(core * half, half), half)
    for p in range(reach_ref.shape[1] // LANES):
        lanes = slice(p * LANES, (p + 1) * LANES)
        carried = product(masked_heads(reach_ref[tokens, lanes]), state_of(p), 1, 1)
        for h in range(2):
            place = slice((2 * p + h) * VALUE_DIM, (2 * p + h + 1) * VALUE_DIM)
            attended = partial_ref[tokens, place] + carried[h * half : (h + 1) * half]
            scale = lax.rsqrt(jnp.mean(attended * attended, axis=1, keepdims=True) + 1e-06)
            result_ref[:, place] = (attended * scale * gating_ref[tokens, place]).astype(jnp.bfloat16)


def given_kernel(
    place_ref, plane_ref, back1_ref, back2_ref, back3_ref, before_y_ref, decay_y_ref, before_x_ref, decay_x_ref,
    partial_ref, reach_ref, gating_ref, given_ref, state_ref,
):
    plane = plane_ref[0]
    received = [unpack(ref) for ref in (back1_ref, back2_ref, back3_ref)]

    def state_of(p):
        rows = slice(p * VALUE_DIM, (p + 1) * VALUE_DIM)
        state = jnp.zeros((VALUE_DIM, LANES), jnp.float32)
        for k in (3, 2, 1):
            decay, grown = received[k - 1][0][p], received[k - 1][1][p]
            state = jnp.where(plane >= k, decay * state + grown, state)
        state = before_y_ref[rows] + decay_y_ref[p * 8 : p * 8 + 1] * state
        state = before_x_ref[rows] + decay_x_ref[p * 8 : p * 8 + 1] * state
        state_ref[rows] = state.astype(jnp.bfloat16)
        return state.astype(jnp.bfloat16)

    finish_half(1 - place_ref[0], reach_ref, partial_ref, gating_ref, state_of, given_ref)


def kept_kernel(place_ref, state_ref, partial_ref, reach_ref, gating_ref, kept_ref):
    def state_of(p):
        return state_ref[p * VALUE_DIM : (p + 1) * VALUE_DIM]

    finish_half(place_ref[0], reach_ref, partial_ref, gating_ref, state_of, kept_ref)


def own_kernel(place_ref, kept_ref, weight_ref, residual_ref, partial_ref):
    core = place_ref[0]
    depth = kept_ref.shape[1]
    tile = 256
    own = pl.ds(pl.multiple_of(core * depth, depth), depth)
    for n in range(residual_ref.shape[1] // tile):
        part = slice(n * tile, (n + 1) * tile)
        partial_ref[:, part] = residual_ref[:, part].astype(jnp.float32) + product(kept_ref[...], weight_ref[own, part])


def project_kernel(
    place_ref, owners_vmem, taken_ref, weight_ref, partial_ref, norm_gain_ref, merged_ref, outgoing_ref,
    chunked, owners_ref, sem,
):
    indices = pltpu.make_async_copy(owners_vmem, owners_ref, sem.at[0])
    indices.start()
    core = place_ref[0]
    rows, width = partial_ref.shape
    depth = taken_ref.shape[1]
    tile = 256
    other = pl.ds(pl.multiple_of((1 - core) * depth, depth), depth)
    square = jnp.zeros((rows, 1), jnp.float32)
    for n in range(width // tile):
        part = slice(n * tile, (n + 1) * tile)
        merged = (partial_ref[:, part] + product(taken_ref[...], weight_ref[other, part])).astype(jnp.bfloat16)
        merged_ref[:, part] = merged
        widened = merged.astype(jnp.float32)
        square = square + jnp.sum(widened * widened, axis=1, keepdims=True)
    scale = lax.rsqrt(square / width + 1e-06)
    swap = swap_matrix()
    for g in range(0, rows // SUB, 2):
        blocks = []
        for k in (g, g + 1):
            group = slice(k * SUB, (k + 1) * SUB)
            stacked = []
            for j in range(width // LANES):
                lanes = slice(j * LANES, (j + 1) * LANES)
                widened = merged_ref[group, lanes].astype(jnp.float32)
                stacked.append((widened * scale[group] * norm_gain_ref[:, lanes]).astype(jnp.bfloat16))
            blocks.append(jnp.concatenate(stacked, axis=0))
        for k, turned in zip((g, g + 1), swap_groups(swap, blocks, False)):
            chunked[k * SUB : (k + 1) * SUB] = turned.astype(jnp.bfloat16).reshape(SUB, SUB, LANES)

    experts_total = owners_ref.shape[1]
    capacity = outgoing_ref.shape[0] // experts_total

    indices.wait()
    batch = 8
    for first in range(0, experts_total, batch):
        rows = [chunked[owners_ref[place, first + k]] for k in range(batch) for place in range(capacity)]
        for k, row in enumerate(rows):
            outgoing_ref[capacity * first + k] = row


def shape_of(shape, dtype):
    return jax.ShapeDtypeStruct(shape, dtype)


def limited(mebibytes):
    return pltpu.CompilerParams(vmem_limit_bytes=int(mebibytes * 1048576))


def call(kernel, outs, operands, scalars=0, scratch=(), cost=10000000, room=6, far=False):
    return pl.pallas_call(
        kernel,
        out_shape=outs,
        in_specs=[SMEM_SPEC] * scalars + [ANY_SPEC if far else VMEM_SPEC] * (len(operands) - scalars),
        out_specs=jax.tree.map(lambda _: VMEM_SPEC, outs),
        scratch_shapes=list(scratch),
        cost_estimate=pl.CostEstimate(flops=cost * 400, bytes_accessed=cost, transcendentals=0),
        compiler_params=limited(room),
    )(*operands)


def from_behind(message, axis):
    moved = []
    for k in range(1, RING):
        moved.append(lax.ppermute(message, axis, [(i, (i + k) % RING) for i in range(RING)]))
    return moved


def local(
    residual,
    queries,
    key_rows,
    value_rows,
    out_gate,
    gate_logits,
    head_gain,
    out_weight,
    norm_gain,
    routes,
    group_score,
    expert_score,
    gate_weight,
    up_weight,
    down_weight,
):
    row_count, model_width = residual.shape
    length, channels = queries.shape
    values = value_rows.shape[1]
    f32, bf16 = jnp.float32, jnp.bfloat16
    z, y, x, core = (lax.axis_index(axis).astype(jnp.int32).reshape(1) for axis in SP_TP)
    pairs = channels // LANES
    message_shape = shape_of((pairs * VALUE_DIM + SUB, LANES), bf16)
    state_shape = shape_of((pairs * VALUE_DIM, LANES), f32)
    decay_shape = shape_of((pairs * 8, LANES), f32)
    message = call(
        state_kernel,
        message_shape,
        (key_rows, value_rows, gate_logits),
        scratch=[
            pltpu.VMEM(key_rows.shape, bf16),
            pltpu.VMEM(value_rows.shape, bf16),
            pltpu.VMEM(gate_logits.shape, bf16),
            pltpu.SemaphoreType.DMA((3,)),
        ],
        room=53.8,
        far=True,
    )
    experts_total = lax.axis_size(SP_TP)
    capacity = 3 * row_count // experts_total
    slots, owners, weights = routing(routes, group_score, expert_score)
    behind = from_behind(message, "sp_2")
    slots, owners, weights, *behind = lax.optimization_barrier((slots, owners, weights, *behind))
    before_x, decay_x, message_x = call(
        stage_kernel, (state_shape, decay_shape, message_shape), (x, message, *behind), 1
    )
    behind = from_behind(message_x, "sp_1")
    before_y, decay_y, message_y = call(
        stage_kernel, (state_shape, decay_shape, message_shape), (y, message_x, *behind), 1
    )
    behind = from_behind(message_y, "sp_0")
    message_y, queries, key_rows = lax.optimization_barrier((message_y, queries, key_rows))
    partial, reach, gating = call(
        within_kernel,
        (shape_of((length, values), f32), shape_of((length, channels), f32), shape_of((length, values), f32)),
        (queries, key_rows, value_rows, gate_logits, head_gain.reshape(1, -1), out_gate),
    )
    partial, reach, gating, *behind = lax.optimization_barrier((partial, reach, gating, *behind))
    half = shape_of((length // 2, values), bf16)
    given, entering = call(
        given_kernel,
        (half, shape_of((pairs * VALUE_DIM, LANES), bf16)),
        (core, z, *behind, before_y, decay_y, before_x, decay_x, partial, reach, gating),
        2,
        cost=300000,
    )
    kept = call(kept_kernel, half, (core, entering, partial, reach, gating), 1, cost=300000)
    taken = lax.ppermute(given, "tp", [(0, 1), (1, 0)])
    projected = call(own_kernel, shape_of((row_count, model_width), f32), (core, kept, out_weight, residual), 1, room=8)
    projected, taken = lax.optimization_barrier((projected, taken))
    merged, outgoing = call(
        project_kernel,
        (
            shape_of((row_count, model_width), bf16),
            shape_of((experts_total * capacity, SUB, LANES), bf16),
        ),
        (core, owners, taken, out_weight, projected, norm_gain.reshape(1, -1)),
        1,
        [
            pltpu.VMEM((row_count, SUB, LANES), bf16),
            pltpu.SMEM(owners.shape, jnp.int32),
            pltpu.SemaphoreType.DMA((1,)),
        ],
        room=14,
    )
    block = (experts_total, capacity * SUB, LANES)
    arrived = lax.all_to_all(outgoing.reshape(block), SP_TP, split_axis=0, concat_axis=0, tiled=True)
    served = experts(arrived.reshape(outgoing.shape), gate_weight, up_weight, down_weight)
    returned = lax.all_to_all(served.reshape(block), SP_TP, split_axis=0, concat_axis=0, tiled=True)
    return combine(slots, returned.reshape(outgoing.shape), merged, weights)


def solution(mesh):
    torus = Mesh(mesh.devices.reshape(4, 4, 4, mesh.shape["tp"]), ("sp_0", "sp_1", "sp_2", "tp"))
    in_specs = (
        P(SP_TP, None),
        P(SP, "tp"),
        P(SP, "tp"),
        P(SP, "tp"),
        P(SP, "tp"),
        P(SP, "tp"),
        P(),
        P(),
        P(),
        P(SP_TP, None),
        P(SP_TP),
        P(SP_TP, None),
        P(SP_TP, None, None),
        P(SP_TP, None, None),
        P(SP_TP, None, None),
    )
    out_specs = P(SP_TP, None)
    return jax.shard_map(local, mesh=torus, in_specs=in_specs, out_specs=out_specs, check_vma=False)
```
